32 devices in a mesh: sp: 8 (over z, x), tp: 4 (over y, core).
Axes of the slice: x: 2, y: 2, z: 4, core: 2. Of those that a mesh axis runs over, the one named last changes fastest.
Arguments:
- tokens: bfloat16 [2, 1536, 4096], P(None, 'sp', 'tp'), may hold values from -12 to 12
- query_weight: bfloat16 [4096, 2048], P(None, 'tp'), may hold values from -0.09375 to 0.09375
- key_weight: bfloat16 [4096, 2048], P(None, 'tp'), may hold values from -0.09375 to 0.09375
- value_weight: bfloat16 [4096, 2048], P(None, 'tp'), may hold values from -0.09375 to 0.09375
- gate_weight: bfloat16 [4096, 2048], P(None, 'tp'), may hold values from -0.09375 to 0.09375
- beta_weight: bfloat16 [4096, 16], P(None, 'tp'), may hold values from -0.09375 to 0.09375
- decay_weight: bfloat16 [4096, 16], P(None, 'tp'), may hold values from -0.09375 to 0.09375
- beta_bias: float32 [16], P('tp'), may hold values from -6 to -3
- rate_log: float32 [16], P('tp'), may hold values from -12 to -2.5
- out_gain: float32 [128], replicated, may hold values from 0.1 to 1.9
- new_query: bfloat16 [2, 16, 128], P(None, 'tp'), may hold values from -6 to 6
- new_key: bfloat16 [2, 16, 128], P(None, 'tp'), may hold values from -6 to 6
- new_value: bfloat16 [2, 16, 128], P(None, 'tp'), may hold values from -6 to 6
- new_beta: float32 [2, 16], P(None, 'tp'), may hold values from 0.1 to 0.9
- new_decay: float32 [2, 16], P(None, 'tp'), may hold values from 0.3 to 1
Outputs:
- mixed_out: bfloat16 [2, 1536, 2048], P(None, 'sp', 'tp')
- cache: bfloat16 [2, 16, 128, 128], P(None, 'tp', 'sp')
- first_out: float32 [2, 2048], P(None, 'tp')
The draws below stay inside these ranges and needn't reach their ends.
All inputs are finite; a program needn't handle non-finite values.
Results may differ from the reference program's by a relative error of at most 0.0073.
Values may be sent and summed in bfloat16 or wider, within the bound.
A program may use at most 64 MiB of HBM per device.

```python
import jax
import jax.numpy as jnp
from jax import lax

D = 4096
HEADS = 16
HEAD = 128
BLOCK = 64
SEQS = 2
LEN = 1536


def draw_tokens(key, part):
    key_base, key_level, key_common = jax.random.split(key, 3)
    blocks = LEN // BLOCK
    base_draw = jax.random.truncated_normal(key_base, -4.0, 4.0, (SEQS, LEN, D), jnp.float32)
    level_log = jax.random.uniform(key_level, (SEQS, blocks, 1, 1), jnp.float32, -1.0, 1.0)
    common = jnp.zeros((1, 1, D), jnp.float32)
    row_scale = jnp.broadcast_to(jnp.exp(level_log), (SEQS, blocks, BLOCK, 1)).reshape(SEQS, LEN, 1)
    return ((base_draw + common) * row_scale).astype(jnp.bfloat16)


def draw_rate_log(key, part):
    key_slow, key_quick, key_pick = jax.random.split(key, 3)
    slow_rates = jnp.log(jax.random.uniform(key_slow, (HEADS,), jnp.float32, 0.2, 0.6) / LEN)
    quick_rates = jnp.log(jax.random.uniform(key_quick, (HEADS,), jnp.float32, 0.02, 0.06))
    slow_picks = jax.random.randint(key_pick, (HEADS,), 0, 2)
    return jnp.where(slow_picks == 1, slow_rates, quick_rates)


def block_scale(stream_key, shape, shards, low, largest):
    factor_of = 1.0
    for dim, shards_of in shards:
        heights = jax.random.uniform(jax.random.fold_in(jax.random.fold_in(stream_key, 6), dim), (shards_of,), jnp.float32, low / len(shards), largest / len(shards))
        factor_of = factor_of * jnp.repeat(jnp.exp(heights), shape[dim] // shards_of).reshape((-1,) + (1,) * (len(shape) - 1 - dim))
    return factor_of


def centred(key, shape, scale, reach, pieces=(), kind=jnp.bfloat16):
    array = scale * jax.random.normal(key, shape, jnp.float32)
    if pieces:
        array = array * block_scale(key, shape, pieces, -0.22, 0.18)
    return jnp.clip(array, -reach, reach).astype(kind)


def setup_inputs(seed: int = 0) -> dict:
    streams_of = jax.random.split(jax.random.key(seed), 16)
    return {
        "tokens": draw_tokens(jax.random.fold_in(streams_of[15], 71), 0),
        "query_weight": centred(streams_of[1], (D, HEADS * HEAD), D ** -0.5, 0.09375, ((1, 4),)),
        "key_weight": centred(streams_of[2], (D, HEADS * HEAD), D ** -0.5, 0.09375, ((1, 4),)),
        "value_weight": centred(streams_of[3], (D, HEADS * HEAD), D ** -0.5, 0.09375, ((1, 4),)),
        "gate_weight": centred(streams_of[4], (D, HEADS * HEAD), D ** -0.5, 0.09375, ((1, 4),)),
        "beta_weight": centred(streams_of[5], (D, HEADS), D ** -0.5, 0.09375, ((1, 4),)),
        "decay_weight": centred(streams_of[6], (D, HEADS), D ** -0.5, 0.09375, ((1, 4),)),
        "beta_bias": jnp.clip(-6.0 + 3.0 * jax.random.uniform(streams_of[7], (HEADS,), jnp.float32) ** block_scale(streams_of[7], (HEADS,), ((0, 4),), -0.2, 0.2), -6.0, -3.0),
        "rate_log": draw_rate_log(jax.random.fold_in(streams_of[15], 71), 0),
        "out_gain": jnp.clip(1.0 + 0.18 * jax.random.normal(streams_of[9], (HEAD,), jnp.float32), 0.1, 1.9),
        "new_query": centred(streams_of[10], (SEQS, HEADS, HEAD), 1.0, 6.0, ((1, 4),)),
        "new_key": centred(streams_of[11], (SEQS, HEADS, HEAD), 1.0, 6.0, ((1, 4),)),
        "new_value": centred(streams_of[12], (SEQS, HEADS, HEAD), 1.0, 6.0, ((1, 4),)),
        "new_beta": jnp.clip(0.1 + 0.79999997 * jax.random.uniform(streams_of[13], (SEQS, HEADS), jnp.float32) ** block_scale(streams_of[13], (SEQS, HEADS), ((1, 4),), -0.2, 0.2), 0.1, 0.9),
        "new_decay": jnp.clip(0.3 + 0.7 * jax.random.uniform(streams_of[14], (SEQS, HEADS), jnp.float32) ** block_scale(streams_of[14], (SEQS, HEADS), ((1, 4),), -0.2, 0.2), 0.3, 1.0),
    }


unit_floor = 1.0
norm_floor = 0.001
highest = lax.Precision.HIGHEST

def matmul(form, left, right):
    return jnp.einsum(form, left, right, precision=highest)

def unit_rows(values):
    return values * lax.rsqrt(lax.optimization_barrier(jnp.sum(values * values, axis=-1, keepdims=True)) + unit_floor)

def head_norm(values, out_gain):
    return values * lax.rsqrt(lax.optimization_barrier(jnp.mean(values * values, axis=-1, keepdims=True)) + norm_floor) * out_gain

def stored(values):
    return lax.optimization_barrier(values.astype(jnp.bfloat16)).astype(jnp.float32)

def unit_lower_inverse(lower_part):
    extent = lower_part.shape[-1]
    nilpotent = -lower_part
    inverse = jnp.eye(extent, dtype=jnp.float32) + nilpotent
    for _ in range(extent.bit_length() - 2):
        nilpotent = matmul('...ij,...jk->...ik', nilpotent, nilpotent)
        inverse = inverse + matmul('...ij,...jk->...ik', nilpotent, inverse)
    return inverse

def prepare(query_rows, key_rows, value_rows, beta_in, decay_in, beta_bias, rate_log, seq_count, length, head_count):
    extent = query_rows.shape[-1] // head_count
    blocks = length // BLOCK

    def by_head(values):
        shaped = values.reshape(seq_count, blocks, BLOCK, head_count, extent)
        return shaped.transpose(0, 3, 1, 2, 4).reshape(seq_count * head_count, blocks, BLOCK, extent)

    def by_scalar(values):
        shaped = values.reshape(seq_count, blocks, BLOCK, head_count)
        return shaped.transpose(0, 3, 1, 2).reshape(seq_count * head_count, blocks, BLOCK)
    queries = unit_rows(by_head(query_rows))
    key_unit = unit_rows(by_head(key_rows))
    values = by_head(value_rows)
    strength = by_scalar(jax.nn.sigmoid(beta_in + beta_bias))
    decays = by_scalar(-jnp.exp(rate_log) * jax.nn.softplus(decay_in))
    return (queries, key_unit, values, strength, decays)

def block_terms(queries, key_unit, values, strength, decays):
    extent = decays.shape[-1]
    cumulative = jnp.cumsum(decays, axis=-1)
    causal = jnp.tril(jnp.ones((extent, extent), bool))
    strict = jnp.tril(jnp.ones((extent, extent), bool), -1)
    spread = cumulative[..., :, None] - cumulative[..., None, :]
    weights = jnp.where(causal, jnp.exp(jnp.where(causal, spread, 0.0)), 0.0)
    key_beta = key_unit * strength[..., None]
    lower_part = jnp.where(strict, matmul('...td,...sd->...ts', key_beta, key_unit) * weights, 0.0)
    inverse = unit_lower_inverse(lower_part)
    update = matmul('...ts,...se->...te', inverse, values * strength[..., None])
    carry_w = matmul('...ts,...sd->...td', inverse, key_beta * jnp.exp(cumulative)[..., None])
    scores = matmul('...td,...sd->...ts', queries, key_unit) * weights
    query_decay = queries * jnp.exp(cumulative)[..., None]
    last_log = cumulative[..., -1]
    key_decay = key_unit * jnp.exp(last_log[..., None] - cumulative)[..., None]
    return (update, carry_w, query_decay, scores, key_decay, last_log)

def first_read(cache_whole, new_query, new_key, new_value, new_beta, new_decay, out_gain):
    seq_count, head_count, extent, _ = cache_whole.shape
    memory = lax.optimization_barrier(cache_whole).astype(jnp.float32)
    query_unit = unit_rows(new_query.astype(jnp.float32))
    key_unit = unit_rows(new_key.astype(jnp.float32))
    recall = matmul('shde,shd->she', memory, query_unit)
    retrieve = matmul('shde,shd->she', memory, key_unit)
    intersect = lax.optimization_barrier(jnp.sum(key_unit * query_unit, axis=-1))
    fresh_values = new_value.astype(jnp.float32) - new_decay[..., None] * retrieve
    read_heads = new_decay[..., None] * recall + (new_beta * intersect)[..., None] * fresh_values
    return head_norm(read_heads, out_gain).reshape(seq_count, head_count * extent)

def reference(tokens, query_weight, key_weight, value_weight, gate_weight, beta_weight, decay_weight, beta_bias, rate_log, out_gain, new_query, new_key, new_value, new_beta, new_decay):
    flat_rows = tokens.reshape(SEQS * LEN, D)

    def project(weight):
        return jnp.dot(flat_rows, weight, preferred_element_type=jnp.float32)
    query_rows = stored(project(query_weight))
    key_rows = stored(project(key_weight))
    value_rows = stored(project(value_weight))
    gate_rows = stored(project(gate_weight))
    beta_in = project(beta_weight)
    decay_in = project(decay_weight)
    prepared = prepare(query_rows, key_rows, value_rows, beta_in, decay_in, beta_bias, rate_log, SEQS, LEN, HEADS)
    block_data = block_terms(*prepared)

    def advance(state_now, inputs):
        update, carry_w, query_decay, scores, key_decay, last_log = inputs
        fresh_values = update - matmul('btd,bde->bte', carry_w, state_now)
        block_out = matmul('btd,bde->bte', query_decay, state_now) + matmul('bts,bse->bte', scores, fresh_values)
        state_next = state_now * jnp.exp(last_log)[:, None, None] + matmul('bsd,bse->bde', key_decay, fresh_values)
        return (state_next, block_out)
    inputs = tuple((jnp.moveaxis(member, 1, 0) for member in block_data))
    batch_size = SEQS * HEADS
    final_state, outputs = lax.scan(advance, jnp.zeros((batch_size, HEAD, HEAD), jnp.float32), inputs)
    heads_out = outputs.reshape(LEN // BLOCK, SEQS, HEADS, BLOCK, HEAD).transpose(1, 0, 3, 2, 4)
    heads_out = heads_out.reshape(SEQS, LEN, HEADS, HEAD)
    gate_values = gate_rows.reshape(SEQS, LEN, HEADS, HEAD)
    mixed_out = (head_norm(heads_out, out_gain) * jax.nn.silu(gate_values)).astype(jnp.bfloat16)
    mixed_out = mixed_out.reshape(SEQS, LEN, HEADS * HEAD)
    cache = final_state.reshape(SEQS, HEADS, HEAD, HEAD).astype(jnp.bfloat16)
    first_out = first_read(cache, new_query, new_key, new_value, new_beta, new_decay, out_gain)
    return (mixed_out, cache, first_out)
```

```python
import functools

import jax
import jax.numpy as jnp
from jax import lax
from jax.experimental import pallas as pl
from jax.experimental.pallas import tpu as pltpu
from jax.sharding import PartitionSpec as P

unit_floor = 1.0
norm_floor = 0.001
highest = lax.Precision.HIGHEST
MESH = pl.DeviceIdType.MESH
PAD = 8
INNER, OUTER = 8, 64
f32 = jnp.float32
bf16 = jnp.bfloat16

NN = (((1,), (0,)), ((), ()))
NT = (((1,), (1,)), ((), ()))
TN = (((0,), (0,)), ((), ()))


def dot(left, right, dims=NN, precision=None):
    return lax.dot_general(left, right, dims, precision=precision, preferred_element_type=f32)


def unit_rows(values):
    return values * lax.rsqrt(jnp.sum(values * values, axis=-1, keepdims=True) + unit_floor)


def group_of(n, heads):
    g = 1
    while g < n and (g < heads or g * g < n):
        g *= 2
    return g


def fused_kernel(
    tn, sn, seqs, heads, x_ref, wq_ref, wk_ref, wv_ref, wg_ref, bw_ref, dw_ref, bias_ref, rate_ref, gain_ref,
    nq_ref, nk_ref, nv_ref, nb_ref, nd_ref, mixed_ref, cache_ref, first_ref,
    bd, xs, wbuf, acc, sacc, masks, cum_col, kh_buf, spread, uw_buf, local_out, reach, gated,
    out_box, in_box, mid_out, mid_in, back_out, back_in, tail_out, tail_in,
    xsem, wsem, cross_sem, part_sem, fwd_sem, rx, prx,
    send1, recv1, send2, recv2, send3, recv3, send4, recv4,
):
    _, _, span, kd = xs.shape
    width = wq_ref.shape[1]
    extent = width // heads
    key_rows = extent // sn
    chunks = xsem.shape[1]
    kc = kd // chunks
    tme, me = lax.axis_index("tp"), lax.axis_index("sp")
    y, c = tme // 2, lax.rem(tme, 2)
    chips = tn // 2
    partner = y * 2 + (1 - c)
    g = group_of(sn, heads)
    groups = sn // g
    team, m = me // g, lax.rem(me, g)
    weights = (wq_ref, wk_ref, wv_ref, wg_ref)

    barrier = pltpu.get_barrier_semaphore()
    pl.semaphore_signal(barrier, inc=1, device_id={"tp": partner}, device_id_type=MESH)
    for d in range(1, chips):
        to = lax.rem(y + d, chips) * 2 + c
        pl.semaphore_signal(barrier, inc=1, device_id={"tp": to}, device_id_type=MESH)
    for d in range(1, sn):
        pl.semaphore_signal(barrier, inc=1, device_id={"sp": lax.rem(me + d, sn)}, device_id_type=MESH)

    order = [tme, partner]
    for d in range(1, chips):
        source = lax.rem(y - d + chips, chips)
        order += [source * 2 + c, source * 2 + (1 - c)]

    def cols(ck):
        return pl.ds(ck * kc, kc)

    def token_copy(s, ck):
        return pltpu.make_async_copy(
            x_ref.at[pl.ds(s * span, span), cols(ck)], xs.at[tme, s, :, cols(ck)], xsem.at[s, ck]
        )

    def weight_copy(w, slot):
        start = pl.multiple_of(order[slot] * kd, kd)
        return pltpu.make_async_copy(
            weights[w].at[pl.ds(start, kd), :], wbuf.at[w, slot], wsem.at[w, slot]
        )

    for s in range(seqs):
        for ck in range(chunks):
            token_copy(s, ck).start()
    for slot in range(tn):
        for w in range(4):
            weight_copy(w, slot).start()

    bd[...] = jnp.zeros_like(bd)
    bd[0 : bw_ref.shape[0]] = bw_ref[...]
    bd[PAD : PAD + dw_ref.shape[0]] = dw_ref[...]
    row = lax.broadcasted_iota(jnp.int32, (span, span), 0)
    col = lax.broadcasted_iota(jnp.int32, (span, span), 1)
    same_in = row // INNER == col // INNER
    same_out = row // OUTER == col // OUTER
    masks[0] = jnp.where(same_in, 1.0, 0.0).astype(bf16)
    masks[1] = jnp.where(same_out & ~same_in, 1.0, 0.0).astype(bf16)
    masks[2] = jnp.where(same_out, 0.0, 1.0).astype(bf16)
    slot_of = lax.broadcasted_iota(jnp.int32, (PAD, 1), 0)
    bias = jnp.zeros((PAD, 1), f32)
    rate = jnp.zeros((PAD, 1), f32)
    for h in range(heads):
        bias = jnp.where(slot_of == h, bias_ref[h], bias)
        rate = jnp.where(slot_of == h, rate_ref[h], rate)
    pl.semaphore_wait(barrier, chips + sn - 1)

    def cross_copy(d, s, ck):
        to = lax.rem(y + d, chips) * 2 + c
        return pltpu.make_async_remote_copy(
            src_ref=xs.at[tme, s, :, cols(ck)], dst_ref=xs.at[tme, s, :, cols(ck)],
            send_sem=cross_sem.at[d - 1, s, ck], recv_sem=rx.at[tme, s, ck],
            device_id={"tp": to}, device_id_type=MESH,
        )

    def part_copy(s):
        return pltpu.make_async_remote_copy(
            src_ref=xs.at[tme, s], dst_ref=xs.at[tme, s],
            send_sem=part_sem.at[s], recv_sem=prx.at[s],
            device_id={"tp": partner}, device_id_type=MESH,
        )

    def fwd_copy(d, s, ck):
        b = order[2 * d]
        return pltpu.make_async_remote_copy(
            src_ref=xs.at[b, s, :, cols(ck)], dst_ref=xs.at[b, s, :, cols(ck)],
            send_sem=fwd_sem.at[d - 1, s, ck], recv_sem=rx.at[b, s, ck],
            device_id={"tp": partner}, device_id_type=MESH,
        )

    def arrive(b, s, ck):
        pltpu.make_async_remote_copy(
            src_ref=xs.at[b, s, :, cols(ck)], dst_ref=xs.at[b, s, :, cols(ck)],
            send_sem=part_sem.at[0], recv_sem=rx.at[b, s, ck],
            device_id={"tp": partner}, device_id_type=MESH,
        ).wait_recv()

    for s in range(seqs):
        for ck in range(chunks):
            token_copy(s, ck).wait()
            for d in range(1, chips):
                cross_copy(d, s, ck).start()
        part_copy(s).start()

    def small(x, start, depth, s, first):
        piece = bd[:, pl.ds(pl.multiple_of(start, depth), depth)]
        term = dot(piece, x, NT)
        sacc[s] = term if first else sacc[s] + term

    def use_whole(slot, s):
        b = order[slot]
        x = xs[b, s]
        for w in range(4):
            if s == 0:
                weight_copy(w, slot).wait()
            term = dot(x, wbuf[w, slot])
            acc[s, w] = term if slot == 0 else acc[s, w] + term
        small(x, b * kd, kd, s, slot == 0)

    def use(slot, s, ck):
        b = order[slot]
        x = xs[b, s, :, cols(ck)]
        for w in range(4):
            if s == 0 and ck == 0:
                weight_copy(w, slot).wait()
            acc[s, w] += dot(x, wbuf[w, slot, cols(ck), :])
        small(x, b * kd + ck * kc, kc, s, False)

    def forward(d, s, ck):
        arrive(order[2 * d], s, ck)
        fwd_copy(d, s, ck).start()

    def finish_chunk(d, s, ck):
        use(2 * d, s, ck)
        arrive(order[2 * d + 1], s, ck)
        use(2 * d + 1, s, ck)

    def heads_of(w, s):
        return [acc[s, w, :, h * extent : (h + 1) * extent].astype(bf16).astype(f32) for h in range(heads)]

    def owner_of(s, h):
        return (s * heads + h) % g

    def box_copy(s, h):
        return pltpu.make_async_remote_copy(
            src_ref=out_box.at[s, h], dst_ref=in_box.at[s, m],
            send_sem=send1.at[s, h], recv_sem=recv1.at[s, m],
            device_id={"sp": team * g + owner_of(s, h)}, device_id_type=MESH,
        )

    def boxes(s):
        beta = jax.nn.sigmoid(sacc[s, 0:PAD, :] + bias)
        pre = sacc[s, PAD : 2 * PAD, :]
        soft = jnp.maximum(pre, 0.0) + jnp.log1p(jnp.exp(-jnp.abs(pre)))
        upper = jnp.where(row <= col, 1.0, 0.0)
        cum = dot(-jnp.exp(rate) * soft, upper, NN, highest)
        cum_t, beta_t = cum.T, beta.T
        cum_col[s] = cum_t
        causal = row >= col
        strict = row > col
        unit = jnp.where(row == col, 1.0, 0.0)
        hs = range(heads)
        k = [unit_rows(v) for v in heads_of(1, s)]
        kh = [v.astype(bf16) for v in k]
        kk = [dot(v, v, NT) for v in kh]
        low, right, kdec, last = [], [], [], []
        v = heads_of(2, s)
        for h in hs:
            cumc, bt = cum_t[:, h : h + 1], beta_t[:, h : h + 1]
            wts = jnp.where(causal, jnp.exp(jnp.where(causal, cumc - cum[h : h + 1, :], 0.0)), 0.0)
            spread[h] = wts
            kh_buf[h] = kh[h]
            low.append(jnp.where(strict, kk[h] * (bt * wts), 0.0).astype(bf16))
            kb = k[h] * bt
            right.append(jnp.concatenate([v[h] * bt, kb * jnp.exp(cumc)], axis=1).astype(bf16))
            end = cumc[span - 1 :, :]
            kdec.append((k[h] * jnp.exp(end - cumc)).astype(bf16))
            last.append(jnp.exp(end))

        def climb(part, inv, size, ratio):
            if inv is None:
                power = part
                total = [unit - p.astype(f32) for p in part]
            else:
                low_h = [i.astype(bf16) for i in inv]
                power = [dot(i, p).astype(bf16) for i, p in zip(low_h, part)]
                total = [i - dot(p, j) for i, p, j in zip(inv, power, low_h)]
            reached = 2
            while reached < ratio:
                power = [dot(p, p).astype(bf16) for p in power]
                total = [t + dot(p, t.astype(bf16)) for t, p in zip(total, power)]
                reached *= 2
            return total

        inv = climb([p * masks[0] for p in low], None, INNER, INNER)
        inv = climb([p * masks[1] for p in low], inv, OUTER, OUTER // INNER)
        inv_h = [i.astype(bf16) for i in inv]
        power = [dot(i, p * masks[2]).astype(bf16) for i, p in zip(inv_h, low)]
        term = [dot(i, r) for i, r in zip(inv_h, right)]
        uw = term
        for level in range(1, -(-span // OUTER)):
            term = [dot(p, t.astype(bf16)) for p, t in zip(power, term)]
            uw = [u - t if level % 2 else u + t for u, t in zip(uw, term)]
        uw = [u.astype(bf16) for u in uw]
        z = [dot(a, u, TN) for a, u in zip(kdec, uw)]
        eye = lax.broadcasted_iota(jnp.int32, (extent, extent), 0) == lax.broadcasted_iota(
            jnp.int32, (extent, extent), 1
        )
        for h in hs:
            out_box[s, h, 0] = (jnp.where(eye, last[h] - 1.0, 0.0) - z[h][:, extent:]).astype(bf16)
            out_box[s, h, 1] = z[h][:, :extent].astype(bf16)
            uw_buf[h] = uw[h]
        for h in hs:
            own = m == owner_of(s, h)

            @pl.when(own)
            def _():
                in_box[s, m] = out_box[s, h]

            @pl.when(jnp.logical_not(own))
            def _():
                box_copy(s, h).start()

    def queries(s):
        cum_t = cum_col[s]
        gain = gain_ref[...]
        hs = range(heads)
        q = [unit_rows(v) for v in heads_of(0, s)]
        scores = [(dot(q[h].astype(bf16), kh_buf[h], NT) * spread[h]).astype(bf16) for h in hs]
        out = [dot(scores[h], uw_buf[h]) for h in hs]
        gates = heads_of(3, s)
        for h in hs:
            local_out[s, h] = out[h][:, :extent]
            reach[s, h] = (q[h] * jnp.exp(cum_t[:, h : h + 1]) - out[h][:, extent:]).astype(bf16)
            gated[s, h] = gates[h] * jax.nn.sigmoid(gates[h]) * gain

    def own_head(s):
        return lax.rem(m + g - (s * heads) % g, g)

    def back_copy(s, i):
        return pltpu.make_async_remote_copy(
            src_ref=back_out.at[s, i], dst_ref=back_in.at[s, own_head(s)],
            send_sem=send2.at[s, i], recv_sem=recv2.at[s, own_head(s)],
            device_id={"sp": team * g + i}, device_id_type=MESH,
        )

    def mid_copy(s):
        return pltpu.make_async_remote_copy(
            src_ref=mid_out.at[s], dst_ref=mid_in.at[s], send_sem=send3.at[s], recv_sem=recv3.at[s],
            device_id={"sp": lax.rem(me + g, sn)}, device_id_type=MESH,
        )

    def tail_copy(s, j):
        return pltpu.make_async_remote_copy(
            src_ref=tail_out.at[s, j], dst_ref=tail_in.at[s, own_head(s)],
            send_sem=send4.at[s, j], recv_sem=recv4.at[s, own_head(s)],
            device_id={"sp": j}, device_id_type=MESH,
        )

    def box_wait(s, i):
        @pl.when(i != m)
        def _():
            pltpu.make_async_remote_copy(
                src_ref=out_box.at[s, 0], dst_ref=in_box.at[s, i],
                send_sem=send1.at[s, 0], recv_sem=recv1.at[s, i],
                device_id={"sp": team * g + i}, device_id_type=MESH,
            ).wait_recv()

    def give_back(s):
        for i in range(g):

            @pl.when(i == m)
            def _():
                back_in[s, own_head(s)] = back_out[s, i]

            @pl.when(i != m)
            def _():
                back_copy(s, i).start()

    def conclude(s, final):
        memory = final.astype(bf16).astype(f32)
        h = own_head(s)
        shape3 = nq_ref.shape
        mine = (lax.broadcasted_iota(jnp.int32, shape3, 0) == s) & (lax.broadcasted_iota(jnp.int32, shape3, 1) == h)

        def own(ref):
            kept = jnp.where(mine, ref[...].astype(f32), 0.0)
            return jnp.sum(jnp.sum(kept, axis=0), axis=0, keepdims=True)

        qn, kn = unit_rows(own(nq_ref)), unit_rows(own(nk_ref))
        both = jnp.concatenate([jnp.broadcast_to(qn, (PAD, extent)), jnp.broadcast_to(kn, (PAD, extent))], axis=0)
        reads = dot(both, memory, NN, highest)
        recall, retrieve = reads[0:1], reads[PAD : PAD + 1]
        beta_new, decay_new = nb_ref[s, h], nd_ref[s, h]
        fresh = own(nv_ref) - decay_new * retrieve
        meet = jnp.sum(kn * qn, axis=-1, keepdims=True)
        read = decay_new * recall + (beta_new * meet) * fresh
        norm = lax.rsqrt(jnp.mean(read * read, axis=-1, keepdims=True) + norm_floor)
        answer = jnp.broadcast_to(read * norm * gain_ref[...], (PAD, extent))
        for j in range(sn):
            tail_out[s, j, 0:key_rows, :] = memory[j * key_rows : (j + 1) * key_rows]
            tail_out[s, j, tail_out.shape[2] - PAD :, :] = answer

        def push(j, _):
            @pl.when(j == me)
            def _():
                tail_in[s, h] = tail_out[s, me]

            @pl.when(j != me)
            def _():
                tail_copy(s, j).start()

            return 0

        lax.fori_loop(0, sn, push, 0)

    def chain_first(s):
        @pl.when((own_head(s) < heads) & (team == 0))
        def _():
            for i in range(g):
                box_wait(s, i)
            state = jnp.zeros((extent, extent), f32)
            for i in range(g):
                half = state.astype(bf16)
                back_out[s, i] = half
                if i == 0:
                    state = in_box[s, i, 1].astype(f32)
                else:
                    state = state + dot(in_box[s, i, 0], half) + in_box[s, i, 1].astype(f32)
            if groups > 1:
                mid_out[s] = state.astype(bf16)
                mid_copy(s).start()
            give_back(s)
            if groups == 1:
                conclude(s, state)

    def chain_later(s):
        if groups == 1:
            return

        @pl.when((own_head(s) < heads) & (team > 0))
        def _():
            for i in range(g):
                box_wait(s, i)
            shift, drive = [None], [None]
            for i in range(g):
                step, push = in_box[s, i, 0], in_box[s, i, 1].astype(f32)
                if i == 0:
                    shift.append(step.astype(f32))
                    drive.append(push)
                else:
                    shift.append(shift[i] + step.astype(f32) + dot(step, shift[i].astype(bf16)))
                    drive.append(drive[i] + push + dot(step, drive[i].astype(bf16)))
            moves = jnp.concatenate([a.astype(bf16) for a in shift[1:]], axis=0)
            pltpu.make_async_remote_copy(
                src_ref=mid_out.at[s], dst_ref=mid_in.at[s], send_sem=send3.at[s], recv_sem=recv3.at[s],
                device_id={"sp": lax.rem(me + sn - g, sn)}, device_id_type=MESH,
            ).wait_recv()
            start = mid_in[s]
            moved = dot(moves, start)
            base = start.astype(f32)
            back_out[s, 0] = start
            for i in range(1, g):
                back_out[s, i] = (base + moved[(i - 1) * extent : i * extent] + drive[i]).astype(bf16)
            state = base + moved[(g - 1) * extent :] + drive[g]

            @pl.when(team < groups - 1)
            def _():
                mid_out[s] = state.astype(bf16)
                mid_copy(s).start()

            give_back(s)

            @pl.when(team == groups - 1)
            def _():
                conclude(s, state)

    def finish(s):
        for h in range(heads):
            o = owner_of(s, h)

            @pl.when(m != o)
            def _():
                pltpu.make_async_remote_copy(
                    src_ref=back_out.at[s, 0], dst_ref=back_in.at[s, h],
                    send_sem=send2.at[s, 0], recv_sem=recv2.at[s, h],
                    device_id={"sp": team * g + o}, device_id_type=MESH,
                ).wait_recv()

        outs = [local_out[s, h] + dot(reach[s, h], back_in[s, h]) for h in range(heads)]
        for h in range(heads):
            o = outs[h]
            norm = lax.rsqrt(jnp.mean(o * o, axis=-1, keepdims=True) + norm_floor)
            mixed_ref[s * span : (s + 1) * span, h * extent : (h + 1) * extent] = (o * norm * gated[s, h]).astype(bf16)

    def take_tail(s):
        for h in range(heads):
            source = (groups - 1) * g + owner_of(s, h)

            @pl.when(me != source)
            def _():
                pltpu.make_async_remote_copy(
                    src_ref=tail_out.at[s, 0], dst_ref=tail_in.at[s, h],
                    send_sem=send4.at[s, 0], recv_sem=recv4.at[s, h],
                    device_id={"sp": source}, device_id_type=MESH,
                ).wait_recv()

            p = s * heads + h
            cache_ref[p] = tail_in[s, h, 0:key_rows, :].astype(bf16)
            edge = tail_in.shape[2] - PAD
            first_ref[p : p + 1, :] = tail_in[s, h, edge : edge + 1, :]

    for s in range(seqs):
        use_whole(0, s)
    for s in range(seqs):
        pltpu.make_async_remote_copy(
            src_ref=xs.at[partner, s], dst_ref=xs.at[partner, s], send_sem=part_sem.at[s], recv_sem=prx.at[s],
            device_id={"tp": partner}, device_id_type=MESH,
        ).wait_recv()
        use_whole(1, s)

    for s in range(seqs):
        for ck in range(chunks):
            for d in range(1, chips):
                if s == 0 or ck > 0:
                    forward(d, s, ck)
                if s > 0 and ck == chunks - 1 and d == chips - 1:
                    chain_first(s - 1)
                finish_chunk(d, s, ck)
        boxes(s)
        if s > 0:
            chain_later(s - 1)
        if s < seqs - 1:
            for d in range(1, chips):
                forward(d, s + 1, 0)
        queries(s)
    for s in range(seqs - 1):
        finish(s)
        take_tail(s)
    chain_first(seqs - 1)
    chain_later(seqs - 1)
    finish(seqs - 1)
    take_tail(seqs - 1)

    for s in range(seqs):
        part_copy(s).wait_send()
        for ck in range(chunks):
            for d in range(1, chips):
                cross_copy(d, s, ck).wait_send()
                fwd_copy(d, s, ck).wait_send()
        for h in range(heads):

            @pl.when(m != owner_of(s, h))
            def _():
                box_copy(s, h).wait_send()

        @pl.when(own_head(s) < heads)
        def _():
            for i in range(g):

                @pl.when(i != m)
                def _():
                    back_copy(s, i).wait_send()

            @pl.when(team < groups - 1)
            def _():
                mid_copy(s).wait_send()

            @pl.when(team == groups - 1)
            def _():
                for j in range(sn):

                    @pl.when(j != me)
                    def _():
                        tail_copy(s, j).wait_send()


def fused(tn, sn, seqs, heads, tokens, weights, bw, dw, bias, rate, gain, nq, nk, nv, nb, nd):
    rows, kd = tokens.shape
    width = weights[0].shape[1]
    kc = 256 if kd % 256 == 0 else kd
    chunks, chips, span = kd // kc, tn // 2, rows // seqs
    extent = width // heads
    pairs, key_rows = seqs * heads, extent // sn
    tail = -(-key_rows // PAD) * PAD + PAD
    g = group_of(sn, heads)
    vmem = pl.BlockSpec(memory_space=pltpu.VMEM)
    smem = pl.BlockSpec(memory_space=pltpu.SMEM)
    hbm = pl.BlockSpec(memory_space=pl.ANY)
    dma = pltpu.SemaphoreType.DMA
    return pl.pallas_call(
        functools.partial(fused_kernel, tn, sn, seqs, heads),
        out_shape=(
            jax.ShapeDtypeStruct((rows, width), bf16),
            jax.ShapeDtypeStruct((pairs, key_rows, extent), bf16),
            jax.ShapeDtypeStruct((pairs, extent), f32),
        ),
        in_specs=[hbm] * 5 + [vmem] * 2 + [smem] * 2 + [vmem] * 4 + [smem] * 2,
        out_specs=(vmem,) * 3,
        scratch_shapes=[
            pltpu.VMEM((2 * PAD, bw.shape[1]), bf16),
            pltpu.VMEM((tn, seqs, span, kd), bf16),
            pltpu.VMEM((4, tn, kd, width), bf16),
            pltpu.VMEM((seqs, 4, span, width), f32),
            pltpu.VMEM((seqs, 2 * PAD, span), f32),
            pltpu.VMEM((3, span, span), bf16),
            pltpu.VMEM((seqs, span, PAD), f32),
            pltpu.VMEM((heads, span, extent), bf16),
            pltpu.VMEM((heads, span, span), f32),
            pltpu.VMEM((heads, span, 2 * extent), bf16),
            pltpu.VMEM((seqs, heads, span, extent), f32),
            pltpu.VMEM((seqs, heads, span, extent), bf16),
            pltpu.VMEM((seqs, heads, span, extent), f32),
            pltpu.VMEM((seqs, heads, 2, extent, extent), bf16),
            pltpu.VMEM((seqs, g, 2, extent, extent), bf16),
            pltpu.VMEM((seqs, extent, extent), bf16),
            pltpu.VMEM((seqs, extent, extent), bf16),
            pltpu.VMEM((seqs, g, extent, extent), bf16),
            pltpu.VMEM((seqs, heads, extent, extent), bf16),
            pltpu.VMEM((seqs, sn, tail, extent), f32),
            pltpu.VMEM((seqs, heads, tail, extent), f32),
            dma((seqs, chunks)),
            dma((4, tn)),
            dma((chips - 1, seqs, chunks)),
            dma((seqs,)),
            dma((chips - 1, seqs, chunks)),
            dma((tn, seqs, chunks)),
            dma((seqs,)),
            dma((seqs, heads)),
            dma((seqs, g)),
            dma((seqs, g)),
            dma((seqs, heads)),
            dma((seqs,)),
            dma((seqs,)),
            dma((seqs, sn)),
            dma((seqs, heads)),
        ],
        compiler_params=pltpu.CompilerParams(
            collective_id=0, has_side_effects=True, vmem_limit_bytes=60 * 1024 * 1024
        ),
    )(tokens, *weights, bw, dw, bias, rate, gain, nq, nk, nv, nb, nd)


def shards(
    tokens, query_weight, key_weight, value_weight, gate_weight, beta_weight, decay_weight,
    beta_bias, rate_log, out_gain, new_query, new_key, new_value, new_beta, new_decay,
):
    seqs, span, kd = tokens.shape
    heads = rate_log.shape[0]
    extent = out_gain.shape[0]
    tp, sp = lax.axis_size("tp"), lax.axis_size("sp")
    weights = (query_weight, key_weight, value_weight, gate_weight)
    mixed, cache, first = fused(
        tp, sp, seqs, heads, tokens.reshape(seqs * span, kd), weights, beta_weight.T, decay_weight.T, beta_bias,
        rate_log, out_gain[None], new_query, new_key, new_value, new_beta, new_decay,
    )
    return (
        mixed.reshape(seqs, span, heads * extent),
        cache.reshape(seqs, heads, extent // sp, extent),
        first.reshape(seqs, heads * extent),
    )


def solution(mesh):
    placed = (
        P(None, "sp", "tp"),
        P(None, "tp"),
        P(None, "tp"),
        P(None, "tp"),
        P(None, "tp"),
        P(None, "tp"),
        P(None, "tp"),
        P("tp"),
        P("tp"),
        P(),
        P(None, "tp", None),
        P(None, "tp", None),
        P(None, "tp", None),
        P(None, "tp"),
        P(None, "tp"),
    )
    return jax.shard_map(
        shards,
        mesh=mesh,
        in_specs=placed,
        out_specs=(P(None, "sp", "tp"), P(None, "tp", "sp", None), P(None, "tp")),
        check_vma=False,
    )
```

```python
import functools

import jax
import jax.numpy as jnp
from jax import lax
from jax.experimental import pallas as pl
from jax.experimental.pallas import tpu as pltpu
from jax.sharding import PartitionSpec as P

unit_floor = 1.0
norm_floor = 0.001
highest = lax.Precision.HIGHEST
MESH = pl.DeviceIdType.MESH
PAD = 8
INNER, OUTER = 8, 64
f32 = jnp.float32
bf16 = jnp.bfloat16

NN = (((1,), (0,)), ((), ()))
NT = (((1,), (1,)), ((), ()))
TN = (((0,), (0,)), ((), ()))


def dot(left, right, dims=NN, precision=None):
    return lax.dot_general(left, right, dims, precision=precision, preferred_element_type=f32)


def unit_rows(values):
    return values * lax.rsqrt(jnp.sum(values * values, axis=-1, keepdims=True) + unit_floor)


def group_of(n, heads):
    g = 1
    while g < n and (g < heads or g * g < n):
        g *= 2
    return g


def fused_kernel(
    tn, sn, seqs, heads, x_ref, wq_ref, wk_ref, wv_ref, wg_ref, bw_ref, dw_ref, bias_ref, rate_ref, gain_ref,
    nq_ref, nk_ref, nv_ref, nb_ref, nd_ref, mixed_ref, cache_ref, first_ref,
    bd, xs, wbuf, acc, sacc, masks, cum_col, kh_buf, spread, uw_buf, local_out, reach, gated,
    out_box, in_box, mid_out, mid_in, back_out, back_in, tail_out, tail_in,
    xsem, wsem, cross_sem, part_sem, fwd_sem, rx, prx,
    send1, recv1, send2, recv2, send3, recv3, send4, recv4, hello,
):
    _, _, span, kd = xs.shape
    width = wq_ref.shape[1]
    extent = width // heads
    key_rows = extent // sn
    chunks = rx.shape[2]
    kc = kd // chunks
    tme, me = lax.axis_index("tp"), lax.axis_index("sp")
    y, c = tme // 2, lax.rem(tme, 2)
    chips = tn // 2
    partner = y * 2 + (1 - c)
    g = group_of(sn, heads)
    groups = sn // g
    team, m = me // g, lax.rem(me, g)
    weights = (wq_ref, wk_ref, wv_ref, wg_ref)

    barrier = pltpu.get_barrier_semaphore()
    pl.semaphore_signal(barrier, inc=1, device_id={"tp": partner}, device_id_type=MESH)
    for d in range(1, chips):
        to = lax.rem(y + d, chips) * 2 + c
        pl.semaphore_signal(barrier, inc=1, device_id={"tp": to}, device_id_type=MESH)
    for d in range(1, sn):

        @pl.when(me + d < sn)
        def _():
            pl.semaphore_signal(barrier, inc=1, device_id={"sp": me + d}, device_id_type=MESH)

    order = [tme, partner]
    for d in range(1, chips):
        source = lax.rem(y - d + chips, chips)
        order += [source * 2 + c, source * 2 + (1 - c)]

    def cols(ck):
        return pl.ds(ck * kc, kc)

    def token_copy(s):
        return pltpu.make_async_copy(x_ref.at[pl.ds(s * span, span), :], xs.at[tme, s], xsem.at[s])

    def weight_copy(w, slot):
        start = pl.multiple_of(order[slot] * kd, kd)
        return pltpu.make_async_copy(
            weights[w].at[pl.ds(start, kd), :], wbuf.at[w, slot], wsem.at[w, slot]
        )

    for s in range(seqs):
        token_copy(s).start()
    pl.semaphore_wait(barrier, chips + me)

    def cross_copy(d, s, ck):
        to = lax.rem(y + d, chips) * 2 + c
        return pltpu.make_async_remote_copy(
            src_ref=xs.at[tme, s, :, cols(ck)], dst_ref=xs.at[tme, s, :, cols(ck)],
            send_sem=cross_sem.at[d - 1, s, ck], recv_sem=rx.at[tme, s, ck],
            device_id={"tp": to}, device_id_type=MESH,
        )

    def part_copy(s):
        return pltpu.make_async_remote_copy(
            src_ref=xs.at[tme, s], dst_ref=xs.at[tme, s],
            send_sem=part_sem.at[s], recv_sem=prx.at[s],
            device_id={"tp": partner}, device_id_type=MESH,
        )

    for s in range(seqs):
        token_copy(s).wait()
        for ck in range(chunks):
            for d in range(1, chips):
                cross_copy(d, s, ck).start()
        part_copy(s).start()
    for slot in range(tn):
        for w in range(4):
            weight_copy(w, slot).start()
    for d in range(1, sn):

        @pl.when(me >= d)
        def _():
            pl.semaphore_signal(hello, inc=1, device_id={"sp": me - d}, device_id_type=MESH)

    bd[...] = jnp.zeros_like(bd)
    bd[0 : bw_ref.shape[0]] = bw_ref[...]
    bd[PAD : PAD + dw_ref.shape[0]] = dw_ref[...]
    row = lax.broadcasted_iota(jnp.int32, (span, span), 0)
    col = lax.broadcasted_iota(jnp.int32, (span, span), 1)
    same_in = row // INNER == col // INNER
    same_out = row // OUTER == col // OUTER
    masks[0] = jnp.where(same_in, 1.0, 0.0).astype(bf16)
    masks[1] = jnp.where(same_out & ~same_in, 1.0, 0.0).astype(bf16)
    masks[2] = jnp.where(same_out, 0.0, 1.0).astype(bf16)
    slot_of = lax.broadcasted_iota(jnp.int32, (PAD, 1), 0)
    bias = jnp.zeros((PAD, 1), f32)
    rate = jnp.zeros((PAD, 1), f32)
    for h in range(heads):
        bias = jnp.where(slot_of == h, bias_ref[h], bias)
        rate = jnp.where(slot_of == h, rate_ref[h], rate)

    def fwd_copy(d, s, ck):
        b = order[2 * d]
        return pltpu.make_async_remote_copy(
            src_ref=xs.at[b, s, :, cols(ck)], dst_ref=xs.at[b, s, :, cols(ck)],
            send_sem=fwd_sem.at[d - 1, s, ck], recv_sem=rx.at[b, s, ck],
            device_id={"tp": partner}, device_id_type=MESH,
        )

    def arrive(b, s, ck):
        pltpu.make_async_remote_copy(
            src_ref=xs.at[b, s, :, cols(ck)], dst_ref=xs.at[b, s, :, cols(ck)],
            send_sem=part_sem.at[0], recv_sem=rx.at[b, s, ck],
            device_id={"tp": partner}, device_id_type=MESH,
        ).wait_recv()

    def small(x, start, depth, s, first):
        piece = bd[:, pl.ds(pl.multiple_of(start, depth), depth)]
        term = dot(piece, x, NT)
        sacc[s] = term if first else sacc[s] + term

    def use_whole(slot, s):
        b = order[slot]
        x = xs[b, s]
        for w in range(4):
            if s == 0:
                weight_copy(w, slot).wait()
            term = dot(x, wbuf[w, slot])
            acc[s, w] = term if slot == 0 else acc[s, w] + term
        small(x, b * kd, kd, s, slot == 0)

    def use(slot, s, ck):
        b = order[slot]
        x = xs[b, s, :, cols(ck)]
        for w in range(4):
            if s == 0 and ck == 0:
                weight_copy(w, slot).wait()
            acc[s, w] += dot(x, wbuf[w, slot, cols(ck), :])
        small(x, b * kd + ck * kc, kc, s, False)

    def forward(d, s, ck):
        arrive(order[2 * d], s, ck)
        fwd_copy(d, s, ck).start()

    def finish_chunk(d, s, ck):
        use(2 * d, s, ck)
        arrive(order[2 * d + 1], s, ck)
        use(2 * d + 1, s, ck)

    def heads_of(w, s):
        return [acc[s, w, :, h * extent : (h + 1) * extent].astype(bf16).astype(f32) for h in range(heads)]

    def owner_of(s, h):
        return (s * heads + h) % g

    def box_copy(s, h):
        return pltpu.make_async_remote_copy(
            src_ref=out_box.at[s, h], dst_ref=in_box.at[s, m],
            send_sem=send1.at[s, h], recv_sem=recv1.at[s, m],
            device_id={"sp": team * g + owner_of(s, h)}, device_id_type=MESH,
        )

    def boxes(s):
        beta = jax.nn.sigmoid(sacc[s, 0:PAD, :] + bias)
        pre = sacc[s, PAD : 2 * PAD, :]
        soft = jnp.maximum(pre, 0.0) + jnp.log1p(jnp.exp(-jnp.abs(pre)))
        upper = jnp.where(row <= col, 1.0, 0.0)
        cum = dot(-jnp.exp(rate) * soft, upper, NN, highest)
        cum_t, beta_t = cum.T, beta.T
        cum_col[s] = cum_t
        causal = row >= col
        strict = row > col
        unit = jnp.where(row == col, 1.0, 0.0)
        hs = range(heads)
        k = [unit_rows(v) for v in heads_of(1, s)]
        kh = [v.astype(bf16) for v in k]
        kk = [dot(v, v, NT) for v in kh]
        low, right, kdec, last = [], [], [], []
        v = heads_of(2, s)
        for h in hs:
            cumc, bt = cum_t[:, h : h + 1], beta_t[:, h : h + 1]
            wts = jnp.where(causal, jnp.exp(jnp.where(causal, cumc - cum[h : h + 1, :], 0.0)), 0.0)
            spread[h] = wts
            kh_buf[h] = kh[h]
            low.append(jnp.where(strict, kk[h] * (bt * wts), 0.0).astype(bf16))
            kb = k[h] * bt
            right.append(jnp.concatenate([v[h] * bt, kb * jnp.exp(cumc)], axis=1).astype(bf16))
            end = cumc[span - 1 :, :]
            kdec.append((k[h] * jnp.exp(end - cumc)).astype(bf16))
            last.append(jnp.exp(end))

        def climb(part, inv, size, ratio):
            if inv is None:
                power = part
                total = [unit - p.astype(f32) for p in part]
            else:
                low_h = [i.astype(bf16) for i in inv]
                power = [dot(i, p).astype(bf16) for i, p in zip(low_h, part)]
                total = [i - dot(p, j) for i, p, j in zip(inv, power, low_h)]
            reached = 2
            while reached < ratio:
                power = [dot(p, p).astype(bf16) for p in power]
                total = [t + dot(p, t.astype(bf16)) for t, p in zip(total, power)]
                reached *= 2
            return total

        inv = climb([p * masks[0] for p in low], None, INNER, INNER)
        inv = climb([p * masks[1] for p in low], inv, OUTER, OUTER // INNER)
        inv_h = [i.astype(bf16) for i in inv]
        power = [dot(i, p * masks[2]).astype(bf16) for i, p in zip(inv_h, low)]
        term = [dot(i, r) for i, r in zip(inv_h, right)]
        uw = term
        for level in range(1, -(-span // OUTER)):
            term = [dot(p, t.astype(bf16)) for p, t in zip(power, term)]
            uw = [u - t if level % 2 else u + t for u, t in zip(uw, term)]
        uw = [u.astype(bf16) for u in uw]
        z = [dot(a, u, TN) for a, u in zip(kdec, uw)]
        eye = lax.broadcasted_iota(jnp.int32, (extent, extent), 0) == lax.broadcasted_iota(
            jnp.int32, (extent, extent), 1
        )
        for h in hs:
            out_box[s, h, 0] = (jnp.where(eye, last[h] - 1.0, 0.0) - z[h][:, extent:]).astype(bf16)
            out_box[s, h, 1] = z[h][:, :extent].astype(bf16)
            uw_buf[h] = uw[h]
        if s == 0:

            @pl.when(me < sn - 1)
            def _():
                pl.semaphore_wait(hello, sn - 1 - me)

        for h in hs:
            own = m == owner_of(s, h)

            @pl.when(own)
            def _():
                in_box[s, m] = out_box[s, h]

            @pl.when(jnp.logical_not(own))
            def _():
                box_copy(s, h).start()

    def queries(s):
        cum_t = cum_col[s]
        gain = gain_ref[...]
        hs = range(heads)
        q = [unit_rows(v) for v in heads_of(0, s)]
        scores = [(dot(q[h].astype(bf16), kh_buf[h], NT) * spread[h]).astype(bf16) for h in hs]
        out = [dot(scores[h], uw_buf[h]) for h in hs]
        gates = heads_of(3, s)
        for h in hs:
            local_out[s, h] = out[h][:, :extent]
            reach[s, h] = (q[h] * jnp.exp(cum_t[:, h : h + 1]) - out[h][:, extent:]).astype(bf16)
            gated[s, h] = gates[h] * jax.nn.sigmoid(gates[h]) * gain

    def own_head(s):
        return lax.rem(m + g - (s * heads) % g, g)

    def back_copy(s, i):
        return pltpu.make_async_remote_copy(
            src_ref=back_out.at[s, i], dst_ref=back_in.at[s, own_head(s)],
            send_sem=send2.at[s, i], recv_sem=recv2.at[s, own_head(s)],
            device_id={"sp": team * g + i}, device_id_type=MESH,
        )

    def mid_copy(s):
        return pltpu.make_async_remote_copy(
            src_ref=mid_out.at[s], dst_ref=mid_in.at[s], send_sem=send3.at[s], recv_sem=recv3.at[s],
            device_id={"sp": lax.rem(me + g, sn)}, device_id_type=MESH,
        )

    def tail_copy(s, j):
        return pltpu.make_async_remote_copy(
            src_ref=tail_out.at[s, j], dst_ref=tail_in.at[s, own_head(s)],
            send_sem=send4.at[s, j], recv_sem=recv4.at[s, own_head(s)],
            device_id={"sp": j}, device_id_type=MESH,
        )

    def box_wait(s, i):
        @pl.when(i != m)
        def _():
            pltpu.make_async_remote_copy(
                src_ref=out_box.at[s, 0], dst_ref=in_box.at[s, i],
                send_sem=send1.at[s, 0], recv_sem=recv1.at[s, i],
                device_id={"sp": team * g + i}, device_id_type=MESH,
            ).wait_recv()

    def give_back(s):
        for i in range(g):

            @pl.when(i == m)
            def _():
                back_in[s, own_head(s)] = back_out[s, i]

            @pl.when(i != m)
            def _():
                back_copy(s, i).start()

    def conclude(s, final):
        memory = final.astype(bf16).astype(f32)
        h = own_head(s)
        shape3 = nq_ref.shape
        mine = (lax.broadcasted_iota(jnp.int32, shape3, 0) == s) & (lax.broadcasted_iota(jnp.int32, shape3, 1) == h)

        def own(ref):
            kept = jnp.where(mine, ref[...].astype(f32), 0.0)
            return jnp.sum(jnp.sum(kept, axis=0), axis=0, keepdims=True)

        qn, kn = unit_rows(own(nq_ref)), unit_rows(own(nk_ref))
        both = jnp.concatenate([jnp.broadcast_to(qn, (PAD, extent)), jnp.broadcast_to(kn, (PAD, extent))], axis=0)
        reads = dot(both, memory, NN, highest)
        recall, retrieve = reads[0:1], reads[PAD : PAD + 1]
        beta_new, decay_new = nb_ref[s, h], nd_ref[s, h]
        fresh = own(nv_ref) - decay_new * retrieve
        meet = jnp.sum(kn * qn, axis=-1, keepdims=True)
        read = decay_new * recall + (beta_new * meet) * fresh
        norm = lax.rsqrt(jnp.mean(read * read, axis=-1, keepdims=True) + norm_floor)
        answer = jnp.broadcast_to(read * norm * gain_ref[...], (PAD, extent))
        for j in range(sn):
            tail_out[s, j, 0:key_rows, :] = memory[j * key_rows : (j + 1) * key_rows]
            tail_out[s, j, tail_out.shape[2] - PAD :, :] = answer

        def push(j, _):
            @pl.when(j == me)
            def _():
                tail_in[s, h] = tail_out[s, me]

            @pl.when(j != me)
            def _():
                tail_copy(s, j).start()

            return 0

        lax.fori_loop(0, sn, push, 0)

    def chain_first(s):
        @pl.when((own_head(s) < heads) & (team == 0))
        def _():
            for i in range(g):
                box_wait(s, i)
            state = jnp.zeros((extent, extent), f32)
            for i in range(g):
                half = state.astype(bf16)
                back_out[s, i] = half
                if i == 0:
                    state = in_box[s, i, 1].astype(f32)
                else:
                    state = state + dot(in_box[s, i, 0], half) + in_box[s, i, 1].astype(f32)
            if groups > 1:
                mid_out[s] = state.astype(bf16)
                mid_copy(s).start()
            give_back(s)
            if groups == 1:
                conclude(s, state)

    def chain_later(s):
        if groups == 1:
            return

        @pl.when((own_head(s) < heads) & (team > 0))
        def _():
            for i in range(g):
                box_wait(s, i)
            shift, drive = [None], [None]
            for i in range(g):
                step, push = in_box[s, i, 0], in_box[s, i, 1].astype(f32)
                if i == 0:
                    shift.append(step.astype(f32))
                    drive.append(push)
                else:
                    shift.append(shift[i] + step.astype(f32) + dot(step, shift[i].astype(bf16)))
                    drive.append(drive[i] + push + dot(step, drive[i].astype(bf16)))
            moves = jnp.concatenate([a.astype(bf16) for a in shift[1:]], axis=0)
            pltpu.make_async_remote_copy(
                src_ref=mid_out.at[s], dst_ref=mid_in.at[s], send_sem=send3.at[s], recv_sem=recv3.at[s],
                device_id={"sp": lax.rem(me + sn - g, sn)}, device_id_type=MESH,
            ).wait_recv()
            start = mid_in[s]
            moved = dot(moves, start)
            base = start.astype(f32)
            back_out[s, 0] = start
            for i in range(1, g):
                back_out[s, i] = (base + moved[(i - 1) * extent : i * extent] + drive[i]).astype(bf16)
            state = base + moved[(g - 1) * extent :] + drive[g]

            @pl.when(team < groups - 1)
            def _():
                mid_out[s] = state.astype(bf16)
                mid_copy(s).start()

            give_back(s)

            @pl.when(team == groups - 1)
            def _():
                conclude(s, state)

    def finish(s):
        for h in range(heads):
            o = owner_of(s, h)

            @pl.when(m != o)
            def _():
                pltpu.make_async_remote_copy(
                    src_ref=back_out.at[s, 0], dst_ref=back_in.at[s, h],
                    send_sem=send2.at[s, 0], recv_sem=recv2.at[s, h],
                    device_id={"sp": team * g + o}, device_id_type=MESH,
                ).wait_recv()

        outs = [local_out[s, h] + dot(reach[s, h], back_in[s, h]) for h in range(heads)]
        for h in range(heads):
            o = outs[h]
            norm = lax.rsqrt(jnp.mean(o * o, axis=-1, keepdims=True) + norm_floor)
            mixed_ref[s * span : (s + 1) * span, h * extent : (h + 1) * extent] = (o * norm * gated[s, h]).astype(bf16)

    def take_tail(s):
        for h in range(heads):
            source = (groups - 1) * g + owner_of(s, h)

            @pl.when(me != source)
            def _():
                pltpu.make_async_remote_copy(
                    src_ref=tail_out.at[s, 0], dst_ref=tail_in.at[s, h],
                    send_sem=send4.at[s, 0], recv_sem=recv4.at[s, h],
                    device_id={"sp": source}, device_id_type=MESH,
                ).wait_recv()

            p = s * heads + h
            cache_ref[p] = tail_in[s, h, 0:key_rows, :].astype(bf16)
            edge = tail_in.shape[2] - PAD
            first_ref[s : s + 1, h * extent : (h + 1) * extent] = tail_in[s, h, edge : edge + 1, :]

    for s in range(seqs):
        use_whole(0, s)
    for s in range(seqs):
        pltpu.make_async_remote_copy(
            src_ref=xs.at[partner, s], dst_ref=xs.at[partner, s], send_sem=part_sem.at[s], recv_sem=prx.at[s],
            device_id={"tp": partner}, device_id_type=MESH,
        ).wait_recv()
        use_whole(1, s)

    for s in range(seqs):
        for ck in range(chunks):
            for d in range(1, chips):
                if s == 0 or ck > 0:
                    forward(d, s, ck)
                if s > 0 and ck == chunks - 1 and d == chips - 1:
                    chain_first(s - 1)
                finish_chunk(d, s, ck)
        boxes(s)
        if s > 0:
            chain_later(s - 1)
        if s < seqs - 1:
            for d in range(1, chips):
                forward(d, s + 1, 0)
        queries(s)
    for s in range(seqs - 1):
        finish(s)
    chain_first(seqs - 1)
    chain_later(seqs - 1)
    finish(seqs - 1)
    for s in range(seqs):
        take_tail(s)

    for s in range(seqs):
        part_copy(s).wait_send()
        for ck in range(chunks):
            for d in range(1, chips):
                cross_copy(d, s, ck).wait_send()
                fwd_copy(d, s, ck).wait_send()
        for h in range(heads):

            @pl.when(m != owner_of(s, h))
            def _():
                box_copy(s, h).wait_send()

        @pl.when(own_head(s) < heads)
        def _():
            for i in range(g):

                @pl.when(i != m)
                def _():
                    back_copy(s, i).wait_send()

            @pl.when(team < groups - 1)
            def _():
                mid_copy(s).wait_send()

            @pl.when(team == groups - 1)
            def _():
                for j in range(sn):

                    @pl.when(j != me)
                    def _():
                        tail_copy(s, j).wait_send()


def fused(tn, sn, seqs, heads, tokens, weights, bw, dw, bias, rate, gain, nq, nk, nv, nb, nd):
    rows, kd = tokens.shape
    width = weights[0].shape[1]
    kc = 256 if kd % 256 == 0 else kd
    chunks, chips, span = kd // kc, tn // 2, rows // seqs
    extent = width // heads
    pairs, key_rows = seqs * heads, extent // sn
    tail = -(-key_rows // PAD) * PAD + PAD
    g = group_of(sn, heads)
    operands = (tokens, *weights, bw, dw, bias, rate, gain, nq, nk, nv, nb, nd)
    vmem = pl.BlockSpec(memory_space=pltpu.VMEM)
    smem = pl.BlockSpec(memory_space=pltpu.SMEM)
    hbm = pl.BlockSpec(memory_space=pltpu.HBM)
    dma = pltpu.SemaphoreType.DMA
    return pl.pallas_call(
        functools.partial(fused_kernel, tn, sn, seqs, heads),
        out_shape=(
            jax.ShapeDtypeStruct((rows, width), bf16),
            jax.ShapeDtypeStruct((pairs, key_rows, extent), bf16),
            jax.ShapeDtypeStruct((seqs, width), f32),
        ),
        in_specs=[hbm] * 5 + [vmem] * 2 + [smem] * 2 + [vmem] * 4 + [smem] * 2,
        out_specs=(vmem,) * 3,
        scratch_shapes=[
            pltpu.VMEM((2 * PAD, bw.shape[1]), bf16),
            pltpu.VMEM((tn, seqs, span, kd), bf16),
            pltpu.VMEM((4, tn, kd, width), bf16),
            pltpu.VMEM((seqs, 4, span, width), f32),
            pltpu.VMEM((seqs, 2 * PAD, span), f32),
            pltpu.VMEM((3, span, span), bf16),
            pltpu.VMEM((seqs, span, PAD), f32),
            pltpu.VMEM((heads, span, extent), bf16),
            pltpu.VMEM((heads, span, span), f32),
            pltpu.VMEM((heads, span, 2 * extent), bf16),
            pltpu.VMEM((seqs, heads, span, extent), f32),
            pltpu.VMEM((seqs, heads, span, extent), bf16),
            pltpu.VMEM((seqs, heads, span, extent), f32),
            pltpu.VMEM((seqs, heads, 2, extent, extent), bf16),
            pltpu.VMEM((seqs, g, 2, extent, extent), bf16),
            pltpu.VMEM((seqs, extent, extent), bf16),
            pltpu.VMEM((seqs, extent, extent), bf16),
            pltpu.VMEM((seqs, g, extent, extent), bf16),
            pltpu.VMEM((seqs, heads, extent, extent), bf16),
            pltpu.VMEM((seqs, sn, tail, extent), f32),
            pltpu.VMEM((seqs, heads, tail, extent), f32),
            dma((seqs,)),
            dma((4, tn)),
            dma((chips - 1, seqs, chunks)),
            dma((seqs,)),
            dma((chips - 1, seqs, chunks)),
            dma((tn, seqs, chunks)),
            dma((seqs,)),
            dma((seqs, heads)),
            dma((seqs, g)),
            dma((seqs, g)),
            dma((seqs, heads)),
            dma((seqs,)),
            dma((seqs,)),
            dma((seqs, sn)),
            dma((seqs, heads)),
            pltpu.SemaphoreType.REGULAR,
        ],
        compiler_params=pltpu.CompilerParams(
            collective_id=0, has_side_effects=True, vmem_limit_bytes=53 * 1024 * 1024
        ),
    )(*[pltpu.with_memory_space_constraint(a, pltpu.HBM) for a in operands])


def emit_kernel(mixed_ref, cache_ref, first_ref, mixed_out, cache_out, first_out, sem):
    copies = [
        pltpu.make_async_copy(a, b, sem.at[i])
        for i, (a, b) in enumerate(((mixed_ref, mixed_out), (cache_ref, cache_out), (first_ref, first_out)))
    ]
    for copy in copies:
        copy.start()
    for copy in copies:
        copy.wait()


def emit(*results):
    return pl.pallas_call(
        emit_kernel,
        out_shape=tuple(jax.ShapeDtypeStruct(r.shape, r.dtype) for r in results),
        in_specs=[pl.BlockSpec(memory_space=pltpu.VMEM)] * 3,
        out_specs=(pl.BlockSpec(memory_space=pltpu.HBM),) * 3,
        scratch_shapes=[pltpu.SemaphoreType.DMA((3,))],
        compiler_params=pltpu.CompilerParams(vmem_limit_bytes=4 * 1024 * 1024),
    )(*results)


def shards(
    tokens, query_weight, key_weight, value_weight, gate_weight, beta_weight, decay_weight,
    beta_bias, rate_log, out_gain, new_query, new_key, new_value, new_beta, new_decay,
):
    seqs, span, kd = tokens.shape
    heads = rate_log.shape[0]
    extent = out_gain.shape[0]
    tp, sp = lax.axis_size("tp"), lax.axis_size("sp")
    weights = (query_weight, key_weight, value_weight, gate_weight)
    mixed, cache, first = fused(
        tp, sp, seqs, heads, tokens.reshape(seqs * span, kd), weights, beta_weight.T, decay_weight.T, beta_bias,
        rate_log, out_gain[None], new_query, new_key, new_value, new_beta, new_decay,
    )
    return emit(
        mixed.reshape(seqs, span, heads * extent), cache.reshape(seqs, heads, extent // sp, extent), first
    )


def solution(mesh):
    placed = (
        P(None, "sp", "tp"),
        P(None, "tp"),
        P(None, "tp"),
        P(None, "tp"),
        P(None, "tp"),
        P(None, "tp"),
        P(None, "tp"),
        P("tp"),
        P("tp"),
        P(),
        P(None, "tp", None),
        P(None, "tp", None),
        P(None, "tp", None),
        P(None, "tp"),
        P(None, "tp"),
    )
    return jax.shard_map(
        shards,
        mesh=mesh,
        in_specs=placed,
        out_specs=(P(None, "sp", "tp"), P(None, "tp", "sp", None), P(None, "tp")),
        check_vma=False,
    )
```

```python
import functools

import jax
import jax.numpy as jnp
from jax import lax
from jax.experimental import pallas as pl
from jax.experimental.pallas import tpu as pltpu
from jax.sharding import PartitionSpec as P

unit_floor = 1.0
norm_floor = 0.001
highest = lax.Precision.HIGHEST
MESH = pl.DeviceIdType.MESH
PAD = 8
INNER, OUTER = 8, 64
f32 = jnp.float32
bf16 = jnp.bfloat16

NN = (((1,), (0,)), ((), ()))
NT = (((1,), (1,)), ((), ()))
TN = (((0,), (0,)), ((), ()))


def dot(left, right, dims=NN, precision=None):
    return lax.dot_general(left, right, dims, precision=precision, preferred_element_type=f32)


def unit_rows(values):
    return values * lax.rsqrt(jnp.sum(values * values, axis=-1, keepdims=True) + unit_floor)


def group_of(n, heads):
    g = 1
    while g < n and (g < heads or g * g < n):
        g *= 2
    return g


def fused_kernel(
    tn, sn, seqs, heads, x_ref, wq_ref, wk_ref, wv_ref, wg_ref, bw_hbm, dw_hbm, bias_hbm, rate_hbm, gain_hbm,
    nq_hbm, nk_hbm, nv_hbm, nb_hbm, nd_hbm, mixed_ref, cache_ref, first_ref,
    bw_ref, dw_ref, bias_ref, rate_ref, gain_ref, nq_ref, nk_ref, nv_ref, nb_ref, nd_ref, small_sem,
    bd, xs, wbuf, acc, sacc, cum_row, cum_col, kh_buf, uw_buf, local_out, reach, gated,
    out_box, in_box, mid_out, mid_in, back_out, back_in, tail_out, tail_in, word_out, word_in,
    xsem, wsem, cross_sem, part_sem, fwd_sem, rx, prx,
    send1, recv1, send2, recv2, send3, recv3, send4, recv4, send5, recv5, hello,
):
    _, _, span, kd = xs.shape
    width = wq_ref.shape[1]
    extent = width // heads
    key_rows = extent // sn
    chunks = rx.shape[2]
    kc = kd // chunks
    tme, me = lax.axis_index("tp"), lax.axis_index("sp")
    y, c = tme // 2, lax.rem(tme, 2)
    chips = tn // 2
    partner = y * 2 + (1 - c)
    g = group_of(sn, heads)
    groups = sn // g
    team, m = me // g, lax.rem(me, g)
    weights = (wq_ref, wk_ref, wv_ref, wg_ref)

    barrier = pltpu.get_barrier_semaphore()
    pl.semaphore_signal(barrier, inc=1, device_id={"tp": partner}, device_id_type=MESH)
    for d in range(1, chips):
        to = lax.rem(y + d, chips) * 2 + c
        pl.semaphore_signal(barrier, inc=1, device_id={"tp": to}, device_id_type=MESH)
    for d in range(1, sn):

        @pl.when(me + d < sn)
        def _():
            pl.semaphore_signal(barrier, inc=1, device_id={"sp": me + d}, device_id_type=MESH)

    order = [tme, partner]
    for d in range(1, chips):
        source = lax.rem(y - d + chips, chips)
        order += [source * 2 + c, source * 2 + (1 - c)]

    def cols(ck):
        return pl.ds(ck * kc, kc)

    def token_copy(s):
        return pltpu.make_async_copy(x_ref.at[pl.ds(s * span, span), :], xs.at[tme, s], xsem.at[s])

    def weight_copy(w, slot):
        start = pl.multiple_of(order[slot] * kd, kd)
        return pltpu.make_async_copy(
            weights[w].at[pl.ds(start, kd), :], wbuf.at[w, slot], wsem.at[w, slot]
        )

    small_copies = [
        pltpu.make_async_copy(a, b, small_sem.at[i])
        for i, (a, b) in enumerate(
            (
                (bw_hbm, bw_ref), (dw_hbm, dw_ref), (bias_hbm, bias_ref), (rate_hbm, rate_ref), (gain_hbm, gain_ref),
                (nq_hbm, nq_ref), (nk_hbm, nk_ref), (nv_hbm, nv_ref), (nb_hbm, nb_ref), (nd_hbm, nd_ref),
            )
        )
    ]
    for s in range(seqs):
        token_copy(s).start()
    for copy in small_copies:
        copy.start()
    pl.semaphore_wait(barrier, chips + me)

    def cross_copy(d, s, ck):
        to = lax.rem(y + d, chips) * 2 + c
        return pltpu.make_async_remote_copy(
            src_ref=xs.at[tme, s, :, cols(ck)], dst_ref=xs.at[tme, s, :, cols(ck)],
            send_sem=cross_sem.at[d - 1, s, ck], recv_sem=rx.at[tme, s, ck],
            device_id={"tp": to}, device_id_type=MESH,
        )

    def part_copy(s):
        return pltpu.make_async_remote_copy(
            src_ref=xs.at[tme, s], dst_ref=xs.at[tme, s],
            send_sem=part_sem.at[s], recv_sem=prx.at[s],
            device_id={"tp": partner}, device_id_type=MESH,
        )

    for s in range(seqs):
        token_copy(s).wait()
        for ck in range(chunks):
            for d in range(1, chips):
                cross_copy(d, s, ck).start()
        part_copy(s).start()
    for slot in range(tn):
        for w in range(4):
            weight_copy(w, slot).start()
    for d in range(1, sn):

        @pl.when(me >= d)
        def _():
            pl.semaphore_signal(hello, inc=1, device_id={"sp": me - d}, device_id_type=MESH)

    for copy in small_copies:
        copy.wait()
    bd[...] = jnp.zeros_like(bd)
    bd[0 : bw_ref.shape[0]] = bw_ref[...]
    bd[PAD : PAD + dw_ref.shape[0]] = dw_ref[...]
    row = lax.broadcasted_iota(jnp.int32, (span, span), 0)
    col = lax.broadcasted_iota(jnp.int32, (span, span), 1)
    slot_of = lax.broadcasted_iota(jnp.int32, (PAD, 1), 0)
    bias = jnp.zeros((PAD, 1), f32)
    rate = jnp.zeros((PAD, 1), f32)
    for h in range(heads):
        bias = jnp.where(slot_of == h, bias_ref[h], bias)
        rate = jnp.where(slot_of == h, rate_ref[h], rate)

    def fwd_copy(d, s, ck):
        b = order[2 * d]
        return pltpu.make_async_remote_copy(
            src_ref=xs.at[b, s, :, cols(ck)], dst_ref=xs.at[b, s, :, cols(ck)],
            send_sem=fwd_sem.at[d - 1, s, ck], recv_sem=rx.at[b, s, ck],
            device_id={"tp": partner}, device_id_type=MESH,
        )

    def arrive(b, s, ck):
        pltpu.make_async_remote_copy(
            src_ref=xs.at[b, s, :, cols(ck)], dst_ref=xs.at[b, s, :, cols(ck)],
            send_sem=part_sem.at[0], recv_sem=rx.at[b, s, ck],
            device_id={"tp": partner}, device_id_type=MESH,
        ).wait_recv()

    def small(x, start, depth, s, first):
        piece = bd[:, pl.ds(pl.multiple_of(start, depth), depth)]
        term = dot(piece, x, NT)
        sacc[s] = term if first else sacc[s] + term

    def use_whole(slot, s):
        b = order[slot]
        x = xs[b, s]
        for w in range(4):
            if s == 0:
                weight_copy(w, slot).wait()
            term = dot(x, wbuf[w, slot])
            acc[s, w] = term if slot == 0 else acc[s, w] + term
        small(x, b * kd, kd, s, slot == 0)

    def use(slot, s, ck):
        b = order[slot]
        x = xs[b, s, :, cols(ck)]
        for w in range(4):
            if s == 0 and ck == 0:
                weight_copy(w, slot).wait()
            acc[s, w] += dot(x, wbuf[w, slot, cols(ck), :])
        small(x, b * kd + ck * kc, kc, s, False)

    def forward(d, s, ck):
        arrive(order[2 * d], s, ck)
        fwd_copy(d, s, ck).start()

    def finish_chunk(d, s, ck):
        use(2 * d, s, ck)
        arrive(order[2 * d + 1], s, ck)
        use(2 * d + 1, s, ck)

    def heads_of(w, s):
        return [acc[s, w, :, h * extent : (h + 1) * extent].astype(bf16).astype(f32) for h in range(heads)]

    def owner_of(s, h):
        return (s * heads + h) % g

    def box_copy(s, h):
        return pltpu.make_async_remote_copy(
            src_ref=out_box.at[s, h], dst_ref=in_box.at[s, m],
            send_sem=send1.at[s, h], recv_sem=recv1.at[s, m],
            device_id={"sp": team * g + owner_of(s, h)}, device_id_type=MESH,
        )

    def boxes(s):
        beta = jax.nn.sigmoid(sacc[s, 0:PAD, :] + bias)
        pre = sacc[s, PAD : 2 * PAD, :]
        soft = jnp.maximum(pre, 0.0) + jnp.log1p(jnp.exp(-jnp.abs(pre)))
        upper = jnp.where(row <= col, 1.0, 0.0)
        cum = dot(-jnp.exp(rate) * soft, upper, NN, highest)
        cum_t, beta_t = cum.T, beta.T
        cum_row[s] = cum
        cum_col[s] = cum_t
        hs, bs = range(heads), range(span // OUTER)
        line = lax.broadcasted_iota(jnp.int32, (OUTER, 2 * OUTER), 0)
        lane = lax.broadcasted_iota(jnp.int32, (OUTER, 2 * OUTER), 1)
        high = lane >= OUTER
        place = lane % OUTER
        same = line // INNER == place // INNER
        fill = jnp.zeros((OUTER, 2 * OUTER), bf16)
        unit = jnp.where(line == place, 1.0, 0.0)

        def part(b):
            return slice(b * OUTER, (b + 1) * OUTER)

        twice = [jnp.concatenate([cum[:, part(b)]] * 2, axis=1) for b in bs]
        k = [unit_rows(v) for v in heads_of(1, s)]
        kh = [v.astype(bf16) for v in k]
        pairs = [(h, b) for h in hs for b in bs]
        kk = [dot(kh[h][part(b)], jnp.concatenate([kh[h][part(b)]] * 2, axis=0), NT) for h, b in pairs]
        far = {(h, b): dot(kh[h][part(b)], kh[h][: b * OUTER], NT) for h, b in pairs if b > 0}
        right, kdec, last, low = [], [], [], []
        v = heads_of(2, s)
        for h in hs:
            cumc, bt = cum_t[:, h : h + 1], beta_t[:, h : h + 1]
            kh_buf[h] = kh[h]
            for b in bs:
                here = cumc[part(b)]
                wts = bt[part(b)] * jnp.exp(jnp.where(line >= place, here - twice[b][h : h + 1, :], 0.0))
                low.append(jnp.where(line > place, kk[h * len(bs) + b] * wts, 0.0))
                if b > 0:
                    wts = bt[part(b)] * jnp.exp(here - cum[h : h + 1, : b * OUTER])
                    far[h, b] = (far[h, b] * wts).astype(bf16)
            kb = k[h] * bt
            right.append(jnp.concatenate([v[h] * bt, kb * jnp.exp(cumc)], axis=1).astype(bf16))
            end = cumc[span - 1 :, :]
            kdec.append((k[h] * jnp.exp(end - cumc)).astype(bf16))
            last.append(jnp.exp(end))

        def climb(block):
            half = block.astype(bf16)
            return dot(half[:, :OUTER], half)

        z = [jnp.where(high, unit - n, n) for n in (jnp.where(same, m, 0.0) for m in low)]
        z = [jnp.where(high, a, climb(a)) for a in z]
        reached = 2
        while reached < INNER:
            z = [climb(a) + jnp.where(high, a, 0.0) for a in z]
            reached *= 2
        under = [jnp.concatenate([fill, jnp.where(high | same, 0.0, m).astype(bf16)], axis=0) for m in low]
        z = [a + dot(a.astype(bf16), u) for a, u in zip(z, under)]
        z = [jnp.where(high, a - t, t) for a, t in ((a, climb(a)) for a in z)]
        reached = 2
        while reached < OUTER // INNER:
            z = [climb(a) + jnp.where(high, a, 0.0) for a in z]
            reached *= 2
        inv = {p: a.astype(bf16) for p, a in zip(pairs, z)}
        none = jnp.zeros((OUTER, 2 * extent), bf16)
        term = {(h, b): dot(inv[h, b], jnp.concatenate([none, right[h][part(b)]], axis=0)) for h, b in pairs}
        far = {
            (h, b): dot(inv[h, b], jnp.concatenate([jnp.zeros_like(m), m], axis=0)).astype(bf16)
            for (h, b), m in far.items()
        }
        done = [[term[h, 0].astype(bf16)] for h in hs]
        for b in bs[1:]:
            for h in hs:
                seen = jnp.concatenate(done[h], axis=0) if b > 1 else done[h][0]
                done[h].append((term[h, b] - dot(far[h, b], seen)).astype(bf16))
        uw = [jnp.concatenate(d, axis=0) for d in done]
        z = [dot(a, u, TN) for a, u in zip(kdec, uw)]
        eye = lax.broadcasted_iota(jnp.int32, (extent, extent), 0) == lax.broadcasted_iota(
            jnp.int32, (extent, extent), 1
        )
        for h in hs:
            out_box[s, h, 0] = (jnp.where(eye, last[h] - 1.0, 0.0) - z[h][:, extent:]).astype(bf16)
            out_box[s, h, 1] = z[h][:, :extent].astype(bf16)
            uw_buf[h] = uw[h]
        if s == 0:

            @pl.when(me < sn - 1)
            def _():
                pl.semaphore_wait(hello, sn - 1 - me)

        for h in hs:
            own = m == owner_of(s, h)

            @pl.when(own)
            def _():
                in_box[s, m] = out_box[s, h]

            @pl.when(jnp.logical_not(own))
            def _():
                box_copy(s, h).start()

    def queries(s):
        cum, cum_t = cum_row[s], cum_col[s]
        gain = gain_ref[...]
        hs = range(heads)
        causal = row >= col

        def spread(h):
            gap = jnp.where(causal, cum_t[:, h : h + 1] - cum[h : h + 1, :], 0.0)
            return jnp.where(causal, jnp.exp(gap), 0.0)

        q = [unit_rows(v) for v in heads_of(0, s)]
        scores = [(dot(q[h].astype(bf16), kh_buf[h], NT) * spread(h)).astype(bf16) for h in hs]
        out = [dot(scores[h], uw_buf[h]) for h in hs]
        gates = heads_of(3, s)
        for h in hs:
            local_out[s, h] = out[h][:, :extent]
            reach[s, h] = (q[h] * jnp.exp(cum_t[:, h : h + 1]) - out[h][:, extent:]).astype(bf16)
            gated[s, h] = gates[h] * jax.nn.sigmoid(gates[h]) * gain

    def own_head(s):
        return lax.rem(m + g - (s * heads) % g, g)

    def back_copy(s, i):
        return pltpu.make_async_remote_copy(
            src_ref=back_out.at[s, i], dst_ref=back_in.at[s, own_head(s)],
            send_sem=send2.at[s, i], recv_sem=recv2.at[s, own_head(s)],
            device_id={"sp": team * g + i}, device_id_type=MESH,
        )

    def mid_copy(s):
        return pltpu.make_async_remote_copy(
            src_ref=mid_out.at[s], dst_ref=mid_in.at[s], send_sem=send3.at[s], recv_sem=recv3.at[s],
            device_id={"sp": lax.rem(me + g, sn)}, device_id_type=MESH,
        )

    def tail_copies(s, j):
        h = own_head(s)
        return (
            pltpu.make_async_remote_copy(
                src_ref=tail_out.at[s, j], dst_ref=tail_in.at[s, h], send_sem=send4.at[s, j], recv_sem=recv4.at[s, h],
                device_id={"sp": j}, device_id_type=MESH,
            ),
            pltpu.make_async_remote_copy(
                src_ref=word_out.at[s], dst_ref=word_in.at[s, h], send_sem=send5.at[s, j], recv_sem=recv5.at[s, h],
                device_id={"sp": j}, device_id_type=MESH,
            ),
        )

    def box_wait(s, i):
        @pl.when(i != m)
        def _():
            pltpu.make_async_remote_copy(
                src_ref=out_box.at[s, 0], dst_ref=in_box.at[s, i],
                send_sem=send1.at[s, 0], recv_sem=recv1.at[s, i],
                device_id={"sp": team * g + i}, device_id_type=MESH,
            ).wait_recv()

    def give_back(s):
        for i in range(g):

            @pl.when(i == m)
            def _():
                back_in[s, own_head(s)] = back_out[s, i]

            @pl.when(i != m)
            def _():
                back_copy(s, i).start()

    def conclude(s, final):
        kept_h = final.astype(bf16)
        memory = kept_h.astype(f32)
        h = own_head(s)
        for j in range(sn):
            tail_out[s, j] = kept_h[j * key_rows : (j + 1) * key_rows]
        shape3 = nq_ref.shape
        mine = (lax.broadcasted_iota(jnp.int32, shape3, 0) == s) & (lax.broadcasted_iota(jnp.int32, shape3, 1) == h)

        def own(ref):
            kept = jnp.where(mine, ref[...].astype(f32), 0.0)
            return jnp.sum(jnp.sum(kept, axis=0), axis=0, keepdims=True)

        qn, kn = unit_rows(own(nq_ref)), unit_rows(own(nk_ref))
        both = jnp.concatenate([jnp.broadcast_to(qn, (PAD, extent)), jnp.broadcast_to(kn, (PAD, extent))], axis=0)
        reads = dot(both, memory, NN, highest)
        recall, retrieve = reads[0:1], reads[PAD : PAD + 1]
        beta_new, decay_new = nb_ref[s, h], nd_ref[s, h]
        fresh = own(nv_ref) - decay_new * retrieve
        meet = jnp.sum(kn * qn, axis=-1, keepdims=True)
        read = decay_new * recall + (beta_new * meet) * fresh
        norm = lax.rsqrt(jnp.mean(read * read, axis=-1, keepdims=True) + norm_floor)
        word_out[s] = read * norm * gain_ref[...]
        for j in range(sn):

            @pl.when(j == me)
            def _():
                tail_in[s, h] = tail_out[s, j]
                word_in[s, h] = word_out[s]

            @pl.when(j != me)
            def _():
                for copy in tail_copies(s, j):
                    copy.start()

    def chain_first(s):
        @pl.when((own_head(s) < heads) & (team == 0))
        def _():
            for i in range(g):
                box_wait(s, i)
            state = jnp.zeros((extent, extent), f32)
            for i in range(g):
                half = state.astype(bf16)
                back_out[s, i] = half
                if i == 0:
                    state = in_box[s, i, 1].astype(f32)
                else:
                    state = state + dot(in_box[s, i, 0], half) + in_box[s, i, 1].astype(f32)
            if groups > 1:
                mid_out[s] = state.astype(bf16)
                mid_copy(s).start()
            if groups == 1:
                conclude(s, state)
            give_back(s)

    def chain_later(s):
        if groups == 1:
            return

        @pl.when((own_head(s) < heads) & (team > 0))
        def _():
            for i in range(g):
                box_wait(s, i)
            shift, drive = [None], [None]
            for i in range(g):
                step, push = in_box[s, i, 0], in_box[s, i, 1].astype(f32)
                if i == 0:
                    shift.append(step.astype(f32))
                    drive.append(push)
                else:
                    shift.append(shift[i] + step.astype(f32) + dot(step, shift[i].astype(bf16)))
                    drive.append(drive[i] + push + dot(step, drive[i].astype(bf16)))
            moves = jnp.concatenate([a.astype(bf16) for a in shift[1:]], axis=0)
            pltpu.make_async_remote_copy(
                src_ref=mid_out.at[s], dst_ref=mid_in.at[s], send_sem=send3.at[s], recv_sem=recv3.at[s],
                device_id={"sp": lax.rem(me + sn - g, sn)}, device_id_type=MESH,
            ).wait_recv()
            start = mid_in[s]
            moved = dot(moves, start)
            base = start.astype(f32)
            back_out[s, 0] = start
            for i in range(1, g):
                back_out[s, i] = (base + moved[(i - 1) * extent : i * extent] + drive[i]).astype(bf16)
            state = base + moved[(g - 1) * extent :] + drive[g]

            @pl.when(team < groups - 1)
            def _():
                mid_out[s] = state.astype(bf16)
                mid_copy(s).start()

            @pl.when(team == groups - 1)
            def _():
                conclude(s, state)

            give_back(s)

    def finish(s):
        for h in range(heads):
            o = owner_of(s, h)

            @pl.when(m != o)
            def _():
                pltpu.make_async_remote_copy(
                    src_ref=back_out.at[s, 0], dst_ref=back_in.at[s, h],
                    send_sem=send2.at[s, 0], recv_sem=recv2.at[s, h],
                    device_id={"sp": team * g + o}, device_id_type=MESH,
                ).wait_recv()

        outs = [local_out[s, h] + dot(reach[s, h], back_in[s, h]) for h in range(heads)]
        for h in range(heads):
            o = outs[h]
            norm = lax.rsqrt(jnp.mean(o * o, axis=-1, keepdims=True) + norm_floor)
            mixed_ref[s * span : (s + 1) * span, h * extent : (h + 1) * extent] = (o * norm * gated[s, h]).astype(bf16)

    def take_tail(s):
        for h in range(heads):
            source = (groups - 1) * g + owner_of(s, h)

            @pl.when(me != source)
            def _():
                pltpu.make_async_remote_copy(
                    src_ref=tail_out.at[s, 0], dst_ref=tail_in.at[s, h],
                    send_sem=send4.at[s, 0], recv_sem=recv4.at[s, h],
                    device_id={"sp": source}, device_id_type=MESH,
                ).wait_recv()
                pltpu.make_async_remote_copy(
                    src_ref=word_out.at[s], dst_ref=word_in.at[s, h],
                    send_sem=send5.at[s, 0], recv_sem=recv5.at[s, h],
                    device_id={"sp": source}, device_id_type=MESH,
                ).wait_recv()

            cache_ref[s * heads + h] = tail_in[s, h]
            first_ref[s : s + 1, h * extent : (h + 1) * extent] = word_in[s, h]

    for s in range(seqs):
        use_whole(0, s)
    for s in range(seqs):
        pltpu.make_async_remote_copy(
            src_ref=xs.at[partner, s], dst_ref=xs.at[partner, s], send_sem=part_sem.at[s], recv_sem=prx.at[s],
            device_id={"tp": partner}, device_id_type=MESH,
        ).wait_recv()
        use_whole(1, s)

    for s in range(seqs):
        for ck in range(chunks):
            for d in range(1, chips):
                if s == 0 or ck > 0:
                    forward(d, s, ck)
                if s > 0 and ck == chunks - 1 and d == chips - 1:
                    chain_first(s - 1)
                finish_chunk(d, s, ck)
        boxes(s)
        if s > 0:
            chain_later(s - 1)
        if s < seqs - 1:
            for d in range(1, chips):
                forward(d, s + 1, 0)
        queries(s)
    for s in range(seqs - 1):
        finish(s)
    chain_first(seqs - 1)
    chain_later(seqs - 1)
    finish(seqs - 1)
    for s in range(seqs):
        part_copy(s).wait_send()
        for ck in range(chunks):
            for d in range(1, chips):
                cross_copy(d, s, ck).wait_send()
                fwd_copy(d, s, ck).wait_send()
        for h in range(heads):

            @pl.when(m != owner_of(s, h))
            def _():
                box_copy(s, h).wait_send()

        @pl.when(own_head(s) < heads)
        def _():
            for i in range(g):

                @pl.when(i != m)
                def _():
                    back_copy(s, i).wait_send()

            @pl.when(team < groups - 1)
            def _():
                mid_copy(s).wait_send()

            @pl.when(team == groups - 1)
            def _():
                for j in range(sn):

                    @pl.when(j != me)
                    def _():
                        for copy in tail_copies(s, j):
                            copy.wait_send()

    for s in range(seqs):
        take_tail(s)


def fused(tn, sn, seqs, heads, tokens, weights, bw, dw, bias, rate, gain, nq, nk, nv, nb, nd):
    rows, kd = tokens.shape
    width = weights[0].shape[1]
    kc = 256 if kd % 256 == 0 else kd
    chunks, chips, span = kd // kc, tn // 2, rows // seqs
    extent = width // heads
    pairs, key_rows = seqs * heads, extent // sn
    g = group_of(sn, heads)
    operands = (tokens, *weights, bw, dw, bias, rate, gain, nq, nk, nv, nb, nd)
    vmem = pl.BlockSpec(memory_space=pltpu.VMEM)
    hbm = pl.BlockSpec(memory_space=pltpu.HBM)
    dma = pltpu.SemaphoreType.DMA
    return pl.pallas_call(
        functools.partial(fused_kernel, tn, sn, seqs, heads),
        out_shape=(
            jax.ShapeDtypeStruct((rows, width), bf16),
            jax.ShapeDtypeStruct((pairs, key_rows, extent), bf16),
            jax.ShapeDtypeStruct((seqs, width), f32),
        ),
        in_specs=[hbm] * 15,
        out_specs=(vmem,) * 3,
        scratch_shapes=[
            pltpu.VMEM(bw.shape, bf16),
            pltpu.VMEM(dw.shape, bf16),
            pltpu.SMEM(bias.shape, f32),
            pltpu.SMEM(rate.shape, f32),
            pltpu.VMEM(gain.shape, f32),
            pltpu.VMEM(nq.shape, bf16),
            pltpu.VMEM(nk.shape, bf16),
            pltpu.VMEM(nv.shape, bf16),
            pltpu.SMEM(nb.shape, f32),
            pltpu.SMEM(nd.shape, f32),
            dma((10,)),
            pltpu.VMEM((2 * PAD, bw.shape[1]), bf16),
            pltpu.VMEM((tn, seqs, span, kd), bf16),
            pltpu.VMEM((4, tn, kd, width), bf16),
            pltpu.VMEM((seqs, 4, span, width), f32),
            pltpu.VMEM((seqs, 2 * PAD, span), f32),
            pltpu.VMEM((seqs, PAD, span), f32),
            pltpu.VMEM((seqs, span, PAD), f32),
            pltpu.VMEM((heads, span, extent), bf16),
            pltpu.VMEM((heads, span, 2 * extent), bf16),
            pltpu.VMEM((seqs, heads, span, extent), f32),
            pltpu.VMEM((seqs, heads, span, extent), bf16),
            pltpu.VMEM((seqs, heads, span, extent), f32),
            pltpu.VMEM((seqs, heads, 2, extent, extent), bf16),
            pltpu.VMEM((seqs, g, 2, extent, extent), bf16),
            pltpu.VMEM((seqs, extent, extent), bf16),
            pltpu.VMEM((seqs, extent, extent), bf16),
            pltpu.VMEM((seqs, g, extent, extent), bf16),
            pltpu.VMEM((seqs, heads, extent, extent), bf16),
            pltpu.VMEM((seqs, sn, key_rows, extent), bf16),
            pltpu.VMEM((seqs, heads, key_rows, extent), bf16),
            pltpu.VMEM((seqs, 1, extent), f32),
            pltpu.VMEM((seqs, heads, 1, extent), f32),
            dma((seqs,)),
            dma((4, tn)),
            dma((chips - 1, seqs, chunks)),
            dma((seqs,)),
            dma((chips - 1, seqs, chunks)),
            dma((tn, seqs, chunks)),
            dma((seqs,)),
            dma((seqs, heads)),
            dma((seqs, g)),
            dma((seqs, g)),
            dma((seqs, heads)),
            dma((seqs,)),
            dma((seqs,)),
            dma((seqs, sn)),
            dma((seqs, heads)),
            dma((seqs, sn)),
            dma((seqs, heads)),
            pltpu.SemaphoreType.REGULAR,
        ],
        compiler_params=pltpu.CompilerParams(
            collective_id=0, has_side_effects=True, vmem_limit_bytes=53 * 1024 * 1024
        ),
    )(*[pltpu.with_memory_space_constraint(a, pltpu.HBM) for a in operands])


def emit_kernel(mixed_ref, cache_ref, first_ref, mixed_out, cache_out, first_out, sem):
    copies = [
        pltpu.make_async_copy(a, b, sem.at[i])
        for i, (a, b) in enumerate(((mixed_ref, mixed_out), (cache_ref, cache_out), (first_ref, first_out)))
    ]
    for copy in copies:
        copy.start()
    for copy in copies:
        copy.wait()


def emit(*results):
    return pl.pallas_call(
        emit_kernel,
        out_shape=tuple(jax.ShapeDtypeStruct(r.shape, r.dtype) for r in results),
        in_specs=[pl.BlockSpec(memory_space=pltpu.VMEM)] * 3,
        out_specs=(pl.BlockSpec(memory_space=pltpu.HBM),) * 3,
        scratch_shapes=[pltpu.SemaphoreType.DMA((3,))],
        compiler_params=pltpu.CompilerParams(vmem_limit_bytes=4 * 1024 * 1024),
    )(*results)


def shards(
    tokens, query_weight, key_weight, value_weight, gate_weight, beta_weight, decay_weight,
    beta_bias, rate_log, out_gain, new_query, new_key, new_value, new_beta, new_decay,
):
    seqs, span, kd = tokens.shape
    heads = rate_log.shape[0]
    extent = out_gain.shape[0]
    tp, sp = lax.axis_size("tp"), lax.axis_size("sp")
    weights = (query_weight, key_weight, value_weight, gate_weight)
    mixed, cache, first = fused(
        tp, sp, seqs, heads, tokens.reshape(seqs * span, kd), weights, beta_weight.T, decay_weight.T, beta_bias,
        rate_log, out_gain[None], new_query, new_key, new_value, new_beta, new_decay,
    )
    return emit(
        mixed.reshape(seqs, span, heads * extent), cache.reshape(seqs, heads, extent // sp, extent), first
    )


def solution(mesh):
    placed = (
        P(None, "sp", "tp"),
        P(None, "tp"),
        P(None, "tp"),
        P(None, "tp"),
        P(None, "tp"),
        P(None, "tp"),
        P(None, "tp"),
        P("tp"),
        P("tp"),
        P(),
        P(None, "tp", None),
        P(None, "tp", None),
        P(None, "tp", None),
        P(None, "tp"),
        P(None, "tp"),
    )
    return jax.shard_map(
        shards,
        mesh=mesh,
        in_specs=placed,
        out_specs=(P(None, "sp", "tp"), P(None, "tp", "sp", None), P(None, "tp")),
        check_vma=False,
    )
```

```python
import functools

import jax
import jax.numpy as jnp
from jax import lax
from jax.experimental import pallas as pl
from jax.experimental.pallas import tpu as pltpu
from jax.sharding import PartitionSpec as P

unit_floor = 1.0
norm_floor = 0.001
highest = lax.Precision.HIGHEST
MESH = pl.DeviceIdType.MESH
PAD = 8
INNER, OUTER = 8, 64
f32 = jnp.float32
bf16 = jnp.bfloat16

NN = (((1,), (0,)), ((), ()))
NT = (((1,), (1,)), ((), ()))
TN = (((0,), (0,)), ((), ()))


def dot(left, right, dims=NN, precision=None):
    return lax.dot_general(left, right, dims, precision=precision, preferred_element_type=f32)


def unit_rows(values):
    return values * lax.rsqrt(jnp.sum(values * values, axis=-1, keepdims=True) + unit_floor)


def group_of(n, heads):
    g = 1
    while g < n and (g < heads or g * g < n):
        g *= 2
    return g


def fused_kernel(
    tn, sn, seqs, heads, x_ref, wq_ref, wk_ref, wv_ref, wg_ref, bw_hbm, dw_hbm, bias_hbm, rate_hbm, gain_hbm,
    nq_hbm, nk_hbm, nv_hbm, nb_hbm, nd_hbm, mixed_ref, cache_ref, first_ref,
    bw_ref, dw_ref, bias_ref, rate_ref, gain_ref, nq_ref, nk_ref, nv_ref, nb_ref, nd_ref, small_sem,
    bd, xs, wbuf, acc, sacc, cum_row, cum_col, kh_buf, uw_buf, local_out, reach, gated,
    out_box, in_box, mid_out, mid_in, back_out, back_in, tail_out, tail_in, word_out, word_in, moves, drives, asks, extra,
    xsem, wsem, cross_sem, part_sem, fwd_sem, rx, prx,
    send1, recv1, send2, recv2, send3, recv3, send4, recv4, send5, recv5, hello,
):
    _, _, span, kd = xs.shape
    width = wq_ref.shape[1]
    extent = width // heads
    key_rows = extent // sn
    chunks = rx.shape[3]
    kc = kd // chunks
    tme, me = lax.axis_index("tp"), lax.axis_index("sp")
    y, c = tme // 2, lax.rem(tme, 2)
    chips = tn // 2
    partner = y * 2 + (1 - c)
    g = group_of(sn, heads)
    groups = sn // g
    team, m = me // g, lax.rem(me, g)
    weights = (wq_ref, wk_ref, wv_ref, wg_ref)

    barrier = pltpu.get_barrier_semaphore()
    pl.semaphore_signal(barrier, inc=1, device_id={"tp": partner}, device_id_type=MESH)
    for d in range(1, chips):
        to = lax.rem(y + d, chips) * 2 + c
        pl.semaphore_signal(barrier, inc=1, device_id={"tp": to}, device_id_type=MESH)
    for d in range(1, sn):

        @pl.when(me + d < sn)
        def _():
            pl.semaphore_signal(barrier, inc=1, device_id={"sp": me + d}, device_id_type=MESH)

    order = [tme, partner]
    for d in range(1, chips):
        source = lax.rem(y - d + chips, chips)
        order += [source * 2 + c, source * 2 + (1 - c)]

    def cols(ck):
        return pl.ds(ck * kc, kc)

    def token_copy(s):
        return pltpu.make_async_copy(x_ref.at[pl.ds(s * span, span), :], xs.at[tme, s], xsem.at[s])

    def weight_copy(w, slot):
        start = pl.multiple_of(order[slot] * kd, kd)
        return pltpu.make_async_copy(
            weights[w].at[pl.ds(start, kd), :], wbuf.at[slot, w], wsem.at[slot]
        )

    small_copies = [
        pltpu.make_async_copy(a, b, small_sem.at[i])
        for i, (a, b) in enumerate(
            (
                (bw_hbm, bw_ref), (dw_hbm, dw_ref), (bias_hbm, bias_ref), (rate_hbm, rate_ref), (gain_hbm, gain_ref),
                (nq_hbm, nq_ref), (nk_hbm, nk_ref), (nv_hbm, nv_ref), (nb_hbm, nb_ref), (nd_hbm, nd_ref),
            )
        )
    ]
    for s in range(seqs):
        token_copy(s).start()
    for copy in small_copies:
        copy.start()
    pl.semaphore_wait(barrier, chips + me)

    def cross_copy(d, s, ck):
        to = lax.rem(y + d, chips) * 2 + c
        return pltpu.make_async_remote_copy(
            src_ref=xs.at[tme, s, :, cols(ck)], dst_ref=xs.at[tme, s, :, cols(ck)],
            send_sem=cross_sem.at[d - 1], recv_sem=rx.at[d - 1, 0, s, ck],
            device_id={"tp": to}, device_id_type=MESH,
        )

    def part_copy(s):
        return pltpu.make_async_remote_copy(
            src_ref=xs.at[tme, s], dst_ref=xs.at[tme, s],
            send_sem=part_sem.at[0], recv_sem=prx.at[s],
            device_id={"tp": partner}, device_id_type=MESH,
        )

    for s in range(seqs):
        token_copy(s).wait()
        for ck in range(chunks):
            for d in range(1, chips):
                cross_copy(d, s, ck).start()
        part_copy(s).start()
    for slot in range(tn):
        for w in range(4):
            weight_copy(w, slot).start()
    for d in range(1, sn):

        @pl.when(me >= d)
        def _():
            pl.semaphore_signal(hello, inc=1, device_id={"sp": me - d}, device_id_type=MESH)

    for copy in small_copies:
        copy.wait()
    bd[...] = jnp.zeros_like(bd)
    bd[0 : bw_ref.shape[0]] = bw_ref[...]
    bd[PAD : PAD + dw_ref.shape[0]] = dw_ref[...]
    row = lax.broadcasted_iota(jnp.int32, (span, span), 0)
    col = lax.broadcasted_iota(jnp.int32, (span, span), 1)
    slot_of = lax.broadcasted_iota(jnp.int32, (PAD, 1), 0)
    bias = jnp.zeros((PAD, 1), f32)
    rate = jnp.zeros((PAD, 1), f32)
    for h in range(heads):
        bias = jnp.where(slot_of == h, bias_ref[h], bias)
        rate = jnp.where(slot_of == h, rate_ref[h], rate)

    def fwd_copy(d, s, ck):
        b = order[2 * d]
        return pltpu.make_async_remote_copy(
            src_ref=xs.at[b, s, :, cols(ck)], dst_ref=xs.at[b, s, :, cols(ck)],
            send_sem=fwd_sem.at[d - 1], recv_sem=rx.at[d - 1, 1, s, ck],
            device_id={"tp": partner}, device_id_type=MESH,
        )

    def arrive(d, side, s, ck):
        b = order[2 * d + side]
        pltpu.make_async_remote_copy(
            src_ref=xs.at[b, s, :, cols(ck)], dst_ref=xs.at[b, s, :, cols(ck)],
            send_sem=part_sem.at[0], recv_sem=rx.at[d - 1, side, s, ck],
            device_id={"tp": partner}, device_id_type=MESH,
        ).wait_recv()

    def small(x, start, depth, s, first):
        piece = bd[:, pl.ds(pl.multiple_of(start, depth), depth)]
        term = dot(piece, x, NT)
        sacc[s] = term if first else sacc[s] + term

    def use_whole(slot, s):
        b = order[slot]
        x = xs[b, s]
        if s == 0:
            weights_wait(slot)
        for w in range(4):
            term = dot(x, wbuf[slot, w])
            acc[s, w] = term if slot == 0 else acc[s, w] + term
        small(x, b * kd, kd, s, slot == 0)

    def weights_wait(slot):
        pltpu.make_async_copy(wbuf.at[slot], wbuf.at[slot], wsem.at[slot]).wait()

    def use(slot, s, ck, parts=(1, 2, 0, 3)):
        b = order[slot]
        x = xs[b, s, :, cols(ck)]
        if 1 in parts:
            if s == 0 and ck == 0:
                weights_wait(slot)
            small(x, b * kd + ck * kc, kc, s, False)
        for w in parts:
            acc[s, w] += dot(x, wbuf[slot, w, cols(ck), :])

    def forward(d, s, ck):
        arrive(d, 0, s, ck)
        fwd_copy(d, s, ck).start()

    def finish_chunk(d, s, ck, parts):
        use(2 * d, s, ck, parts)
        arrive(d, 1, s, ck)
        use(2 * d + 1, s, ck, parts)

    def heads_of(w, s):
        return [acc[s, w, :, h * extent : (h + 1) * extent].astype(bf16).astype(f32) for h in range(heads)]

    def owner_of(s, h):
        return (s * heads + h) % g

    def box_copy(s, h):
        return pltpu.make_async_remote_copy(
            src_ref=out_box.at[s, h], dst_ref=in_box.at[s, m],
            send_sem=send1.at[s], recv_sem=recv1.at[s],
            device_id={"sp": team * g + owner_of(s, h)}, device_id_type=MESH,
        )

    def boxes(s):
        beta = jax.nn.sigmoid(sacc[s, 0:PAD, :] + bias)
        pre = sacc[s, PAD : 2 * PAD, :]
        soft = jnp.maximum(pre, 0.0) + jnp.log1p(jnp.exp(-jnp.abs(pre)))
        upper = jnp.where(row <= col, 1.0, 0.0).astype(bf16)
        rest, pieces = -jnp.exp(rate) * soft, []
        for _ in range(3):
            pieces.append(rest.astype(bf16).astype(f32))
            rest = rest - pieces[-1]
        sums = dot(jnp.concatenate(pieces, axis=0).astype(bf16), upper)
        cum = sums[0:PAD] + sums[PAD : 2 * PAD] + sums[2 * PAD :]
        cum_t, beta_t = cum.T, beta.T
        cum_row[s] = cum
        cum_col[s] = cum_t
        hs, bs = range(heads), range(span // OUTER)
        line = lax.broadcasted_iota(jnp.int32, (OUTER, 2 * OUTER), 0)
        lane = lax.broadcasted_iota(jnp.int32, (OUTER, 2 * OUTER), 1)
        high = lane >= OUTER
        place = lane % OUTER
        same = line // INNER == place // INNER
        fill = jnp.zeros((OUTER, 2 * OUTER), bf16)
        unit = jnp.where(line == place, 1.0, 0.0)

        def part(b):
            return slice(b * OUTER, (b + 1) * OUTER)

        twice = [jnp.concatenate([cum[:, part(b)]] * 2, axis=1) for b in bs]
        k = [unit_rows(v) for v in heads_of(1, s)]
        kh = [v.astype(bf16) for v in k]
        pairs = [(h, b) for h in hs for b in bs]
        kk = [dot(kh[h][part(b)], jnp.concatenate([kh[h][part(b)]] * 2, axis=0), NT) for h, b in pairs]
        far = {(h, b): dot(kh[h][part(b)], kh[h][: b * OUTER], NT) for h, b in pairs if b > 0}
        right, kdec, last, low = [], [], [], []
        v = heads_of(2, s)
        for h in hs:
            cumc, bt = cum_t[:, h : h + 1], beta_t[:, h : h + 1]
            kh_buf[h] = kh[h]
            for b in bs:
                here = cumc[part(b)]
                wts = bt[part(b)] * jnp.exp(jnp.where(line >= place, here - twice[b][h : h + 1, :], 0.0))
                low.append(jnp.where(line > place, kk[h * len(bs) + b] * wts, 0.0))
                if b > 0:
                    wts = bt[part(b)] * jnp.exp(here - cum[h : h + 1, : b * OUTER])
                    far[h, b] = (far[h, b] * wts).astype(bf16)
            kb = k[h] * bt
            right.append(jnp.concatenate([v[h] * bt, kb * jnp.exp(cumc)], axis=1).astype(bf16))
            end = cumc[span - 1 :, :]
            kdec.append((k[h] * jnp.exp(end - cumc)).astype(bf16))
            last.append(jnp.exp(end))

        def climb(block):
            half = block.astype(bf16)
            return dot(half[:, :OUTER], half)

        z = [jnp.where(high, unit - n, n) for n in (jnp.where(same, m, 0.0) for m in low)]
        z = [jnp.where(high, a, climb(a)) for a in z]
        reached = 2
        while reached < INNER:
            z = [climb(a) + jnp.where(high, a, 0.0) for a in z]
            reached *= 2
        under = [jnp.concatenate([fill, jnp.where(high | same, 0.0, m).astype(bf16)], axis=0) for m in low]
        z = [a + dot(a.astype(bf16), u) for a, u in zip(z, under)]
        z = [jnp.where(high, a - t, t) for a, t in ((a, climb(a)) for a in z)]
        reached = 2
        while reached < OUTER // INNER:
            z = [climb(a) + jnp.where(high, a, 0.0) for a in z]
            reached *= 2
        inv = {p: a.astype(bf16) for p, a in zip(pairs, z)}
        none = jnp.zeros((OUTER, 2 * extent), bf16)
        term = {(h, b): dot(inv[h, b], jnp.concatenate([none, right[h][part(b)]], axis=0)) for h, b in pairs}
        far = {
            (h, b): dot(inv[h, b], jnp.concatenate([jnp.zeros_like(m), m], axis=0)).astype(bf16)
            for (h, b), m in far.items()
        }
        done = [[term[h, 0].astype(bf16)] for h in hs]
        for b in bs[1:]:
            for h in hs:
                seen = jnp.concatenate(done[h], axis=0) if b > 1 else done[h][0]
                done[h].append((term[h, b] - dot(far[h, b], seen)).astype(bf16))
        uw = [jnp.concatenate(d, axis=0) for d in done]
        z = [dot(a, u, TN) for a, u in zip(kdec, uw)]
        eye = lax.broadcasted_iota(jnp.int32, (extent, extent), 0) == lax.broadcasted_iota(
            jnp.int32, (extent, extent), 1
        )
        for h in hs:
            out_box[s, h, 0] = (jnp.where(eye, last[h] - 1.0, 0.0) - z[h][:, extent:]).astype(bf16)
            out_box[s, h, 1] = z[h][:, :extent].astype(bf16)
            uw_buf[h] = uw[h]
        if s == 0:

            @pl.when(me < sn - 1)
            def _():
                pl.semaphore_wait(hello, sn - 1 - me)

        for h in hs:
            own = m == owner_of(s, h)

            @pl.when(own)
            def _():
                in_box[s, m] = out_box[s, h]

            @pl.when(jnp.logical_not(own))
            def _():
                box_copy(s, h).start()

    def queries(s):
        cum, cum_t = cum_row[s], cum_col[s]
        gain = gain_ref[...]
        hs = range(heads)
        causal = row >= col

        def spread(h):
            gap = jnp.where(causal, cum_t[:, h : h + 1] - cum[h : h + 1, :], 0.0)
            return jnp.where(causal, jnp.exp(gap), 0.0)

        q = [unit_rows(v) for v in heads_of(0, s)]
        scores = [(dot(q[h].astype(bf16), kh_buf[h], NT) * spread(h)).astype(bf16) for h in hs]
        out = [dot(scores[h], uw_buf[h]) for h in hs]
        gates = heads_of(3, s)
        for h in hs:
            local_out[s, h] = out[h][:, :extent]
            reach[s, h] = (q[h] * jnp.exp(cum_t[:, h : h + 1]) - out[h][:, extent:]).astype(bf16)
            gated[s, h] = gates[h] * jax.nn.sigmoid(gates[h]) * gain

    def own_head(s):
        return lax.rem(m + g - (s * heads) % g, g)

    def back_copy(s, i):
        return pltpu.make_async_remote_copy(
            src_ref=back_out.at[s, i], dst_ref=back_in.at[s, own_head(s)],
            send_sem=send2.at[s], recv_sem=recv2.at[s],
            device_id={"sp": team * g + i}, device_id_type=MESH,
        )

    def mid_copy(s):
        return pltpu.make_async_remote_copy(
            src_ref=mid_out.at[s], dst_ref=mid_in.at[s], send_sem=send3.at[s], recv_sem=recv3.at[s],
            device_id={"sp": lax.rem(me + g, sn)}, device_id_type=MESH,
        )

    def tail_copies(s, j):
        h = own_head(s)
        return (
            pltpu.make_async_remote_copy(
                src_ref=tail_out.at[s, j], dst_ref=tail_in.at[s, h], send_sem=send4.at[s], recv_sem=recv4.at[s],
                device_id={"sp": j}, device_id_type=MESH,
            ),
            pltpu.make_async_remote_copy(
                src_ref=word_out.at[s, j], dst_ref=word_in.at[s, h], send_sem=send5.at[s], recv_sem=recv5.at[s],
                device_id={"sp": j}, device_id_type=MESH,
            ),
        )

    def settle(ref, sem):
        pltpu.make_async_copy(ref, ref, sem).wait()

    def box_wait(s):
        settle(in_box.at[s, pl.ds(0, g - 1)], recv1.at[s])

    def give_back(s):
        for i in range(g):

            @pl.when(i == m)
            def _():
                back_in[s, own_head(s)] = back_out[s, i]

            @pl.when(i != m)
            def _():
                back_copy(s, i).start()

    def prepare(s):
        h = own_head(s)
        shape3 = nq_ref.shape
        mine = (lax.broadcasted_iota(jnp.int32, shape3, 0) == s) & (lax.broadcasted_iota(jnp.int32, shape3, 1) == h)

        def own(ref):
            kept = jnp.where(mine, ref[...].astype(f32), 0.0)
            return jnp.sum(jnp.sum(kept, axis=0), axis=0, keepdims=True)

        qn, kn = unit_rows(own(nq_ref)), unit_rows(own(nk_ref))
        rest = jnp.concatenate([jnp.broadcast_to(qn, (PAD, extent)), jnp.broadcast_to(kn, (PAD, extent))], axis=0)
        for i in range(3):
            piece = rest.astype(bf16)
            asks[s, i * 2 * PAD : (i + 1) * 2 * PAD] = piece
            rest = rest - piece.astype(f32)
        extra[s, 0:1] = own(nv_ref)
        extra[s, 1:2] = jnp.broadcast_to(jnp.sum(kn * qn, axis=-1, keepdims=True), (1, extent))

    def conclude(s, final):
        kept_h = final.astype(bf16)
        h = own_head(s)
        for j in range(sn):
            tail_out[s, j] = kept_h[j * key_rows : (j + 1) * key_rows]
        sums = dot(asks[s], kept_h)
        sums = sums[0 : 2 * PAD] + sums[2 * PAD : 4 * PAD] + sums[4 * PAD :]
        recall, retrieve = sums[0:1], sums[PAD : PAD + 1]
        beta_new, decay_new = nb_ref[s, h], nd_ref[s, h]
        fresh = extra[s, 0:1] - decay_new * retrieve
        read = decay_new * recall + (beta_new * extra[s, 1:2]) * fresh
        norm = lax.rsqrt(jnp.mean(read * read, axis=-1, keepdims=True) + norm_floor)
        word = read * norm * gain_ref[...]
        for j in range(sn):
            word_out[s, j] = word
        for j in range(sn):

            @pl.when(j == me)
            def _():
                tail_in[s, h] = tail_out[s, j]
                word_in[s, h] = word_out[s, j]

            @pl.when(j != me)
            def _():
                for copy in tail_copies(s, j):
                    copy.start()

    def chain_first(s):
        @pl.when((own_head(s) < heads) & (team == 0))
        def _():
            if groups == 1:
                prepare(s)
            box_wait(s)
            state = jnp.zeros((extent, extent), f32)
            for i in range(g):
                half = state.astype(bf16)
                back_out[s, i] = half
                if i == 0:
                    state = in_box[s, i, 1].astype(f32)
                else:
                    state = state + dot(in_box[s, i, 0], half) + in_box[s, i, 1].astype(f32)
            if groups > 1:
                mid_out[s] = state.astype(bf16)
                mid_copy(s).start()
            if groups == 1:
                conclude(s, state)
            give_back(s)

    def compose(s):
        if groups == 1:
            return

        @pl.when((own_head(s) < heads) & (team > 0))
        def _():
            prepare(s)
            box_wait(s)
            for i in range(g):
                step, push = in_box[s, i, 0], in_box[s, i, 1].astype(f32)
                if i == 0:
                    shift, drive = step.astype(f32), push
                else:
                    shift, drive = (
                        shift + step.astype(f32) + dot(step, shift.astype(bf16)),
                        drive + push + dot(step, drive.astype(bf16)),
                    )
                moves[s, i * extent : (i + 1) * extent] = shift.astype(bf16)
                drives[s, i * extent : (i + 1) * extent] = drive

    def relay(s):
        if groups == 1:
            return

        @pl.when((own_head(s) < heads) & (team > 0))
        def _():
            pltpu.make_async_remote_copy(
                src_ref=mid_out.at[s], dst_ref=mid_in.at[s], send_sem=send3.at[s], recv_sem=recv3.at[s],
                device_id={"sp": lax.rem(me + sn - g, sn)}, device_id_type=MESH,
            ).wait_recv()
            start = mid_in[s]
            base = start.astype(f32)
            top = (g - 1) * extent
            state = base + dot(moves[s, top:], start) + drives[s, top:]

            @pl.when(team < groups - 1)
            def _():
                mid_out[s] = state.astype(bf16)
                mid_copy(s).start()

            @pl.when(team == groups - 1)
            def _():
                conclude(s, state)

            moved = dot(moves[s, :top], start) + drives[s, :top]
            back_out[s, 0] = start
            for i in range(1, g):
                back_out[s, i] = (base + moved[(i - 1) * extent : i * extent]).astype(bf16)
            give_back(s)

    def arrivals(owner, ref, sem):
        if heads > 1:

            @pl.when(owner)
            def _():
                settle(ref.at[pl.ds(0, heads - 1)], sem)

        @pl.when(jnp.logical_not(owner))
        def _():
            settle(ref, sem)

    def finish(s):
        arrivals(own_head(s) < heads, back_in.at[s], recv2.at[s])
        outs = [local_out[s, h] + dot(reach[s, h], back_in[s, h]) for h in range(heads)]
        for h in range(heads):
            o = outs[h]
            norm = lax.rsqrt(jnp.mean(o * o, axis=-1, keepdims=True) + norm_floor)
            mixed_ref[s * span : (s + 1) * span, h * extent : (h + 1) * extent] = (o * norm * gated[s, h]).astype(bf16)

    def take_tail(s):
        source = (team == groups - 1) & (own_head(s) < heads)
        arrivals(source, tail_in.at[s], recv4.at[s])
        arrivals(source, word_in.at[s], recv5.at[s])
        for h in range(heads):
            cache_ref[s * heads + h] = tail_in[s, h]
            first_ref[s : s + 1, h * extent : (h + 1) * extent] = word_in[s, h]

    for s in range(seqs):
        use_whole(0, s)
    for s in range(seqs):
        pltpu.make_async_remote_copy(
            src_ref=xs.at[partner, s], dst_ref=xs.at[partner, s], send_sem=part_sem.at[0], recv_sem=prx.at[s],
            device_id={"tp": partner}, device_id_type=MESH,
        ).wait_recv()
        use_whole(1, s)

    for s in range(seqs):
        for ck in range(chunks):
            for d in range(1, chips):
                if s == 0 or ck > 0:
                    forward(d, s, ck)
                finish_chunk(d, s, ck, (1, 2) if ck == chunks - 1 else (1, 2, 0, 3))
        boxes(s)
        if s > 0:
            chain_first(s - 1)
            compose(s - 1)
        if s < seqs - 1:
            for d in range(1, chips):
                forward(d, s + 1, 0)
        for slot in range(2, tn):
            use(slot, s, chunks - 1, (0, 3))
        queries(s)
        if s > 0:
            relay(s - 1)
    compose(seqs - 1)
    chain_first(seqs - 1)
    relay(seqs - 1)
    for s in range(seqs):
        finish(s)
    settle(xs.at[tme], part_sem.at[0])
    for d in range(1, chips):
        settle(xs.at[tme], cross_sem.at[d - 1])
        settle(xs.at[tme], fwd_sem.at[d - 1])
    for s in range(seqs):
        own = own_head(s) < heads
        arrivals(own, out_box.at[s], send1.at[s])

        @pl.when(own)
        def _():
            settle(back_out.at[s, pl.ds(0, g - 1)], send2.at[s])

            @pl.when(team < groups - 1)
            def _():
                mid_copy(s).wait_send()

            @pl.when(team == groups - 1)
            def _():
                settle(tail_out.at[s, pl.ds(0, sn - 1)], send4.at[s])
                settle(word_out.at[s, pl.ds(0, sn - 1)], send5.at[s])

    for s in range(seqs):
        take_tail(s)


def fused(tn, sn, seqs, heads, tokens, weights, bw, dw, bias, rate, gain, nq, nk, nv, nb, nd):
    rows, kd = tokens.shape
    width = weights[0].shape[1]
    kc = 256 if kd % 256 == 0 else kd
    chunks, chips, span = kd // kc, tn // 2, rows // seqs
    extent = width // heads
    pairs, key_rows = seqs * heads, extent // sn
    g = group_of(sn, heads)
    operands = (tokens, *weights, bw, dw, bias, rate, gain, nq, nk, nv, nb, nd)
    vmem = pl.BlockSpec(memory_space=pltpu.VMEM)
    hbm = pl.BlockSpec(memory_space=pltpu.HBM)
    dma = pltpu.SemaphoreType.DMA
    return pl.pallas_call(
        functools.partial(fused_kernel, tn, sn, seqs, heads),
        out_shape=(
            jax.ShapeDtypeStruct((rows, width), bf16),
            jax.ShapeDtypeStruct((pairs, key_rows, extent), bf16),
            jax.ShapeDtypeStruct((seqs, width), f32),
        ),
        in_specs=[hbm] * 15,
        out_specs=(vmem,) * 3,
        scratch_shapes=[
            pltpu.VMEM(bw.shape, bf16),
            pltpu.VMEM(dw.shape, bf16),
            pltpu.SMEM(bias.shape, f32),
            pltpu.SMEM(rate.shape, f32),
            pltpu.VMEM(gain.shape, f32),
            pltpu.VMEM(nq.shape, bf16),
            pltpu.VMEM(nk.shape, bf16),
            pltpu.VMEM(nv.shape, bf16),
            pltpu.SMEM(nb.shape, f32),
            pltpu.SMEM(nd.shape, f32),
            dma((10,)),
            pltpu.VMEM((2 * PAD, bw.shape[1]), bf16),
            pltpu.VMEM((tn, seqs, span, kd), bf16),
            pltpu.VMEM((tn, 4, kd, width), bf16),
            pltpu.VMEM((seqs, 4, span, width), f32),
            pltpu.VMEM((seqs, 2 * PAD, span), f32),
            pltpu.VMEM((seqs, PAD, span), f32),
            pltpu.VMEM((seqs, span, PAD), f32),
            pltpu.VMEM((heads, span, extent), bf16),
            pltpu.VMEM((heads, span, 2 * extent), bf16),
            pltpu.VMEM((seqs, heads, span, extent), f32),
            pltpu.VMEM((seqs, heads, span, extent), bf16),
            pltpu.VMEM((seqs, heads, span, extent), f32),
            pltpu.VMEM((seqs, heads, 2, extent, extent), bf16),
            pltpu.VMEM((seqs, g, 2, extent, extent), bf16),
            pltpu.VMEM((seqs, extent, extent), bf16),
            pltpu.VMEM((seqs, extent, extent), bf16),
            pltpu.VMEM((seqs, g, extent, extent), bf16),
            pltpu.VMEM((seqs, heads, extent, extent), bf16),
            pltpu.VMEM((seqs, sn, key_rows, extent), bf16),
            pltpu.VMEM((seqs, heads, key_rows, extent), bf16),
            pltpu.VMEM((seqs, sn, 1, extent), f32),
            pltpu.VMEM((seqs, heads, 1, extent), f32),
            pltpu.VMEM((seqs, g * extent, extent), bf16),
            pltpu.VMEM((seqs, g * extent, extent), f32),
            pltpu.VMEM((seqs, 6 * PAD, extent), bf16),
            pltpu.VMEM((seqs, PAD, extent), f32),
            dma((seqs,)),
            dma((tn,)),
            dma((chips - 1,)),
            dma((1,)),
            dma((chips - 1,)),
            dma((chips - 1, 2, seqs, chunks)),
            dma((seqs,)),
            dma((seqs,)),
            dma((seqs,)),
            dma((seqs,)),
            dma((seqs,)),
            dma((seqs,)),
            dma((seqs,)),
            dma((seqs,)),
            dma((seqs,)),
            dma((seqs,)),
            dma((seqs,)),
            pltpu.SemaphoreType.REGULAR,
        ],
        compiler_params=pltpu.CompilerParams(
            collective_id=0, has_side_effects=True, vmem_limit_bytes=53 * 1024 * 1024
        ),
    )(*[pltpu.with_memory_space_constraint(a, pltpu.HBM) for a in operands])


def emit_kernel(mixed_ref, cache_ref, first_ref, mixed_out, cache_out, first_out, sem):
    copies = [
        pltpu.make_async_copy(a, b, sem.at[i])
        for i, (a, b) in enumerate(((mixed_ref, mixed_out), (cache_ref, cache_out), (first_ref, first_out)))
    ]
    for copy in copies:
        copy.start()
    for copy in copies:
        copy.wait()


def emit(*results):
    return pl.pallas_call(
        emit_kernel,
        out_shape=tuple(jax.ShapeDtypeStruct(r.shape, r.dtype) for r in results),
        in_specs=[pl.BlockSpec(memory_space=pltpu.VMEM)] * 3,
        out_specs=(pl.BlockSpec(memory_space=pltpu.HBM),) * 3,
        scratch_shapes=[pltpu.SemaphoreType.DMA((3,))],
        compiler_params=pltpu.CompilerParams(vmem_limit_bytes=4 * 1024 * 1024),
    )(*results)


def shards(
    tokens, query_weight, key_weight, value_weight, gate_weight, beta_weight, decay_weight,
    beta_bias, rate_log, out_gain, new_query, new_key, new_value, new_beta, new_decay,
):
    seqs, span, kd = tokens.shape
    heads = rate_log.shape[0]
    extent = out_gain.shape[0]
    tp, sp = lax.axis_size("tp"), lax.axis_size("sp")
    weights = (query_weight, key_weight, value_weight, gate_weight)
    mixed, cache, first = fused(
        tp, sp, seqs, heads, tokens.reshape(seqs * span, kd), weights, beta_weight.T, decay_weight.T, beta_bias,
        rate_log, out_gain[None], new_query, new_key, new_value, new_beta, new_decay,
    )
    return emit(
        mixed.reshape(seqs, span, heads * extent), cache.reshape(seqs, heads, extent // sp, extent), first
    )


def solution(mesh):
    placed = (
        P(None, "sp", "tp"),
        P(None, "tp"),
        P(None, "tp"),
        P(None, "tp"),
        P(None, "tp"),
        P(None, "tp"),
        P(None, "tp"),
        P("tp"),
        P("tp"),
        P(),
        P(None, "tp", None),
        P(None, "tp", None),
        P(None, "tp", None),
        P(None, "tp"),
        P(None, "tp"),
    )
    return jax.shard_map(
        shards,
        mesh=mesh,
        in_specs=placed,
        out_specs=(P(None, "sp", "tp"), P(None, "tp", "sp", None), P(None, "tp")),
        check_vma=False,
    )
```

```python
import functools

import jax
import jax.numpy as jnp
from jax import lax
from jax.experimental import pallas as pl
from jax.experimental.pallas import tpu as pltpu
from jax.sharding import PartitionSpec as P

unit_floor = 1.0
norm_floor = 0.001
highest = lax.Precision.HIGHEST
MESH = pl.DeviceIdType.MESH
PAD = 8
INNER, OUTER = 8, 64
f32 = jnp.float32
bf16 = jnp.bfloat16

NN = (((1,), (0,)), ((), ()))
NT = (((1,), (1,)), ((), ()))
TN = (((0,), (0,)), ((), ()))


def dot(left, right, dims=NN, precision=None):
    return lax.dot_general(left, right, dims, precision=precision, preferred_element_type=f32)


def unit_rows(values):
    return values * lax.rsqrt(jnp.sum(values * values, axis=-1, keepdims=True) + unit_floor)


def group_of(n, heads):
    g = 1
    while g < n and (g < heads or g * g < n):
        g *= 2
    return g


def fused_kernel(
    tn, sn, seqs, heads, x_ref, wq_ref, wk_ref, wv_ref, wg_ref, bw_hbm, dw_hbm, bias_hbm, rate_hbm, gain_hbm,
    nq_hbm, nk_hbm, nv_hbm, nb_hbm, nd_hbm, mixed_ref, cache_ref, first_ref,
    bw_ref, dw_ref, bias_ref, rate_ref, gain_ref, nq_ref, nk_ref, nv_ref, nb_ref, nd_ref, small_sem,
    bd, xs, wbuf, acc, sacc, cum_row, cum_col, kh_buf, uw_buf, local_out, reach, gated,
    out_box, in_box, mid_out, mid_in, back_out, back_in, tail_out, tail_in, moves, drives, asks, extra, news, news_sem,
    xsem, wsem, cross_sem, part_sem, fwd_sem, rx, prx,
    send1, recv1, send2, recv2, send3, recv3, send4, recv4, hello,
):
    _, _, span, kd = xs.shape
    width = wq_ref.shape[1]
    extent = width // heads
    key_rows = extent // sn
    chunks = rx.shape[3]
    kc = kd // chunks
    tme, me = lax.axis_index("tp"), lax.axis_index("sp")
    y, c = tme // 2, lax.rem(tme, 2)
    chips = tn // 2
    partner = y * 2 + (1 - c)
    g = group_of(sn, heads)
    groups = sn // g
    team, m = me // g, lax.rem(me, g)
    weights = (wq_ref, wk_ref, wv_ref, wg_ref)

    barrier = pltpu.get_barrier_semaphore()
    pl.semaphore_signal(barrier, inc=1, device_id={"tp": partner}, device_id_type=MESH)
    for d in range(1, chips):
        to = lax.rem(y + d, chips) * 2 + c
        pl.semaphore_signal(barrier, inc=1, device_id={"tp": to}, device_id_type=MESH)
    for d in range(1, sn):

        @pl.when(me + d < sn)
        def _():
            for t in (tme, partner):
                pl.semaphore_signal(barrier, inc=1, device_id={"sp": me + d, "tp": t}, device_id_type=MESH)

    order = [tme, partner]
    for d in range(1, chips):
        source = lax.rem(y - d + chips, chips)
        order += [source * 2 + c, source * 2 + (1 - c)]

    def cols(ck):
        return pl.ds(ck * kc, kc)

    def token_copy(s):
        return pltpu.make_async_copy(x_ref.at[pl.ds(s * span, span), :], xs.at[tme, s], xsem.at[s])

    def weight_copy(w, slot):
        start = pl.multiple_of(order[slot] * kd, kd)
        return pltpu.make_async_copy(
            weights[w].at[pl.ds(start, kd), :], wbuf.at[slot, w], wsem.at[slot]
        )

    small_copies = [
        pltpu.make_async_copy(a, b, small_sem.at[i])
        for i, (a, b) in enumerate(
            (
                (bw_hbm, bw_ref), (dw_hbm, dw_ref), (bias_hbm, bias_ref), (rate_hbm, rate_ref), (gain_hbm, gain_ref),
                (nq_hbm, nq_ref), (nk_hbm, nk_ref), (nv_hbm, nv_ref), (nb_hbm, nb_ref), (nd_hbm, nd_ref),
            )
        )
    ]
    for s in range(seqs):
        token_copy(s).start()
    for copy in small_copies:
        copy.start()
    pl.semaphore_wait(barrier, chips + 2 * me)

    def cross_copy(d, s, ck):
        to = lax.rem(y + d, chips) * 2 + c
        return pltpu.make_async_remote_copy(
            src_ref=xs.at[tme, s, :, cols(ck)], dst_ref=xs.at[tme, s, :, cols(ck)],
            send_sem=cross_sem.at[d - 1], recv_sem=rx.at[d - 1, 0, s, ck],
            device_id={"tp": to}, device_id_type=MESH,
        )

    def part_copy(s):
        return pltpu.make_async_remote_copy(
            src_ref=xs.at[tme, s], dst_ref=xs.at[tme, s],
            send_sem=part_sem.at[0], recv_sem=prx.at[s],
            device_id={"tp": partner}, device_id_type=MESH,
        )

    for s in range(seqs):
        token_copy(s).wait()
        for ck in range(chunks):
            for d in range(1, chips):
                cross_copy(d, s, ck).start()
        part_copy(s).start()
    for slot in range(tn):
        for w in range(4):
            weight_copy(w, slot).start()
    for d in range(1, sn):

        @pl.when(me >= d)
        def _():
            for t in (tme, partner):
                pl.semaphore_signal(hello, inc=1, device_id={"sp": me - d, "tp": t}, device_id_type=MESH)

    for copy in small_copies:
        copy.wait()
    for s in range(seqs):
        for i, ref in enumerate((nq_ref, nk_ref, nv_ref)):
            news[c, i, s * heads : (s + 1) * heads] = ref[s].astype(f32)
        for i, ref in enumerate((nb_ref, nd_ref)):
            for h in range(heads):
                news[c, 3 + i, s * heads + h : s * heads + h + 1] = jnp.full((1, extent), ref[s, h], f32)

    def news_copy():
        return pltpu.make_async_remote_copy(
            src_ref=news.at[0], dst_ref=news.at[0], send_sem=news_sem.at[0], recv_sem=news_sem.at[1],
            device_id={"tp": partner}, device_id_type=MESH,
        )

    @pl.when(c == 0)
    def _():
        news_copy().start()

    bd[...] = jnp.zeros_like(bd)
    bd[0 : bw_ref.shape[0]] = bw_ref[...]
    bd[PAD : PAD + dw_ref.shape[0]] = dw_ref[...]
    row = lax.broadcasted_iota(jnp.int32, (span, span), 0)
    col = lax.broadcasted_iota(jnp.int32, (span, span), 1)
    slot_of = lax.broadcasted_iota(jnp.int32, (PAD, 1), 0)
    bias = jnp.zeros((PAD, 1), f32)
    rate = jnp.zeros((PAD, 1), f32)
    for h in range(heads):
        bias = jnp.where(slot_of == h, bias_ref[h], bias)
        rate = jnp.where(slot_of == h, rate_ref[h], rate)

    def fwd_copy(d, s, ck):
        b = order[2 * d]
        return pltpu.make_async_remote_copy(
            src_ref=xs.at[b, s, :, cols(ck)], dst_ref=xs.at[b, s, :, cols(ck)],
            send_sem=fwd_sem.at[d - 1], recv_sem=rx.at[d - 1, 1, s, ck],
            device_id={"tp": partner}, device_id_type=MESH,
        )

    def arrive(d, side, s, ck):
        b = order[2 * d + side]
        pltpu.make_async_remote_copy(
            src_ref=xs.at[b, s, :, cols(ck)], dst_ref=xs.at[b, s, :, cols(ck)],
            send_sem=part_sem.at[0], recv_sem=rx.at[d - 1, side, s, ck],
            device_id={"tp": partner}, device_id_type=MESH,
        ).wait_recv()

    def small(x, start, depth, s, first):
        piece = bd[:, pl.ds(pl.multiple_of(start, depth), depth)]
        term = dot(piece, x, NT)
        sacc[s] = term if first else sacc[s] + term

    def use_whole(slot, s):
        b = order[slot]
        x = xs[b, s]
        if s == 0:
            weights_wait(slot)
        for w in range(4):
            term = dot(x, wbuf[slot, w])
            acc[s, w] = term if slot == 0 else acc[s, w] + term
        small(x, b * kd, kd, s, slot == 0)

    def weights_wait(slot):
        pltpu.make_async_copy(wbuf.at[slot], wbuf.at[slot], wsem.at[slot]).wait()

    def use(slot, s, ck, parts=(1, 2, 0, 3)):
        b = order[slot]
        x = xs[b, s, :, cols(ck)]
        if 1 in parts:
            if s == 0 and ck == 0:
                weights_wait(slot)
            small(x, b * kd + ck * kc, kc, s, False)
        for w in parts:
            acc[s, w] += dot(x, wbuf[slot, w, cols(ck), :])

    def forward(d, s, ck):
        arrive(d, 0, s, ck)
        fwd_copy(d, s, ck).start()

    def finish_chunk(d, s, ck, parts):
        use(2 * d, s, ck, parts)
        arrive(d, 1, s, ck)
        use(2 * d + 1, s, ck, parts)

    def heads_of(w, s):
        return [acc[s, w, :, h * extent : (h + 1) * extent].astype(bf16).astype(f32) for h in range(heads)]

    def owner_of(s, h):
        return (s * heads + h) % g

    def box_copy(s, h):
        return pltpu.make_async_remote_copy(
            src_ref=out_box.at[s, h], dst_ref=in_box.at[s, (1 - c) * g + m],
            send_sem=send1.at[s], recv_sem=recv1.at[s],
            device_id={"sp": team * g + owner_of(s, h), "tp": y * 2 + 1}, device_id_type=MESH,
        )

    def boxes(s):
        beta = jax.nn.sigmoid(sacc[s, 0:PAD, :] + bias)
        pre = sacc[s, PAD : 2 * PAD, :]
        soft = jnp.maximum(pre, 0.0) + jnp.log1p(jnp.exp(-jnp.abs(pre)))
        upper = jnp.where(row <= col, 1.0, 0.0).astype(bf16)
        rest, pieces = -jnp.exp(rate) * soft, []
        for _ in range(3):
            pieces.append(rest.astype(bf16).astype(f32))
            rest = rest - pieces[-1]
        sums = dot(jnp.concatenate(pieces, axis=0).astype(bf16), upper)
        cum = sums[0:PAD] + sums[PAD : 2 * PAD] + sums[2 * PAD :]
        cum_t, beta_t = cum.T, beta.T
        cum_row[s] = cum
        cum_col[s] = cum_t
        hs, bs = range(heads), range(span // OUTER)
        line = lax.broadcasted_iota(jnp.int32, (OUTER, 2 * OUTER), 0)
        lane = lax.broadcasted_iota(jnp.int32, (OUTER, 2 * OUTER), 1)
        high = lane >= OUTER
        place = lane % OUTER
        same = line // INNER == place // INNER
        fill = jnp.zeros((OUTER, 2 * OUTER), bf16)
        unit = jnp.where(line == place, 1.0, 0.0)

        def part(b):
            return slice(b * OUTER, (b + 1) * OUTER)

        twice = [jnp.concatenate([cum[:, part(b)]] * 2, axis=1) for b in bs]
        k = [unit_rows(v) for v in heads_of(1, s)]
        kh = [v.astype(bf16) for v in k]
        pairs = [(h, b) for h in hs for b in bs]
        kk = [dot(kh[h][part(b)], jnp.concatenate([kh[h][part(b)]] * 2, axis=0), NT) for h, b in pairs]
        far = {(h, b): dot(kh[h][part(b)], kh[h][: b * OUTER], NT) for h, b in pairs if b > 0}
        right, kdec, last, low = [], [], [], []
        v = heads_of(2, s)
        for h in hs:
            cumc, bt = cum_t[:, h : h + 1], beta_t[:, h : h + 1]
            kh_buf[h] = kh[h]
            for b in bs:
                here = cumc[part(b)]
                wts = bt[part(b)] * jnp.exp(jnp.where(line >= place, here - twice[b][h : h + 1, :], 0.0))
                low.append(jnp.where(line > place, kk[h * len(bs) + b] * wts, 0.0))
                if b > 0:
                    wts = bt[part(b)] * jnp.exp(here - cum[h : h + 1, : b * OUTER])
                    far[h, b] = (far[h, b] * wts).astype(bf16)
            kb = k[h] * bt
            right.append(jnp.concatenate([v[h] * bt, kb * jnp.exp(cumc)], axis=1).astype(bf16))
            end = cumc[span - 1 :, :]
            kdec.append((k[h] * jnp.exp(end - cumc)).astype(bf16))
            last.append(jnp.exp(end))

        def climb(block):
            half = block.astype(bf16)
            return dot(half[:, :OUTER], half)

        z = [jnp.where(high, unit - n, n) for n in (jnp.where(same, m, 0.0) for m in low)]
        z = [jnp.where(high, a, climb(a)) for a in z]
        reached = 2
        while reached < INNER:
            z = [climb(a) + jnp.where(high, a, 0.0) for a in z]
            reached *= 2
        under = [jnp.concatenate([fill, jnp.where(high | same, 0.0, m).astype(bf16)], axis=0) for m in low]
        z = [a + dot(a.astype(bf16), u) for a, u in zip(z, under)]
        z = [jnp.where(high, a - t, t) for a, t in ((a, climb(a)) for a in z)]
        reached = 2
        while reached < OUTER // INNER:
            z = [climb(a) + jnp.where(high, a, 0.0) for a in z]
            reached *= 2
        inv = {p: a.astype(bf16) for p, a in zip(pairs, z)}
        none = jnp.zeros((OUTER, 2 * extent), bf16)
        term = {(h, b): dot(inv[h, b], jnp.concatenate([none, right[h][part(b)]], axis=0)) for h, b in pairs}
        far = {
            (h, b): dot(inv[h, b], jnp.concatenate([jnp.zeros_like(m), m], axis=0)).astype(bf16)
            for (h, b), m in far.items()
        }
        done = [[term[h, 0].astype(bf16)] for h in hs]
        for b in bs[1:]:
            for h in hs:
                seen = jnp.concatenate(done[h], axis=0) if b > 1 else done[h][0]
                done[h].append((term[h, b] - dot(far[h, b], seen)).astype(bf16))
        uw = [jnp.concatenate(d, axis=0) for d in done]
        z = [dot(a, u, TN) for a, u in zip(kdec, uw)]
        eye = lax.broadcasted_iota(jnp.int32, (extent, extent), 0) == lax.broadcasted_iota(
            jnp.int32, (extent, extent), 1
        )
        for h in hs:
            out_box[s, h, 0] = (jnp.where(eye, last[h] - 1.0, 0.0) - z[h][:, extent:]).astype(bf16)
            out_box[s, h, 1] = z[h][:, :extent].astype(bf16)
            uw_buf[h] = uw[h]
        if s == 0:

            @pl.when(me < sn - 1)
            def _():
                pl.semaphore_wait(hello, 2 * (sn - 1 - me))

        for h in hs:
            own = (m == owner_of(s, h)) & (c == 1)

            @pl.when(own)
            def _():
                in_box[s, m] = out_box[s, h]

            @pl.when(jnp.logical_not(own))
            def _():
                box_copy(s, h).start()

    def queries(s):
        cum, cum_t = cum_row[s], cum_col[s]
        gain = gain_ref[...]
        hs = range(heads)
        causal = row >= col

        def spread(h):
            gap = jnp.where(causal, cum_t[:, h : h + 1] - cum[h : h + 1, :], 0.0)
            return jnp.where(causal, jnp.exp(gap), 0.0)

        q = [unit_rows(v) for v in heads_of(0, s)]
        scores = [(dot(q[h].astype(bf16), kh_buf[h], NT) * spread(h)).astype(bf16) for h in hs]
        out = [dot(scores[h], uw_buf[h]) for h in hs]
        gates = heads_of(3, s)
        for h in hs:
            local_out[s, h] = out[h][:, :extent]
            reach[s, h] = (q[h] * jnp.exp(cum_t[:, h : h + 1]) - out[h][:, extent:]).astype(bf16)
            gated[s, h] = gates[h] * jax.nn.sigmoid(gates[h]) * gain

    def own_head(s):
        return lax.rem(m + g - (s * heads) % g, g)

    def owner(s):
        return (own_head(s) < heads) & (c == 1)

    def back_copy(s, e, i):
        return pltpu.make_async_remote_copy(
            src_ref=back_out.at[s, e * g + i], dst_ref=back_in.at[s, own_head(s)],
            send_sem=send2.at[s], recv_sem=recv2.at[s],
            device_id={"sp": team * g + i, "tp": y * 2 + 1 - e}, device_id_type=MESH,
        )

    def mid_copy(s):
        return pltpu.make_async_remote_copy(
            src_ref=mid_out.at[s], dst_ref=mid_in.at[s], send_sem=send3.at[s], recv_sem=recv3.at[s],
            device_id={"sp": lax.rem(me + g, sn)}, device_id_type=MESH,
        )

    def tail_copy(s, e, j):
        return pltpu.make_async_remote_copy(
            src_ref=tail_out.at[s, e * sn + j], dst_ref=tail_in.at[s, own_head(s)],
            send_sem=send4.at[s], recv_sem=recv4.at[s],
            device_id={"sp": j, "tp": y * 2 + 1 - e}, device_id_type=MESH,
        )

    def settle(ref, sem):
        pltpu.make_async_copy(ref, ref, sem).wait()

    def box_wait(s):
        settle(in_box.at[s, pl.ds(0, 2 * g - 1)], recv1.at[s])

    def give_back(s):
        for i in range(g):
            back_copy(s, 1, i).start()

            @pl.when(i == m)
            def _():
                back_in[s, own_head(s)] = back_out[s, i]

            @pl.when(i != m)
            def _():
                back_copy(s, 0, i).start()

    def prepare(s):
        r = s * heads + own_head(s)
        for e in range(2):
            told = [news[1 - e, i, pl.ds(r, 1), :] for i in range(3)]
            qn, kn = unit_rows(told[0]), unit_rows(told[1])
            rest = jnp.concatenate([jnp.broadcast_to(qn, (PAD, extent)), jnp.broadcast_to(kn, (PAD, extent))], axis=0)
            for i in range(3):
                piece = rest.astype(bf16)
                asks[s, e, i * 2 * PAD : (i + 1) * 2 * PAD] = piece
                rest = rest - piece.astype(f32)
            decay, meet = news[1 - e, 4, pl.ds(r, 1), :], jnp.sum(kn * qn, axis=-1, keepdims=True)
            extra[s, e, 0:1] = told[2]
            extra[s, e, 1:2] = news[1 - e, 3, pl.ds(r, 1), :] * meet
            extra[s, e, 2:3] = decay

    def conclude(s, finals):
        kept_h = [final.astype(bf16) for final in finals]
        sums = [dot(asks[s, e], kept_h[e]) for e in range(2)]
        keep = tail_out.shape[2] - PAD
        for e in range(2):
            for j in range(sn):
                tail_out[s, e * sn + j, 0:key_rows] = kept_h[e][j * key_rows : (j + 1) * key_rows]
        words = []
        for e in range(2):
            part = sums[e][0 : 2 * PAD] + sums[e][2 * PAD : 4 * PAD] + sums[e][4 * PAD :]
            recall, retrieve, decay = part[0:1], part[PAD : PAD + 1], extra[s, e, 2:3]
            read = decay * recall + extra[s, e, 1:2] * (extra[s, e, 0:1] - decay * retrieve)
            norm = lax.rsqrt(jnp.mean(read * read, axis=-1, keepdims=True) + norm_floor)
            rest, rows = read * norm * gain_ref[...], []
            for _ in range(3):
                rows.append(rest.astype(bf16).astype(f32))
                rest = rest - rows[-1]
            words.append(jnp.concatenate(rows + [jnp.zeros((PAD - 3, extent), f32)], axis=0).astype(bf16))
        for e in range(2):
            for j in range(sn):
                tail_out[s, e * sn + j, keep:] = words[e]
        for j in range(sn):
            tail_copy(s, 1, j).start()

            @pl.when(j == me)
            def _():
                tail_in[s, own_head(s)] = tail_out[s, j]

            @pl.when(j != me)
            def _():
                tail_copy(s, 0, j).start()

    def chain_first(s):
        @pl.when(owner(s) & (team == 0))
        def _():
            if groups == 1:
                prepare(s)
            box_wait(s)
            state = [jnp.zeros((extent, extent), f32)] * 2
            for i in range(g):
                half = [a.astype(bf16) for a in state]
                for e in range(2):
                    back_out[s, e * g + i] = half[e]
                boxes_i = [in_box.at[s, e * g + i] for e in range(2)]
                if i == 0:
                    state = [b[1].astype(f32) for b in boxes_i]
                else:
                    state = [a + dot(b[0], h) + b[1].astype(f32) for a, b, h in zip(state, boxes_i, half)]
            if groups > 1:
                for e in range(2):
                    mid_out[s, e] = state[e].astype(bf16)
                mid_copy(s).start()
            if groups == 1:
                conclude(s, state)
            give_back(s)

    def compose(s):
        if groups == 1:
            return

        @pl.when(owner(s) & (team > 0))
        def _():
            prepare(s)
            box_wait(s)
            shift, drive = [None] * 2, [None] * 2
            for i in range(g):
                for e in range(2):
                    step, push = in_box[s, e * g + i, 0], in_box[s, e * g + i, 1].astype(f32)
                    if i == 0:
                        shift[e], drive[e] = step.astype(f32), push
                    else:
                        shift[e], drive[e] = (
                            shift[e] + step.astype(f32) + dot(step, shift[e].astype(bf16)),
                            drive[e] + push + dot(step, drive[e].astype(bf16)),
                        )
                    moves[s, e, i * extent : (i + 1) * extent] = shift[e].astype(bf16)
                    drives[s, e, i * extent : (i + 1) * extent] = drive[e]

    def relay(s):
        if groups == 1:
            return

        @pl.when(owner(s) & (team > 0))
        def _():
            pltpu.make_async_remote_copy(
                src_ref=mid_out.at[s], dst_ref=mid_in.at[s], send_sem=send3.at[s], recv_sem=recv3.at[s],
                device_id={"sp": lax.rem(me + sn - g, sn)}, device_id_type=MESH,
            ).wait_recv()
            start = [mid_in[s, e] for e in range(2)]
            base = [a.astype(f32) for a in start]
            top = (g - 1) * extent
            state = [base[e] + dot(moves[s, e, top:], start[e]) + drives[s, e, top:] for e in range(2)]

            @pl.when(team < groups - 1)
            def _():
                for e in range(2):
                    mid_out[s, e] = state[e].astype(bf16)
                mid_copy(s).start()

            @pl.when(team == groups - 1)
            def _():
                conclude(s, state)

            for e in range(2):
                moved = dot(moves[s, e, :top], start[e]) + drives[s, e, :top]
                back_out[s, e * g] = start[e]
                for i in range(1, g):
                    back_out[s, e * g + i] = (base[e] + moved[(i - 1) * extent : i * extent]).astype(bf16)
            give_back(s)

    def arrivals(own, ref, sem):
        if heads > 1:

            @pl.when(own)
            def _():
                settle(ref.at[pl.ds(0, heads - 1)], sem)

        @pl.when(jnp.logical_not(own))
        def _():
            settle(ref, sem)

    def finish(s):
        arrivals(owner(s), back_in.at[s], recv2.at[s])
        outs = [local_out[s, h] + dot(reach[s, h], back_in[s, h]) for h in range(heads)]
        for h in range(heads):
            o = outs[h]
            norm = lax.rsqrt(jnp.mean(o * o, axis=-1, keepdims=True) + norm_floor)
            mixed_ref[s * span : (s + 1) * span, h * extent : (h + 1) * extent] = (o * norm * gated[s, h]).astype(bf16)

    def take_tail(s):
        arrivals((team == groups - 1) & owner(s), tail_in.at[s], recv4.at[s])
        keep = tail_in.shape[2] - PAD
        for h in range(heads):
            cache_ref[s * heads + h] = tail_in[s, h, 0:key_rows]
            rows = tail_in[s, h, keep:].astype(f32)
            first_ref[s : s + 1, h * extent : (h + 1) * extent] = rows[0:1] + rows[1:2] + rows[2:3]

    for s in range(seqs):
        use_whole(0, s)
    for s in range(seqs):
        pltpu.make_async_remote_copy(
            src_ref=xs.at[partner, s], dst_ref=xs.at[partner, s], send_sem=part_sem.at[0], recv_sem=prx.at[s],
            device_id={"tp": partner}, device_id_type=MESH,
        ).wait_recv()
        use_whole(1, s)

    @pl.when(c == 1)
    def _():
        news_copy().wait_recv()

    for s in range(seqs):
        for ck in range(chunks):
            for d in range(1, chips):
                if s == 0 or ck > 0:
                    forward(d, s, ck)
                finish_chunk(d, s, ck, (1, 2) if ck == chunks - 1 else (1, 2, 0, 3))
        boxes(s)
        if s > 0:
            chain_first(s - 1)
            compose(s - 1)
        if s < seqs - 1:
            for d in range(1, chips):
                forward(d, s + 1, 0)
        for slot in range(2, tn):
            use(slot, s, chunks - 1, (0, 3))
        queries(s)
        if s > 0:
            relay(s - 1)
    compose(seqs - 1)
    chain_first(seqs - 1)
    relay(seqs - 1)
    for s in range(seqs):
        finish(s)
    settle(xs.at[tme], part_sem.at[0])
    for d in range(1, chips):
        settle(xs.at[tme], cross_sem.at[d - 1])
        settle(xs.at[tme], fwd_sem.at[d - 1])
    for s in range(seqs):
        arrivals(owner(s), out_box.at[s], send1.at[s])

        @pl.when(owner(s))
        def _():
            settle(back_out.at[s, pl.ds(0, 2 * g - 1)], send2.at[s])

            @pl.when(team < groups - 1)
            def _():
                mid_copy(s).wait_send()

            @pl.when(team == groups - 1)
            def _():
                settle(tail_out.at[s, pl.ds(0, 2 * sn - 1)], send4.at[s])

    @pl.when(c == 0)
    def _():
        news_copy().wait_send()

    for s in range(seqs):
        take_tail(s)


def fused(tn, sn, seqs, heads, tokens, weights, bw, dw, bias, rate, gain, nq, nk, nv, nb, nd):
    rows, kd = tokens.shape
    width = weights[0].shape[1]
    kc = 256 if kd % 256 == 0 else kd
    chunks, chips, span = kd // kc, tn // 2, rows // seqs
    extent = width // heads
    pairs, key_rows = seqs * heads, extent // sn
    g = group_of(sn, heads)
    tail = -(-key_rows // PAD) * PAD + PAD
    operands = (tokens, *weights, bw, dw, bias, rate, gain, nq, nk, nv, nb, nd)
    vmem = pl.BlockSpec(memory_space=pltpu.VMEM)
    hbm = pl.BlockSpec(memory_space=pltpu.HBM)
    dma = pltpu.SemaphoreType.DMA
    return pl.pallas_call(
        functools.partial(fused_kernel, tn, sn, seqs, heads),
        out_shape=(
            jax.ShapeDtypeStruct((rows, width), bf16),
            jax.ShapeDtypeStruct((pairs, key_rows, extent), bf16),
            jax.ShapeDtypeStruct((seqs, width), f32),
        ),
        in_specs=[hbm] * 15,
        out_specs=(vmem,) * 3,
        scratch_shapes=[
            pltpu.VMEM(bw.shape, bf16),
            pltpu.VMEM(dw.shape, bf16),
            pltpu.SMEM(bias.shape, f32),
            pltpu.SMEM(rate.shape, f32),
            pltpu.VMEM(gain.shape, f32),
            pltpu.VMEM(nq.shape, bf16),
            pltpu.VMEM(nk.shape, bf16),
            pltpu.VMEM(nv.shape, bf16),
            pltpu.SMEM(nb.shape, f32),
            pltpu.SMEM(nd.shape, f32),
            dma((10,)),
            pltpu.VMEM((2 * PAD, bw.shape[1]), bf16),
            pltpu.VMEM((tn, seqs, span, kd), bf16),
            pltpu.VMEM((tn, 4, kd, width), bf16),
            pltpu.VMEM((seqs, 4, span, width), f32),
            pltpu.VMEM((seqs, 2 * PAD, span), f32),
            pltpu.VMEM((seqs, PAD, span), f32),
            pltpu.VMEM((seqs, span, PAD), f32),
            pltpu.VMEM((heads, span, extent), bf16),
            pltpu.VMEM((heads, span, 2 * extent), bf16),
            pltpu.VMEM((seqs, heads, span, extent), f32),
            pltpu.VMEM((seqs, heads, span, extent), bf16),
            pltpu.VMEM((seqs, heads, span, extent), f32),
            pltpu.VMEM((seqs, heads, 2, extent, extent), bf16),
            pltpu.VMEM((seqs, 2 * g, 2, extent, extent), bf16),
            pltpu.VMEM((seqs, 2, extent, extent), bf16),
            pltpu.VMEM((seqs, 2, extent, extent), bf16),
            pltpu.VMEM((seqs, 2 * g, extent, extent), bf16),
            pltpu.VMEM((seqs, heads, extent, extent), bf16),
            pltpu.VMEM((seqs, 2 * sn, tail, extent), bf16),
            pltpu.VMEM((seqs, heads, tail, extent), bf16),
            pltpu.VMEM((seqs, 2, g * extent, extent), bf16),
            pltpu.VMEM((seqs, 2, g * extent, extent), f32),
            pltpu.VMEM((seqs, 2, 6 * PAD, extent), bf16),
            pltpu.VMEM((seqs, 2, PAD, extent), f32),
            pltpu.VMEM((2, 5, pairs, extent), f32),
            dma((2,)),
            dma((seqs,)),
            dma((tn,)),
            dma((chips - 1,)),
            dma((1,)),
            dma((chips - 1,)),
            dma((chips - 1, 2, seqs, chunks)),
            dma((seqs,)),
            dma((seqs,)),
            dma((seqs,)),
            dma((seqs,)),
            dma((seqs,)),
            dma((seqs,)),
            dma((seqs,)),
            dma((seqs,)),
            dma((seqs,)),
            pltpu.SemaphoreType.REGULAR,
        ],
        compiler_params=pltpu.CompilerParams(
            collective_id=0, has_side_effects=True, vmem_limit_bytes=53 * 1024 * 1024
        ),
    )(*[pltpu.with_memory_space_constraint(a, pltpu.HBM) for a in operands])


def emit_kernel(mixed_ref, cache_ref, first_ref, mixed_out, cache_out, first_out, sem):
    copies = [
        pltpu.make_async_copy(a, b, sem.at[i])
        for i, (a, b) in enumerate(((mixed_ref, mixed_out), (cache_ref, cache_out), (first_ref, first_out)))
    ]
    for copy in copies:
        copy.start()
    for copy in copies:
        copy.wait()


def emit(*results):
    return pl.pallas_call(
        emit_kernel,
        out_shape=tuple(jax.ShapeDtypeStruct(r.shape, r.dtype) for r in results),
        in_specs=[pl.BlockSpec(memory_space=pltpu.VMEM)] * 3,
        out_specs=(pl.BlockSpec(memory_space=pltpu.HBM),) * 3,
        scratch_shapes=[pltpu.SemaphoreType.DMA((3,))],
        compiler_params=pltpu.CompilerParams(vmem_limit_bytes=4 * 1024 * 1024),
    )(*results)


def shards(
    tokens, query_weight, key_weight, value_weight, gate_weight, beta_weight, decay_weight,
    beta_bias, rate_log, out_gain, new_query, new_key, new_value, new_beta, new_decay,
):
    seqs, span, kd = tokens.shape
    heads = rate_log.shape[0]
    extent = out_gain.shape[0]
    tp, sp = lax.axis_size("tp"), lax.axis_size("sp")
    weights = (query_weight, key_weight, value_weight, gate_weight)
    mixed, cache, first = fused(
        tp, sp, seqs, heads, tokens.reshape(seqs * span, kd), weights, beta_weight.T, decay_weight.T, beta_bias,
        rate_log, out_gain[None], new_query, new_key, new_value, new_beta, new_decay,
    )
    return emit(
        mixed.reshape(seqs, span, heads * extent), cache.reshape(seqs, heads, extent // sp, extent), first
    )


def solution(mesh):
    placed = (
        P(None, "sp", "tp"),
        P(None, "tp"),
        P(None, "tp"),
        P(None, "tp"),
        P(None, "tp"),
        P(None, "tp"),
        P(None, "tp"),
        P("tp"),
        P("tp"),
        P(),
        P(None, "tp", None),
        P(None, "tp", None),
        P(None, "tp", None),
        P(None, "tp"),
        P(None, "tp"),
    )
    return jax.shard_map(
        shards,
        mesh=mesh,
        in_specs=placed,
        out_specs=(P(None, "sp", "tp"), P(None, "tp", "sp", None), P(None, "tp")),
        check_vma=False,
    )
```

```python
import functools

import jax
import jax.numpy as jnp
from jax import lax
from jax.experimental import pallas as pl
from jax.experimental.pallas import tpu as pltpu
from jax.sharding import PartitionSpec as P

unit_floor = 1.0
norm_floor = 0.001
highest = lax.Precision.HIGHEST
MESH = pl.DeviceIdType.MESH
PAD = 8
INNER, OUTER = 8, 64
f32 = jnp.float32
bf16 = jnp.bfloat16

NN = (((1,), (0,)), ((), ()))
NT = (((1,), (1,)), ((), ()))
TN = (((0,), (0,)), ((), ()))


def dot(left, right, dims=NN, precision=None):
    return lax.dot_general(left, right, dims, precision=precision, preferred_element_type=f32)


def unit_rows(values):
    return values * lax.rsqrt(jnp.sum(values * values, axis=-1, keepdims=True) + unit_floor)


def group_of(n, heads):
    g = 1
    while g < n and (g < heads or g * g < n):
        g *= 2
    return g


def fused_kernel(
    tn, sn, seqs, heads, x_ref, wq_ref, wk_ref, wv_ref, wg_ref, bw_hbm, dw_hbm, bias_hbm, rate_hbm, gain_hbm,
    nq_hbm, nk_hbm, nv_hbm, nb_hbm, nd_hbm, mixed_ref, cache_ref, first_ref,
    bw_ref, dw_ref, bias_ref, rate_ref, gain_ref, nq_ref, nk_ref, nv_ref, nb_ref, nd_ref, small_sem,
    bd, xs, wbuf, acc, sacc, cum_row, cum_col, kh_buf, uw_buf, local_out, reach, gated,
    out_box, in_box, mid_out, mid_in, back_out, back_in, tail_out, tail_in, moves, drives, asks, extra, news, news_sem,
    xsem, wsem, cross_sem, part_sem, fwd_sem, rx, prx,
    send1, recv1, send2, recv2, send3, recv3, send4, recv4, hello,
):
    _, _, span, kd = xs.shape
    width = wq_ref.shape[1]
    extent = width // heads
    key_rows = extent // sn
    chunks = rx.shape[3]
    kc = kd // chunks
    tme, me = lax.axis_index("tp"), lax.axis_index("sp")
    y, c = tme // 2, lax.rem(tme, 2)
    chips = tn // 2
    partner = y * 2 + (1 - c)
    g = group_of(sn, heads)
    groups = sn // g
    team, m = me // g, lax.rem(me, g)
    weights = (wq_ref, wk_ref, wv_ref, wg_ref)

    barrier = pltpu.get_barrier_semaphore()
    pl.semaphore_signal(barrier, inc=1, device_id={"tp": partner}, device_id_type=MESH)
    for d in range(1, chips):
        to = lax.rem(y + d, chips) * 2 + c
        pl.semaphore_signal(barrier, inc=1, device_id={"tp": to}, device_id_type=MESH)
    for d in range(1, sn):

        @pl.when(me + d < sn)
        def _():
            for t in (tme, partner):
                pl.semaphore_signal(barrier, inc=1, device_id={"sp": me + d, "tp": t}, device_id_type=MESH)

    order = [tme, partner]
    for d in range(1, chips):
        source = lax.rem(y - d + chips, chips)
        order += [source * 2 + c, source * 2 + (1 - c)]

    def cols(ck):
        return pl.ds(ck * kc, kc)

    def token_copy(s):
        return pltpu.make_async_copy(x_ref.at[pl.ds(s * span, span), :], xs.at[tme, s], xsem.at[s])

    def weight_copy(w, slot):
        start = pl.multiple_of(order[slot] * kd, kd)
        return pltpu.make_async_copy(
            weights[w].at[pl.ds(start, kd), :], wbuf.at[slot, w], wsem.at[slot]
        )

    small_copies = [
        pltpu.make_async_copy(a, b, small_sem.at[i])
        for i, (a, b) in enumerate(
            (
                (bw_hbm, bw_ref), (dw_hbm, dw_ref), (bias_hbm, bias_ref), (rate_hbm, rate_ref), (gain_hbm, gain_ref),
                (nq_hbm, nq_ref), (nk_hbm, nk_ref), (nv_hbm, nv_ref), (nb_hbm, nb_ref), (nd_hbm, nd_ref),
            )
        )
    ]
    for s in range(seqs):
        token_copy(s).start()
    for copy in small_copies:
        copy.start()
    pl.semaphore_wait(barrier, chips + 2 * me)

    def cross_copy(d, s, ck):
        to = lax.rem(y + d, chips) * 2 + c
        return pltpu.make_async_remote_copy(
            src_ref=xs.at[tme, s, :, cols(ck)], dst_ref=xs.at[tme, s, :, cols(ck)],
            send_sem=cross_sem.at[d - 1], recv_sem=rx.at[d - 1, 0, s, ck],
            device_id={"tp": to}, device_id_type=MESH,
        )

    def part_copy(s):
        return pltpu.make_async_remote_copy(
            src_ref=xs.at[tme, s], dst_ref=xs.at[tme, s],
            send_sem=part_sem.at[0], recv_sem=prx.at[s],
            device_id={"tp": partner}, device_id_type=MESH,
        )

    for s in range(seqs):
        token_copy(s).wait()
        for ck in range(chunks):
            for d in range(1, chips):
                cross_copy(d, s, ck).start()
        part_copy(s).start()
    for slot in range(tn):
        for w in range(4):
            weight_copy(w, slot).start()
    for d in range(1, sn):

        @pl.when(me >= d)
        def _():
            for t in (tme, partner):
                pl.semaphore_signal(hello, inc=1, device_id={"sp": me - d, "tp": t}, device_id_type=MESH)

    for copy in small_copies:
        copy.wait()
    for s in range(seqs):
        for i, ref in enumerate((nq_ref, nk_ref, nv_ref)):
            news[c, i, s * heads : (s + 1) * heads] = ref[s].astype(f32)
        for i, ref in enumerate((nb_ref, nd_ref)):
            for h in range(heads):
                news[c, 3 + i, s * heads + h : s * heads + h + 1] = jnp.full((1, extent), ref[s, h], f32)

    def news_copy():
        return pltpu.make_async_remote_copy(
            src_ref=news.at[0], dst_ref=news.at[0], send_sem=news_sem.at[0], recv_sem=news_sem.at[1],
            device_id={"tp": partner}, device_id_type=MESH,
        )

    @pl.when(c == 0)
    def _():
        news_copy().start()

    bd[...] = jnp.zeros_like(bd)
    bd[0 : bw_ref.shape[0]] = bw_ref[...]
    bd[PAD : PAD + dw_ref.shape[0]] = dw_ref[...]
    row = lax.broadcasted_iota(jnp.int32, (span, span), 0)
    col = lax.broadcasted_iota(jnp.int32, (span, span), 1)
    slot_of = lax.broadcasted_iota(jnp.int32, (PAD, 1), 0)
    bias = jnp.zeros((PAD, 1), f32)
    rate = jnp.zeros((PAD, 1), f32)
    for h in range(heads):
        bias = jnp.where(slot_of == h, bias_ref[h], bias)
        rate = jnp.where(slot_of == h, rate_ref[h], rate)

    def fwd_copy(d, s, ck):
        b = order[2 * d]
        return pltpu.make_async_remote_copy(
            src_ref=xs.at[b, s, :, cols(ck)], dst_ref=xs.at[b, s, :, cols(ck)],
            send_sem=fwd_sem.at[d - 1], recv_sem=rx.at[d - 1, 1, s, ck],
            device_id={"tp": partner}, device_id_type=MESH,
        )

    def arrive(d, side, s, ck):
        b = order[2 * d + side]
        pltpu.make_async_remote_copy(
            src_ref=xs.at[b, s, :, cols(ck)], dst_ref=xs.at[b, s, :, cols(ck)],
            send_sem=part_sem.at[0], recv_sem=rx.at[d - 1, side, s, ck],
            device_id={"tp": partner}, device_id_type=MESH,
        ).wait_recv()

    def small(x, start, depth, s, first):
        piece = bd[:, pl.ds(pl.multiple_of(start, depth), depth)]
        term = dot(piece, x, NT)
        sacc[s] = term if first else sacc[s] + term

    def use_whole(slot, s):
        b = order[slot]
        x = xs[b, s]
        if s == 0:
            weights_wait(slot)
        for w in range(4):
            term = dot(x, wbuf[slot, w])
            acc[s, w] = term if slot == 0 else acc[s, w] + term
        small(x, b * kd, kd, s, slot == 0)

    def weights_wait(slot):
        pltpu.make_async_copy(wbuf.at[slot], wbuf.at[slot], wsem.at[slot]).wait()

    def use(slot, s, ck, parts=(1, 2, 0, 3)):
        b = order[slot]
        x = xs[b, s, :, cols(ck)]
        if 1 in parts:
            if s == 0 and ck == 0:
                weights_wait(slot)
            small(x, b * kd + ck * kc, kc, s, False)
        for w in parts:
            acc[s, w] += dot(x, wbuf[slot, w, cols(ck), :])

    def forward(d, s, ck):
        arrive(d, 0, s, ck)
        fwd_copy(d, s, ck).start()

    def finish_chunk(d, s, ck, parts):
        use(2 * d, s, ck, parts)
        arrive(d, 1, s, ck)
        use(2 * d + 1, s, ck, parts)

    def heads_of(w, s):
        return [acc[s, w, :, h * extent : (h + 1) * extent].astype(bf16).astype(f32) for h in range(heads)]

    def owner_of(s, h):
        return (s * heads + h) % g

    def box_copy(s, h, to):
        return pltpu.make_async_remote_copy(
            src_ref=out_box.at[s, h], dst_ref=in_box.at[s, (1 - c) * g + m],
            send_sem=send1.at[s], recv_sem=recv1.at[s],
            device_id={"sp": team * g + to, "tp": y * 2 + 1}, device_id_type=MESH,
        )

    def boxes(s):
        beta = jax.nn.sigmoid(sacc[s, 0:PAD, :] + bias)
        pre = sacc[s, PAD : 2 * PAD, :]
        soft = jnp.maximum(pre, 0.0) + jnp.log1p(jnp.exp(-jnp.abs(pre)))
        upper = jnp.where(row <= col, 1.0, 0.0).astype(bf16)
        rest, pieces = -jnp.exp(rate) * soft, []
        for _ in range(3):
            pieces.append(rest.astype(bf16).astype(f32))
            rest = rest - pieces[-1]
        sums = dot(jnp.concatenate(pieces, axis=0).astype(bf16), upper)
        cum = sums[0:PAD] + sums[PAD : 2 * PAD] + sums[2 * PAD :]
        cum_t, beta_t = cum.T, beta.T
        cum_row[s] = cum
        cum_col[s] = cum_t
        hs, bs = range(heads), range(span // OUTER)
        line = lax.broadcasted_iota(jnp.int32, (OUTER, 2 * OUTER), 0)
        lane = lax.broadcasted_iota(jnp.int32, (OUTER, 2 * OUTER), 1)
        high = lane >= OUTER
        place = lane % OUTER
        same = line // INNER == place // INNER
        fill = jnp.zeros((OUTER, 2 * OUTER), bf16)
        unit = jnp.where(line == place, 1.0, 0.0)

        def part(b):
            return slice(b * OUTER, (b + 1) * OUTER)

        twice = [jnp.concatenate([cum[:, part(b)]] * 2, axis=1) for b in bs]
        k = [unit_rows(v) for v in heads_of(1, s)]
        kh = [v.astype(bf16) for v in k]
        pairs = [(h, b) for h in hs for b in bs]
        kk = [dot(kh[h][part(b)], jnp.concatenate([kh[h][part(b)]] * 2, axis=0), NT) for h, b in pairs]
        far = {(h, b): dot(kh[h][part(b)], kh[h][: b * OUTER], NT) for h, b in pairs if b > 0}
        right, kdec, last, low = [], [], [], []
        v = heads_of(2, s)
        for h in hs:
            cumc, bt = cum_t[:, h : h + 1], beta_t[:, h : h + 1]
            kh_buf[h] = kh[h]
            for b in bs:
                here = cumc[part(b)]
                wts = bt[part(b)] * jnp.exp(jnp.where(line >= place, here - twice[b][h : h + 1, :], 0.0))
                low.append(jnp.where(line > place, kk[h * len(bs) + b] * wts, 0.0))
                if b > 0:
                    wts = bt[part(b)] * jnp.exp(here - cum[h : h + 1, : b * OUTER])
                    far[h, b] = (far[h, b] * wts).astype(bf16)
            kb = k[h] * bt
            right.append(jnp.concatenate([v[h] * bt, kb * jnp.exp(cumc)], axis=1).astype(bf16))
            end = cumc[span - 1 :, :]
            kdec.append((k[h] * jnp.exp(end - cumc)).astype(bf16))
            last.append(jnp.exp(end))

        def climb(block):
            half = block.astype(bf16)
            return dot(half[:, :OUTER], half)

        z = [jnp.where(high, unit - n, n) for n in (jnp.where(same, m, 0.0) for m in low)]
        z = [jnp.where(high, a, climb(a)) for a in z]
        reached = 2
        while reached < INNER:
            z = [climb(a) + jnp.where(high, a, 0.0) for a in z]
            reached *= 2
        under = [jnp.concatenate([fill, jnp.where(high | same, 0.0, m).astype(bf16)], axis=0) for m in low]
        z = [a + dot(a.astype(bf16), u) for a, u in zip(z, under)]
        z = [jnp.where(high, a - t, t) for a, t in ((a, climb(a)) for a in z)]
        reached = 2
        while reached < OUTER // INNER:
            z = [climb(a) + jnp.where(high, a, 0.0) for a in z]
            reached *= 2
        inv = {p: a.astype(bf16) for p, a in zip(pairs, z)}
        none = jnp.zeros((OUTER, 2 * extent), bf16)
        term = {(h, b): dot(inv[h, b], jnp.concatenate([none, right[h][part(b)]], axis=0)) for h, b in pairs}
        far = {
            (h, b): dot(inv[h, b], jnp.concatenate([jnp.zeros_like(m), m], axis=0)).astype(bf16)
            for (h, b), m in far.items()
        }
        done = [[term[h, 0].astype(bf16)] for h in hs]
        for b in bs[1:]:
            for h in hs:
                seen = jnp.concatenate(done[h], axis=0) if b > 1 else done[h][0]
                done[h].append((term[h, b] - dot(far[h, b], seen)).astype(bf16))
        uw = [jnp.concatenate(d, axis=0) for d in done]
        z = [dot(a, u, TN) for a, u in zip(kdec, uw)]
        eye = lax.broadcasted_iota(jnp.int32, (extent, extent), 0) == lax.broadcasted_iota(
            jnp.int32, (extent, extent), 1
        )
        for h in hs:
            out_box[s, h, 0] = (jnp.where(eye, last[h] - 1.0, 0.0) - z[h][:, extent:]).astype(bf16)
            out_box[s, h, 1] = z[h][:, :extent].astype(bf16)
            uw_buf[h] = uw[h]
        if s == 0:

            @pl.when(me < sn - 1)
            def _():
                pl.semaphore_wait(hello, 2 * (sn - 1 - me))

        for r in reversed(range(g)):
            to = m
            for bit in (b for b in (1 << i for i in range(g.bit_length())) if r & b):
                to = to + bit * (1 - 2 * lax.rem(m // bit, 2))
            h = lax.rem(to + g - (s * heads) % g, g)
            if r == 0:

                @pl.when((h < heads) & (c == 1))
                def _():
                    in_box[s, m] = out_box[s, h]

            @pl.when((h < heads) & ((c == 0) | (r > 0)))
            def _():
                box_copy(s, h, to).start()

    def queries(s):
        cum, cum_t = cum_row[s], cum_col[s]
        gain = gain_ref[...]
        hs = range(heads)
        causal = row >= col

        def spread(h):
            gap = jnp.where(causal, cum_t[:, h : h + 1] - cum[h : h + 1, :], 0.0)
            return jnp.where(causal, jnp.exp(gap), 0.0)

        q = [unit_rows(v) for v in heads_of(0, s)]
        scores = [(dot(q[h].astype(bf16), kh_buf[h], NT) * spread(h)).astype(bf16) for h in hs]
        out = [dot(scores[h], uw_buf[h]) for h in hs]
        gates = heads_of(3, s)
        for h in hs:
            local_out[s, h] = out[h][:, :extent]
            reach[s, h] = (q[h] * jnp.exp(cum_t[:, h : h + 1]) - out[h][:, extent:]).astype(bf16)
            gated[s, h] = gates[h] * jax.nn.sigmoid(gates[h]) * gain

    def own_head(s):
        return lax.rem(m + g - (s * heads) % g, g)

    def owner(s):
        return (own_head(s) < heads) & (c == 1)

    def back_copy(s, e, i):
        return pltpu.make_async_remote_copy(
            src_ref=back_out.at[s, e * g + i], dst_ref=back_in.at[s, own_head(s)],
            send_sem=send2.at[s], recv_sem=recv2.at[s],
            device_id={"sp": team * g + i, "tp": y * 2 + 1 - e}, device_id_type=MESH,
        )

    def mid_copy(s):
        return pltpu.make_async_remote_copy(
            src_ref=mid_out.at[s], dst_ref=mid_in.at[s], send_sem=send3.at[s], recv_sem=recv3.at[s],
            device_id={"sp": lax.rem(me + g, sn)}, device_id_type=MESH,
        )

    def tail_copy(s, e, j):
        return pltpu.make_async_remote_copy(
            src_ref=tail_out.at[s, e * sn + j], dst_ref=tail_in.at[s, own_head(s)],
            send_sem=send4.at[s], recv_sem=recv4.at[s],
            device_id={"sp": j, "tp": y * 2 + 1 - e}, device_id_type=MESH,
        )

    def settle(ref, sem):
        pltpu.make_async_copy(ref, ref, sem).wait()

    def box_wait(s):
        settle(in_box.at[s, pl.ds(0, 2 * g - 1)], recv1.at[s])

    def give_back(s):
        for i in range(g):
            back_copy(s, 1, i).start()

            @pl.when(i == m)
            def _():
                back_in[s, own_head(s)] = back_out[s, i]

            @pl.when(i != m)
            def _():
                back_copy(s, 0, i).start()

    def prepare(s):
        r = s * heads + own_head(s)
        for e in range(2):
            told = [news[1 - e, i, pl.ds(r, 1), :] for i in range(3)]
            qn, kn = unit_rows(told[0]), unit_rows(told[1])
            rest = jnp.concatenate([jnp.broadcast_to(qn, (PAD, extent)), jnp.broadcast_to(kn, (PAD, extent))], axis=0)
            for i in range(3):
                piece = rest.astype(bf16)
                asks[s, e, i * 2 * PAD : (i + 1) * 2 * PAD] = piece
                rest = rest - piece.astype(f32)
            decay, meet = news[1 - e, 4, pl.ds(r, 1), :], jnp.sum(kn * qn, axis=-1, keepdims=True)
            extra[s, e, 0:1] = told[2]
            extra[s, e, 1:2] = news[1 - e, 3, pl.ds(r, 1), :] * meet
            extra[s, e, 2:3] = decay

    def conclude(s, finals):
        kept_h = [final.astype(bf16) for final in finals]
        sums = [dot(asks[s, e], kept_h[e]) for e in range(2)]
        keep = tail_out.shape[2] - PAD
        for e in range(2):
            for j in range(sn):
                tail_out[s, e * sn + j, 0:key_rows] = kept_h[e][j * key_rows : (j + 1) * key_rows]
        words = []
        for e in range(2):
            part = sums[e][0 : 2 * PAD] + sums[e][2 * PAD : 4 * PAD] + sums[e][4 * PAD :]
            recall, retrieve, decay = part[0:1], part[PAD : PAD + 1], extra[s, e, 2:3]
            read = decay * recall + extra[s, e, 1:2] * (extra[s, e, 0:1] - decay * retrieve)
            norm = lax.rsqrt(jnp.mean(read * read, axis=-1, keepdims=True) + norm_floor)
            rest, rows = read * norm * gain_ref[...], []
            for _ in range(3):
                rows.append(rest.astype(bf16).astype(f32))
                rest = rest - rows[-1]
            words.append(jnp.concatenate(rows + [jnp.zeros((PAD - 3, extent), f32)], axis=0).astype(bf16))
        for e in range(2):
            for j in range(sn):
                tail_out[s, e * sn + j, keep:] = words[e]
        for j in range(sn):
            tail_copy(s, 1, j).start()

            @pl.when(j == me)
            def _():
                tail_in[s, own_head(s)] = tail_out[s, j]

            @pl.when(j != me)
            def _():
                tail_copy(s, 0, j).start()

    def chain_first(s):
        @pl.when(owner(s) & (team == 0))
        def _():
            if groups == 1:
                prepare(s)
            box_wait(s)
            state = [jnp.zeros((extent, extent), f32)] * 2
            for i in range(g):
                half = [a.astype(bf16) for a in state]
                for e in range(2):
                    back_out[s, e * g + i] = half[e]
                boxes_i = [in_box.at[s, e * g + i] for e in range(2)]
                if i == 0:
                    state = [b[1].astype(f32) for b in boxes_i]
                else:
                    state = [a + dot(b[0], h) + b[1].astype(f32) for a, b, h in zip(state, boxes_i, half)]
            if groups > 1:
                for e in range(2):
                    mid_out[s, e] = state[e].astype(bf16)
                mid_copy(s).start()
            if groups == 1:
                conclude(s, state)
            give_back(s)

    def compose(s):
        if groups == 1:
            return

        @pl.when(owner(s) & (team > 0))
        def _():
            prepare(s)
            box_wait(s)
            shift, drive = [None] * 2, [None] * 2
            for i in range(g):
                for e in range(2):
                    step, push = in_box[s, e * g + i, 0], in_box[s, e * g + i, 1].astype(f32)
                    if i == 0:
                        shift[e], drive[e] = step.astype(f32), push
                    else:
                        shift[e], drive[e] = (
                            shift[e] + step.astype(f32) + dot(step, shift[e].astype(bf16)),
                            drive[e] + push + dot(step, drive[e].astype(bf16)),
                        )
                    moves[s, e, i * extent : (i + 1) * extent] = shift[e].astype(bf16)
                    drives[s, e, i * extent : (i + 1) * extent] = drive[e]

    def relay(s):
        if groups == 1:
            return

        @pl.when(owner(s) & (team > 0))
        def _():
            pltpu.make_async_remote_copy(
                src_ref=mid_out.at[s], dst_ref=mid_in.at[s], send_sem=send3.at[s], recv_sem=recv3.at[s],
                device_id={"sp": lax.rem(me + sn - g, sn)}, device_id_type=MESH,
            ).wait_recv()
            start = [mid_in[s, e] for e in range(2)]
            base = [a.astype(f32) for a in start]
            top = (g - 1) * extent
            state = [base[e] + dot(moves[s, e, top:], start[e]) + drives[s, e, top:] for e in range(2)]

            @pl.when(team < groups - 1)
            def _():
                for e in range(2):
                    mid_out[s, e] = state[e].astype(bf16)
                mid_copy(s).start()

            @pl.when(team == groups - 1)
            def _():
                conclude(s, state)

            for e in range(2):
                moved = dot(moves[s, e, :top], start[e]) + drives[s, e, :top]
                back_out[s, e * g] = start[e]
                for i in range(1, g):
                    back_out[s, e * g + i] = (base[e] + moved[(i - 1) * extent : i * extent]).astype(bf16)
            give_back(s)

    def arrivals(own, ref, sem):
        if heads > 1:

            @pl.when(own)
            def _():
                settle(ref.at[pl.ds(0, heads - 1)], sem)

        @pl.when(jnp.logical_not(own))
        def _():
            settle(ref, sem)

    def finish(s):
        arrivals(owner(s), back_in.at[s], recv2.at[s])
        outs = [local_out[s, h] + dot(reach[s, h], back_in[s, h]) for h in range(heads)]
        for h in range(heads):
            o = outs[h]
            norm = lax.rsqrt(jnp.mean(o * o, axis=-1, keepdims=True) + norm_floor)
            mixed_ref[s * span : (s + 1) * span, h * extent : (h + 1) * extent] = (o * norm * gated[s, h]).astype(bf16)

    def take_tail(s):
        arrivals((team == groups - 1) & owner(s), tail_in.at[s], recv4.at[s])
        keep = tail_in.shape[2] - PAD
        for h in range(heads):
            cache_ref[s * heads + h] = tail_in[s, h, 0:key_rows]
            rows = tail_in[s, h, keep:].astype(f32)
            first_ref[s : s + 1, h * extent : (h + 1) * extent] = rows[0:1] + rows[1:2] + rows[2:3]

    def apart(step, *args):
        @pl.when(me >= 0)
        def _():
            step(*args)

    for s in range(seqs):
        use_whole(0, s)
    for s in range(seqs):
        pltpu.make_async_remote_copy(
            src_ref=xs.at[partner, s], dst_ref=xs.at[partner, s], send_sem=part_sem.at[0], recv_sem=prx.at[s],
            device_id={"tp": partner}, device_id_type=MESH,
        ).wait_recv()
        use_whole(1, s)

    @pl.when(c == 1)
    def _():
        news_copy().wait_recv()

    for s in range(seqs):
        for ck in range(chunks):
            for d in range(1, chips):
                if s == 0 or ck > 0:
                    forward(d, s, ck)
                finish_chunk(d, s, ck, (1, 2) if ck == chunks - 1 else (1, 2, 0, 3))
        apart(boxes, s)
        if s > 0:
            chain_first(s - 1)
            compose(s - 1)
        if s < seqs - 1:
            for d in range(1, chips):
                forward(d, s + 1, 0)
        for slot in range(2, tn):
            use(slot, s, chunks - 1, (0, 3))
        queries(s)
        if s > 0:
            relay(s - 1)
    compose(seqs - 1)
    chain_first(seqs - 1)
    relay(seqs - 1)
    for s in range(seqs):
        finish(s)
    settle(xs.at[tme], part_sem.at[0])
    for d in range(1, chips):
        settle(xs.at[tme], cross_sem.at[d - 1])
        settle(xs.at[tme], fwd_sem.at[d - 1])
    for s in range(seqs):
        arrivals(owner(s), out_box.at[s], send1.at[s])

        @pl.when(owner(s))
        def _():
            settle(back_out.at[s, pl.ds(0, 2 * g - 1)], send2.at[s])

            @pl.when(team < groups - 1)
            def _():
                mid_copy(s).wait_send()

            @pl.when(team == groups - 1)
            def _():
                settle(tail_out.at[s, pl.ds(0, 2 * sn - 1)], send4.at[s])

    @pl.when(c == 0)
    def _():
        news_copy().wait_send()

    for s in range(seqs):
        take_tail(s)


def fused(tn, sn, seqs, heads, tokens, weights, bw, dw, bias, rate, gain, nq, nk, nv, nb, nd):
    rows, kd = tokens.shape
    width = weights[0].shape[1]
    kc = 256 if kd % 256 == 0 else kd
    chunks, chips, span = kd // kc, tn // 2, rows // seqs
    extent = width // heads
    pairs, key_rows = seqs * heads, extent // sn
    g = group_of(sn, heads)
    tail = -(-key_rows // PAD) * PAD + PAD
    operands = (tokens, *weights, bw, dw, bias, rate, gain, nq, nk, nv, nb, nd)
    vmem = pl.BlockSpec(memory_space=pltpu.VMEM)
    hbm = pl.BlockSpec(memory_space=pltpu.HBM)
    dma = pltpu.SemaphoreType.DMA
    return pl.pallas_call(
        functools.partial(fused_kernel, tn, sn, seqs, heads),
        out_shape=(
            jax.ShapeDtypeStruct((rows, width), bf16),
            jax.ShapeDtypeStruct((pairs, key_rows, extent), bf16),
            jax.ShapeDtypeStruct((seqs, width), f32),
        ),
        in_specs=[hbm] * 15,
        out_specs=(vmem,) * 3,
        scratch_shapes=[
            pltpu.VMEM(bw.shape, bf16),
            pltpu.VMEM(dw.shape, bf16),
            pltpu.SMEM(bias.shape, f32),
            pltpu.SMEM(rate.shape, f32),
            pltpu.VMEM(gain.shape, f32),
            pltpu.VMEM(nq.shape, bf16),
            pltpu.VMEM(nk.shape, bf16),
            pltpu.VMEM(nv.shape, bf16),
            pltpu.SMEM(nb.shape, f32),
            pltpu.SMEM(nd.shape, f32),
            dma((10,)),
            pltpu.VMEM((2 * PAD, bw.shape[1]), bf16),
            pltpu.VMEM((tn, seqs, span, kd), bf16),
            pltpu.VMEM((tn, 4, kd, width), bf16),
            pltpu.VMEM((seqs, 4, span, width), f32),
            pltpu.VMEM((seqs, 2 * PAD, span), f32),
            pltpu.VMEM((seqs, PAD, span), f32),
            pltpu.VMEM((seqs, span, PAD), f32),
            pltpu.VMEM((heads, span, extent), bf16),
            pltpu.VMEM((heads, span, 2 * extent), bf16),
            pltpu.VMEM((seqs, heads, span, extent), f32),
            pltpu.VMEM((seqs, heads, span, extent), bf16),
            pltpu.VMEM((seqs, heads, span, extent), f32),
            pltpu.VMEM((seqs, heads, 2, extent, extent), bf16),
            pltpu.VMEM((seqs, 2 * g, 2, extent, extent), bf16),
            pltpu.VMEM((seqs, 2, extent, extent), bf16),
            pltpu.VMEM((seqs, 2, extent, extent), bf16),
            pltpu.VMEM((seqs, 2 * g, extent, extent), bf16),
            pltpu.VMEM((seqs, heads, extent, extent), bf16),
            pltpu.VMEM((seqs, 2 * sn, tail, extent), bf16),
            pltpu.VMEM((seqs, heads, tail, extent), bf16),
            pltpu.VMEM((seqs, 2, g * extent, extent), bf16),
            pltpu.VMEM((seqs, 2, g * extent, extent), f32),
            pltpu.VMEM((seqs, 2, 6 * PAD, extent), bf16),
            pltpu.VMEM((seqs, 2, PAD, extent), f32),
            pltpu.VMEM((2, 5, pairs, extent), f32),
            dma((2,)),
            dma((seqs,)),
            dma((tn,)),
            dma((chips - 1,)),
            dma((1,)),
            dma((chips - 1,)),
            dma((chips - 1, 2, seqs, chunks)),
            dma((seqs,)),
            dma((seqs,)),
            dma((seqs,)),
            dma((seqs,)),
            dma((seqs,)),
            dma((seqs,)),
            dma((seqs,)),
            dma((seqs,)),
            dma((seqs,)),
            pltpu.SemaphoreType.REGULAR,
        ],
        compiler_params=pltpu.CompilerParams(
            collective_id=0, has_side_effects=True, vmem_limit_bytes=53 * 1024 * 1024
        ),
    )(*[pltpu.with_memory_space_constraint(a, pltpu.HBM) for a in operands])


def emit_kernel(mixed_ref, cache_ref, first_ref, mixed_out, cache_out, first_out, sem):
    copies = [
        pltpu.make_async_copy(a, b, sem.at[i])
        for i, (a, b) in enumerate(((mixed_ref, mixed_out), (cache_ref, cache_out), (first_ref, first_out)))
    ]
    for copy in copies:
        copy.start()
    for copy in copies:
        copy.wait()


def emit(*results):
    return pl.pallas_call(
        emit_kernel,
        out_shape=tuple(jax.ShapeDtypeStruct(r.shape, r.dtype) for r in results),
        in_specs=[pl.BlockSpec(memory_space=pltpu.VMEM)] * 3,
        out_specs=(pl.BlockSpec(memory_space=pltpu.HBM),) * 3,
        scratch_shapes=[pltpu.SemaphoreType.DMA((3,))],
        compiler_params=pltpu.CompilerParams(vmem_limit_bytes=4 * 1024 * 1024),
    )(*results)


def shards(
    tokens, query_weight, key_weight, value_weight, gate_weight, beta_weight, decay_weight,
    beta_bias, rate_log, out_gain, new_query, new_key, new_value, new_beta, new_decay,
):
    seqs, span, kd = tokens.shape
    heads = rate_log.shape[0]
    extent = out_gain.shape[0]
    tp, sp = lax.axis_size("tp"), lax.axis_size("sp")
    weights = (query_weight, key_weight, value_weight, gate_weight)
    mixed, cache, first = fused(
        tp, sp, seqs, heads, tokens.reshape(seqs * span, kd), weights, beta_weight.T, decay_weight.T, beta_bias,
        rate_log, out_gain[None], new_query, new_key, new_value, new_beta, new_decay,
    )
    return emit(
        mixed.reshape(seqs, span, heads * extent), cache.reshape(seqs, heads, extent // sp, extent), first
    )


def solution(mesh):
    placed = (
        P(None, "sp", "tp"),
        P(None, "tp"),
        P(None, "tp"),
        P(None, "tp"),
        P(None, "tp"),
        P(None, "tp"),
        P(None, "tp"),
        P("tp"),
        P("tp"),
        P(),
        P(None, "tp", None),
        P(None, "tp", None),
        P(None, "tp", None),
        P(None, "tp"),
        P(None, "tp"),
    )
    return jax.shard_map(
        shards,
        mesh=mesh,
        in_specs=placed,
        out_specs=(P(None, "sp", "tp"), P(None, "tp", "sp", None), P(None, "tp")),
        check_vma=False,
    )
```

```python
import functools

import jax
import jax.numpy as jnp
from jax import lax
from jax.experimental import pallas as pl
from jax.experimental.pallas import tpu as pltpu
from jax.sharding import PartitionSpec as P

unit_floor = 1.0
norm_floor = 0.001
highest = lax.Precision.HIGHEST
MESH = pl.DeviceIdType.MESH
PAD = 8
INNER, OUTER = 8, 64
f32 = jnp.float32
bf16 = jnp.bfloat16

NN = (((1,), (0,)), ((), ()))
NT = (((1,), (1,)), ((), ()))
TN = (((0,), (0,)), ((), ()))


def dot(left, right, dims=NN, precision=None):
    return lax.dot_general(left, right, dims, precision=precision, preferred_element_type=f32)


def unit_rows(values):
    return values * lax.rsqrt(jnp.sum(values * values, axis=-1, keepdims=True) + unit_floor)


def group_of(n, heads):
    g = 1
    while g < n and (g < heads or g * g < n):
        g *= 2
    return g


def fused_kernel(
    tn, sn, seqs, heads, x_ref, wq_ref, wk_ref, wv_ref, wg_ref, bw_hbm, dw_hbm, bias_hbm, rate_hbm, gain_hbm,
    nq_hbm, nk_hbm, nv_hbm, nb_hbm, nd_hbm, mixed_ref, cache_ref, first_ref,
    bw_ref, dw_ref, bias_ref, rate_ref, gain_ref, nq_ref, nk_ref, nv_ref, nb_ref, nd_ref, small_sem,
    bd, xs, wbuf, acc, sacc, cum_row, cum_col, kh_buf, uw_buf, local_out, reach, gated,
    out_box, in_box, mid_out, mid_in, back_out, back_in, tail_out, tail_in, moves, drives, asks, extra, news, news_sem,
    xsem, wsem, cross_sem, part_sem, fwd_sem, rx, prx,
    send1, recv1, send2, recv2, send3, recv3, send4, recv4, hello,
):
    _, _, span, kd = xs.shape
    width = wq_ref.shape[1]
    extent = width // heads
    key_rows = extent // sn
    chunks = rx.shape[3]
    kc = kd // chunks
    tme, me = lax.axis_index("tp"), lax.axis_index("sp")
    y, c = tme // 2, lax.rem(tme, 2)
    chips = tn // 2
    partner = y * 2 + (1 - c)
    g = group_of(sn, heads)
    groups = sn // g
    team, m = me // g, lax.rem(me, g)
    weights = (wq_ref, wk_ref, wv_ref, wg_ref)

    barrier = pltpu.get_barrier_semaphore()
    pl.semaphore_signal(barrier, inc=1, device_id={"tp": partner}, device_id_type=MESH)
    for d in range(1, chips):
        to = lax.rem(y + d, chips) * 2 + c
        pl.semaphore_signal(barrier, inc=1, device_id={"tp": to}, device_id_type=MESH)
    for d in range(1, sn):

        @pl.when(me + d < sn)
        def _():
            for t in (tme, partner):
                pl.semaphore_signal(barrier, inc=1, device_id={"sp": me + d, "tp": t}, device_id_type=MESH)

    order = [tme, partner]
    for d in range(1, chips):
        source = lax.rem(y - d + chips, chips)
        order += [source * 2 + c, source * 2 + (1 - c)]

    def cols(ck):
        return pl.ds(ck * kc, kc)

    def token_copy(s):
        return pltpu.make_async_copy(x_ref.at[pl.ds(s * span, span), :], xs.at[tme, s], xsem.at[s])

    def weight_copy(w, slot):
        start = pl.multiple_of(order[slot] * kd, kd)
        return pltpu.make_async_copy(
            weights[w].at[pl.ds(start, kd), :], wbuf.at[slot, w], wsem.at[slot]
        )

    small_copies = [
        pltpu.make_async_copy(a, b, small_sem.at[i])
        for i, (a, b) in enumerate(
            (
                (bw_hbm, bw_ref), (dw_hbm, dw_ref), (bias_hbm, bias_ref), (rate_hbm, rate_ref), (gain_hbm, gain_ref),
                (nq_hbm, nq_ref), (nk_hbm, nk_ref), (nv_hbm, nv_ref), (nb_hbm, nb_ref), (nd_hbm, nd_ref),
            )
        )
    ]
    for s in range(seqs):
        token_copy(s).start()
    for copy in small_copies:
        copy.start()
    pl.semaphore_wait(barrier, chips + 2 * me)

    def cross_copy(d, s, ck):
        to = lax.rem(y + d, chips) * 2 + c
        return pltpu.make_async_remote_copy(
            src_ref=xs.at[tme, s, :, cols(ck)], dst_ref=xs.at[tme, s, :, cols(ck)],
            send_sem=cross_sem.at[d - 1], recv_sem=rx.at[d - 1, 0, s, ck],
            device_id={"tp": to}, device_id_type=MESH,
        )

    def part_copy(s):
        return pltpu.make_async_remote_copy(
            src_ref=xs.at[tme, s], dst_ref=xs.at[tme, s],
            send_sem=part_sem.at[0], recv_sem=prx.at[s],
            device_id={"tp": partner}, device_id_type=MESH,
        )

    for s in range(seqs):
        token_copy(s).wait()
        for ck in range(chunks):
            for d in range(1, chips):
                cross_copy(d, s, ck).start()
        part_copy(s).start()
    for slot in range(tn):
        for w in range(4):
            weight_copy(w, slot).start()
    for d in range(1, sn):

        @pl.when(me >= d)
        def _():
            for t in (tme, partner):
                pl.semaphore_signal(hello, inc=1, device_id={"sp": me - d, "tp": t}, device_id_type=MESH)

    for copy in small_copies:
        copy.wait()
    for s in range(seqs):
        for i, ref in enumerate((nq_ref, nk_ref, nv_ref)):
            news[c, i, s * heads : (s + 1) * heads] = ref[s].astype(f32)
        for i, ref in enumerate((nb_ref, nd_ref)):
            for h in range(heads):
                news[c, 3 + i, s * heads + h : s * heads + h + 1] = jnp.full((1, extent), ref[s, h], f32)

    def news_copy():
        return pltpu.make_async_remote_copy(
            src_ref=news.at[0], dst_ref=news.at[0], send_sem=news_sem.at[0], recv_sem=news_sem.at[1],
            device_id={"tp": partner}, device_id_type=MESH,
        )

    @pl.when(c == 0)
    def _():
        news_copy().start()

    bd[...] = jnp.zeros_like(bd)
    bd[0 : bw_ref.shape[0]] = bw_ref[...]
    bd[PAD : PAD + dw_ref.shape[0]] = dw_ref[...]
    row = lax.broadcasted_iota(jnp.int32, (span, span), 0)
    col = lax.broadcasted_iota(jnp.int32, (span, span), 1)
    slot_of = lax.broadcasted_iota(jnp.int32, (PAD, 1), 0)
    bias = jnp.zeros((PAD, 1), f32)
    rate = jnp.zeros((PAD, 1), f32)
    for h in range(heads):
        bias = jnp.where(slot_of == h, bias_ref[h], bias)
        rate = jnp.where(slot_of == h, rate_ref[h], rate)

    def fwd_copy(d, s, ck):
        b = order[2 * d]
        return pltpu.make_async_remote_copy(
            src_ref=xs.at[b, s, :, cols(ck)], dst_ref=xs.at[b, s, :, cols(ck)],
            send_sem=fwd_sem.at[d - 1], recv_sem=rx.at[d - 1, 1, s, ck],
            device_id={"tp": partner}, device_id_type=MESH,
        )

    def arrive(d, side, s, ck):
        b = order[2 * d + side]
        pltpu.make_async_remote_copy(
            src_ref=xs.at[b, s, :, cols(ck)], dst_ref=xs.at[b, s, :, cols(ck)],
            send_sem=part_sem.at[0], recv_sem=rx.at[d - 1, side, s, ck],
            device_id={"tp": partner}, device_id_type=MESH,
        ).wait_recv()

    def small(x, start, depth, s, first):
        piece = bd[:, pl.ds(pl.multiple_of(start, depth), depth)]
        term = dot(piece, x, NT)
        sacc[s] = term if first else sacc[s] + term

    def use_whole(slot, s):
        b = order[slot]
        x = xs[b, s]
        if s == 0:
            weights_wait(slot)
        for w in range(4):
            term = dot(x, wbuf[slot, w])
            acc[s, w] = term if slot == 0 else acc[s, w] + term
        small(x, b * kd, kd, s, slot == 0)

    def weights_wait(slot):
        pltpu.make_async_copy(wbuf.at[slot], wbuf.at[slot], wsem.at[slot]).wait()

    def use(slot, s, ck, parts=(1, 2, 0, 3)):
        b = order[slot]
        x = xs[b, s, :, cols(ck)]
        if 1 in parts:
            if s == 0 and ck == 0:
                weights_wait(slot)
            small(x, b * kd + ck * kc, kc, s, False)
        for w in parts:
            acc[s, w] += dot(x, wbuf[slot, w, cols(ck), :])

    def forward(d, s, ck):
        arrive(d, 0, s, ck)
        fwd_copy(d, s, ck).start()

    def finish_chunk(d, s, ck, parts):
        use(2 * d, s, ck, parts)
        arrive(d, 1, s, ck)
        use(2 * d + 1, s, ck, parts)

    def heads_of(w, s):
        return [acc[s, w, :, h * extent : (h + 1) * extent].astype(bf16).astype(f32) for h in range(heads)]

    def owner_of(s, h):
        return (s * heads + h) % g

    def box_copy(s, h, to):
        return pltpu.make_async_remote_copy(
            src_ref=out_box.at[s, h], dst_ref=in_box.at[s, (1 - c) * g + m],
            send_sem=send1.at[s], recv_sem=recv1.at[s, m],
            device_id={"sp": team * g + to, "tp": y * 2 + 1}, device_id_type=MESH,
        )

    def boxes(s):
        beta = jax.nn.sigmoid(sacc[s, 0:PAD, :] + bias)
        pre = sacc[s, PAD : 2 * PAD, :]
        soft = jnp.maximum(pre, 0.0) + jnp.log1p(jnp.exp(-jnp.abs(pre)))
        upper = jnp.where(row <= col, 1.0, 0.0).astype(bf16)
        rest, pieces = -jnp.exp(rate) * soft, []
        for _ in range(3):
            pieces.append(rest.astype(bf16).astype(f32))
            rest = rest - pieces[-1]
        sums = dot(jnp.concatenate(pieces, axis=0).astype(bf16), upper)
        cum = sums[0:PAD] + sums[PAD : 2 * PAD] + sums[2 * PAD :]
        cum_t, beta_t = cum.T, beta.T
        cum_row[s] = cum
        cum_col[s] = cum_t
        hs, bs = range(heads), range(span // OUTER)
        line = lax.broadcasted_iota(jnp.int32, (OUTER, 2 * OUTER), 0)
        lane = lax.broadcasted_iota(jnp.int32, (OUTER, 2 * OUTER), 1)
        high = lane >= OUTER
        place = lane % OUTER
        same = line // INNER == place // INNER
        fill = jnp.zeros((OUTER, 2 * OUTER), bf16)
        unit = jnp.where(line == place, 1.0, 0.0)

        def part(b):
            return slice(b * OUTER, (b + 1) * OUTER)

        twice = [jnp.concatenate([cum[:, part(b)]] * 2, axis=1) for b in bs]
        k = [unit_rows(v) for v in heads_of(1, s)]
        kh = [v.astype(bf16) for v in k]
        pairs = [(h, b) for h in hs for b in bs]
        kk = [dot(kh[h][part(b)], jnp.concatenate([kh[h][part(b)]] * 2, axis=0), NT) for h, b in pairs]
        far = {(h, b): dot(kh[h][part(b)], kh[h][: b * OUTER], NT) for h, b in pairs if b > 0}
        right, kdec, last, low = [], [], [], []
        v = heads_of(2, s)
        for h in hs:
            cumc, bt = cum_t[:, h : h + 1], beta_t[:, h : h + 1]
            kh_buf[h] = kh[h]
            for b in bs:
                here = cumc[part(b)]
                wts = bt[part(b)] * jnp.exp(jnp.where(line >= place, here - twice[b][h : h + 1, :], 0.0))
                low.append(jnp.where(line > place, kk[h * len(bs) + b] * wts, 0.0))
                if b > 0:
                    wts = bt[part(b)] * jnp.exp(here - cum[h : h + 1, : b * OUTER])
                    far[h, b] = (far[h, b] * wts).astype(bf16)
            kb = k[h] * bt
            right.append(jnp.concatenate([v[h] * bt, kb * jnp.exp(cumc)], axis=1).astype(bf16))
            end = cumc[span - 1 :, :]
            kdec.append((k[h] * jnp.exp(end - cumc)).astype(bf16))
            last.append(jnp.exp(end))

        def climb(block):
            half = block.astype(bf16)
            return dot(half[:, :OUTER], half)

        z = [jnp.where(high, unit - n, n) for n in (jnp.where(same, m, 0.0) for m in low)]
        z = [jnp.where(high, a, climb(a)) for a in z]
        reached = 2
        while reached < INNER:
            z = [climb(a) + jnp.where(high, a, 0.0) for a in z]
            reached *= 2
        under = [jnp.concatenate([fill, jnp.where(high | same, 0.0, m).astype(bf16)], axis=0) for m in low]
        z = [a + dot(a.astype(bf16), u) for a, u in zip(z, under)]
        z = [jnp.where(high, a - t, t) for a, t in ((a, climb(a)) for a in z)]
        reached = 2
        while reached < OUTER // INNER:
            z = [climb(a) + jnp.where(high, a, 0.0) for a in z]
            reached *= 2
        inv = {p: a.astype(bf16) for p, a in zip(pairs, z)}
        none = jnp.zeros((OUTER, 2 * extent), bf16)
        term = {(h, b): dot(inv[h, b], jnp.concatenate([none, right[h][part(b)]], axis=0)) for h, b in pairs}
        far = {
            (h, b): dot(inv[h, b], jnp.concatenate([jnp.zeros_like(m), m], axis=0)).astype(bf16)
            for (h, b), m in far.items()
        }
        done = [[term[h, 0].astype(bf16)] for h in hs]
        for b in bs[1:]:
            for h in hs:
                seen = jnp.concatenate(done[h], axis=0) if b > 1 else done[h][0]
                done[h].append((term[h, b] - dot(far[h, b], seen)).astype(bf16))
        uw = [jnp.concatenate(d, axis=0) for d in done]
        z = [dot(a, u, TN) for a, u in zip(kdec, uw)]
        eye = lax.broadcasted_iota(jnp.int32, (extent, extent), 0) == lax.broadcasted_iota(
            jnp.int32, (extent, extent), 1
        )
        for h in hs:
            out_box[s, h, 0] = (jnp.where(eye, last[h] - 1.0, 0.0) - z[h][:, extent:]).astype(bf16)
            out_box[s, h, 1] = z[h][:, :extent].astype(bf16)
            uw_buf[h] = uw[h]
        if s == 0:

            @pl.when(me < sn - 1)
            def _():
                pl.semaphore_wait(hello, 2 * (sn - 1 - me))

        for r in reversed(range(g)):
            to = m
            for bit in (b for b in (1 << i for i in range(g.bit_length())) if r & b):
                to = to + bit * (1 - 2 * lax.rem(m // bit, 2))
            h = lax.rem(to + g - (s * heads) % g, g)
            if r == 0:

                @pl.when((h < heads) & (c == 1))
                def _():
                    in_box[s, m] = out_box[s, h]

            @pl.when((h < heads) & ((c == 0) | (r > 0)))
            def _():
                box_copy(s, h, to).start()

    def queries(s):
        cum, cum_t = cum_row[s], cum_col[s]
        gain = gain_ref[...]
        hs = range(heads)
        causal = row >= col

        def spread(h):
            gap = jnp.where(causal, cum_t[:, h : h + 1] - cum[h : h + 1, :], 0.0)
            return jnp.where(causal, jnp.exp(gap), 0.0)

        q = [unit_rows(v) for v in heads_of(0, s)]
        scores = [(dot(q[h].astype(bf16), kh_buf[h], NT) * spread(h)).astype(bf16) for h in hs]
        out = [dot(scores[h], uw_buf[h]) for h in hs]
        gates = heads_of(3, s)
        for h in hs:
            local_out[s, h] = out[h][:, :extent]
            reach[s, h] = (q[h] * jnp.exp(cum_t[:, h : h + 1]) - out[h][:, extent:]).astype(bf16)
            gated[s, h] = gates[h] * jax.nn.sigmoid(gates[h]) * gain

    def own_head(s):
        return lax.rem(m + g - (s * heads) % g, g)

    def owner(s):
        return (own_head(s) < heads) & (c == 1)

    def back_copy(s, e, i):
        return pltpu.make_async_remote_copy(
            src_ref=back_out.at[s, e * g + i], dst_ref=back_in.at[s, own_head(s)],
            send_sem=send2.at[s], recv_sem=recv2.at[s],
            device_id={"sp": team * g + i, "tp": y * 2 + 1 - e}, device_id_type=MESH,
        )

    def mid_copy(s):
        return pltpu.make_async_remote_copy(
            src_ref=mid_out.at[s], dst_ref=mid_in.at[s], send_sem=send3.at[s], recv_sem=recv3.at[s],
            device_id={"sp": lax.rem(me + g, sn)}, device_id_type=MESH,
        )

    def tail_copy(s, e, j):
        return pltpu.make_async_remote_copy(
            src_ref=tail_out.at[s, e * sn + j], dst_ref=tail_in.at[s, own_head(s)],
            send_sem=send4.at[s], recv_sem=recv4.at[s],
            device_id={"sp": j, "tp": y * 2 + 1 - e}, device_id_type=MESH,
        )

    def settle(ref, sem):
        pltpu.make_async_copy(ref, ref, sem).wait()

    def box_wait(s, i):
        @pl.when(i == m)
        def _():
            settle(in_box.at[s, pl.ds(0, 1)], recv1.at[s, i])

        @pl.when(i != m)
        def _():
            settle(in_box.at[s, pl.ds(0, 2)], recv1.at[s, i])

    def give_back(s):
        for i in range(g):
            back_copy(s, 1, i).start()

            @pl.when(i == m)
            def _():
                back_in[s, own_head(s)] = back_out[s, i]

            @pl.when(i != m)
            def _():
                back_copy(s, 0, i).start()

    def prepare(s):
        r = s * heads + own_head(s)
        for e in range(2):
            told = [news[1 - e, i, pl.ds(r, 1), :] for i in range(3)]
            qn, kn = unit_rows(told[0]), unit_rows(told[1])
            rest = jnp.concatenate([jnp.broadcast_to(qn, (PAD, extent)), jnp.broadcast_to(kn, (PAD, extent))], axis=0)
            for i in range(3):
                piece = rest.astype(bf16)
                asks[s, e, i * 2 * PAD : (i + 1) * 2 * PAD] = piece
                rest = rest - piece.astype(f32)
            decay, meet = news[1 - e, 4, pl.ds(r, 1), :], jnp.sum(kn * qn, axis=-1, keepdims=True)
            extra[s, e, 0:1] = told[2]
            extra[s, e, 1:2] = news[1 - e, 3, pl.ds(r, 1), :] * meet
            extra[s, e, 2:3] = decay

    def conclude(s, finals):
        kept_h = [final.astype(bf16) for final in finals]
        sums = [dot(asks[s, e], kept_h[e]) for e in range(2)]
        keep = tail_out.shape[2] - PAD
        for e in range(2):
            for j in range(sn):
                tail_out[s, e * sn + j, 0:key_rows] = kept_h[e][j * key_rows : (j + 1) * key_rows]
        words = []
        for e in range(2):
            part = sums[e][0 : 2 * PAD] + sums[e][2 * PAD : 4 * PAD] + sums[e][4 * PAD :]
            recall, retrieve, decay = part[0:1], part[PAD : PAD + 1], extra[s, e, 2:3]
            read = decay * recall + extra[s, e, 1:2] * (extra[s, e, 0:1] - decay * retrieve)
            norm = lax.rsqrt(jnp.mean(read * read, axis=-1, keepdims=True) + norm_floor)
            rest, rows = read * norm * gain_ref[...], []
            for _ in range(3):
                rows.append(rest.astype(bf16).astype(f32))
                rest = rest - rows[-1]
            words.append(jnp.concatenate(rows + [jnp.zeros((PAD - 3, extent), f32)], axis=0).astype(bf16))
        for e in range(2):
            for j in range(sn):
                tail_out[s, e * sn + j, keep:] = words[e]
        for j in range(sn):
            tail_copy(s, 1, j).start()

            @pl.when(j == me)
            def _():
                tail_in[s, own_head(s)] = tail_out[s, j]

            @pl.when(j != me)
            def _():
                tail_copy(s, 0, j).start()

    def chain_first(s):
        @pl.when(owner(s) & (team == 0))
        def _():
            if groups == 1:
                prepare(s)
            state = [jnp.zeros((extent, extent), f32)] * 2
            for i in range(g):
                box_wait(s, i)
                half = [a.astype(bf16) for a in state]
                for e in range(2):
                    back_out[s, e * g + i] = half[e]
                boxes_i = [in_box.at[s, e * g + i] for e in range(2)]
                if i == 0:
                    state = [b[1].astype(f32) for b in boxes_i]
                else:
                    state = [a + dot(b[0], h) + b[1].astype(f32) for a, b, h in zip(state, boxes_i, half)]
            if groups > 1:
                for e in range(2):
                    mid_out[s, e] = state[e].astype(bf16)
                mid_copy(s).start()
            if groups == 1:
                conclude(s, state)
            give_back(s)

    def compose(s):
        if groups == 1:
            return

        @pl.when(owner(s) & (team > 0))
        def _():
            prepare(s)
            shift, drive = [None] * 2, [None] * 2
            for i in range(g):
                box_wait(s, i)
                for e in range(2):
                    step, push = in_box[s, e * g + i, 0], in_box[s, e * g + i, 1].astype(f32)
                    if i == 0:
                        shift[e], drive[e] = step.astype(f32), push
                    else:
                        shift[e], drive[e] = (
                            shift[e] + step.astype(f32) + dot(step, shift[e].astype(bf16)),
                            drive[e] + push + dot(step, drive[e].astype(bf16)),
                        )
                    moves[s, e, i * extent : (i + 1) * extent] = shift[e].astype(bf16)
                    drives[s, e, i * extent : (i + 1) * extent] = drive[e]

    def relay(s):
        if groups == 1:
            return

        @pl.when(owner(s) & (team > 0))
        def _():
            pltpu.make_async_remote_copy(
                src_ref=mid_out.at[s], dst_ref=mid_in.at[s], send_sem=send3.at[s], recv_sem=recv3.at[s],
                device_id={"sp": lax.rem(me + sn - g, sn)}, device_id_type=MESH,
            ).wait_recv()
            start = [mid_in[s, e] for e in range(2)]
            base = [a.astype(f32) for a in start]
            top = (g - 1) * extent
            state = [base[e] + dot(moves[s, e, top:], start[e]) + drives[s, e, top:] for e in range(2)]

            @pl.when(team < groups - 1)
            def _():
                for e in range(2):
                    mid_out[s, e] = state[e].astype(bf16)
                mid_copy(s).start()

            @pl.when(team == groups - 1)
            def _():
                conclude(s, state)

            for e in range(2):
                moved = dot(moves[s, e, :top], start[e]) + drives[s, e, :top]
                back_out[s, e * g] = start[e]
                for i in range(1, g):
                    back_out[s, e * g + i] = (base[e] + moved[(i - 1) * extent : i * extent]).astype(bf16)
            give_back(s)

    def arrivals(own, ref, sem):
        if heads > 1:

            @pl.when(own)
            def _():
                settle(ref.at[pl.ds(0, heads - 1)], sem)

        @pl.when(jnp.logical_not(own))
        def _():
            settle(ref, sem)

    def finish(s):
        arrivals(owner(s), back_in.at[s], recv2.at[s])
        outs = [local_out[s, h] + dot(reach[s, h], back_in[s, h]) for h in range(heads)]
        for h in range(heads):
            o = outs[h]
            norm = lax.rsqrt(jnp.mean(o * o, axis=-1, keepdims=True) + norm_floor)
            mixed_ref[s * span : (s + 1) * span, h * extent : (h + 1) * extent] = (o * norm * gated[s, h]).astype(bf16)

    def take_tail(s):
        arrivals((team == groups - 1) & owner(s), tail_in.at[s], recv4.at[s])
        keep = tail_in.shape[2] - PAD
        for h in range(heads):
            cache_ref[s * heads + h] = tail_in[s, h, 0:key_rows]
            rows = tail_in[s, h, keep:].astype(f32)
            first_ref[s : s + 1, h * extent : (h + 1) * extent] = rows[0:1] + rows[1:2] + rows[2:3]

    def apart(step, *args):
        @pl.when(me >= 0)
        def _():
            step(*args)

    for s in range(seqs):
        use_whole(0, s)
    for s in range(seqs):
        pltpu.make_async_remote_copy(
            src_ref=xs.at[partner, s], dst_ref=xs.at[partner, s], send_sem=part_sem.at[0], recv_sem=prx.at[s],
            device_id={"tp": partner}, device_id_type=MESH,
        ).wait_recv()
        use_whole(1, s)

    @pl.when(c == 1)
    def _():
        news_copy().wait_recv()

    for s in range(seqs):
        for ck in range(chunks):
            for d in range(1, chips):
                if s == 0 or ck > 0:
                    forward(d, s, ck)
                finish_chunk(d, s, ck, (1, 2) if ck == chunks - 1 else (1, 2, 0, 3))
        apart(boxes, s)
        if s > 0:
            chain_first(s - 1)
            compose(s - 1)
        if s < seqs - 1:
            for d in range(1, chips):
                forward(d, s + 1, 0)
        for slot in range(2, tn):
            use(slot, s, chunks - 1, (0, 3))
        queries(s)
        if s > 0:
            relay(s - 1)
    compose(seqs - 1)
    chain_first(seqs - 1)
    relay(seqs - 1)
    for s in range(seqs):
        finish(s)
    settle(xs.at[tme], part_sem.at[0])
    for d in range(1, chips):
        settle(xs.at[tme], cross_sem.at[d - 1])
        settle(xs.at[tme], fwd_sem.at[d - 1])
    for s in range(seqs):
        arrivals(owner(s), out_box.at[s], send1.at[s])

        @pl.when(owner(s))
        def _():
            settle(back_out.at[s, pl.ds(0, 2 * g - 1)], send2.at[s])

            @pl.when(team < groups - 1)
            def _():
                mid_copy(s).wait_send()

            @pl.when(team == groups - 1)
            def _():
                settle(tail_out.at[s, pl.ds(0, 2 * sn - 1)], send4.at[s])

    @pl.when(c == 0)
    def _():
        news_copy().wait_send()

    for s in range(seqs):
        take_tail(s)


def fused(tn, sn, seqs, heads, tokens, weights, bw, dw, bias, rate, gain, nq, nk, nv, nb, nd):
    rows, kd = tokens.shape
    width = weights[0].shape[1]
    kc = 256 if kd % 256 == 0 else kd
    chunks, chips, span = kd // kc, tn // 2, rows // seqs
    extent = width // heads
    pairs, key_rows = seqs * heads, extent // sn
    g = group_of(sn, heads)
    tail = -(-key_rows // PAD) * PAD + PAD
    operands = (tokens, *weights, bw, dw, bias, rate, gain, nq, nk, nv, nb, nd)
    vmem = pl.BlockSpec(memory_space=pltpu.VMEM)
    hbm = pl.BlockSpec(memory_space=pltpu.HBM)
    dma = pltpu.SemaphoreType.DMA
    return pl.pallas_call(
        functools.partial(fused_kernel, tn, sn, seqs, heads),
        out_shape=(
            jax.ShapeDtypeStruct((rows, width), bf16),
            jax.ShapeDtypeStruct((pairs, key_rows, extent), bf16),
            jax.ShapeDtypeStruct((seqs, width), f32),
        ),
        in_specs=[hbm] * 15,
        out_specs=(vmem,) * 3,
        scratch_shapes=[
            pltpu.VMEM(bw.shape, bf16),
            pltpu.VMEM(dw.shape, bf16),
            pltpu.SMEM(bias.shape, f32),
            pltpu.SMEM(rate.shape, f32),
            pltpu.VMEM(gain.shape, f32),
            pltpu.VMEM(nq.shape, bf16),
            pltpu.VMEM(nk.shape, bf16),
            pltpu.VMEM(nv.shape, bf16),
            pltpu.SMEM(nb.shape, f32),
            pltpu.SMEM(nd.shape, f32),
            dma((10,)),
            pltpu.VMEM((2 * PAD, bw.shape[1]), bf16),
            pltpu.VMEM((tn, seqs, span, kd), bf16),
            pltpu.VMEM((tn, 4, kd, width), bf16),
            pltpu.VMEM((seqs, 4, span, width), f32),
            pltpu.VMEM((seqs, 2 * PAD, span), f32),
            pltpu.VMEM((seqs, PAD, span), f32),
            pltpu.VMEM((seqs, span, PAD), f32),
            pltpu.VMEM((heads, span, extent), bf16),
            pltpu.VMEM((heads, span, 2 * extent), bf16),
            pltpu.VMEM((seqs, heads, span, extent), f32),
            pltpu.VMEM((seqs, heads, span, extent), bf16),
            pltpu.VMEM((seqs, heads, span, extent), f32),
            pltpu.VMEM((seqs, heads, 2, extent, extent), bf16),
            pltpu.VMEM((seqs, 2 * g, 2, extent, extent), bf16),
            pltpu.VMEM((seqs, 2, extent, extent), bf16),
            pltpu.VMEM((seqs, 2, extent, extent), bf16),
            pltpu.VMEM((seqs, 2 * g, extent, extent), bf16),
            pltpu.VMEM((seqs, heads, extent, extent), bf16),
            pltpu.VMEM((seqs, 2 * sn, tail, extent), bf16),
            pltpu.VMEM((seqs, heads, tail, extent), bf16),
            pltpu.VMEM((seqs, 2, g * extent, extent), bf16),
            pltpu.VMEM((seqs, 2, g * extent, extent), f32),
            pltpu.VMEM((seqs, 2, 6 * PAD, extent), bf16),
            pltpu.VMEM((seqs, 2, PAD, extent), f32),
            pltpu.VMEM((2, 5, pairs, extent), f32),
            dma((2,)),
            dma((seqs,)),
            dma((tn,)),
            dma((chips - 1,)),
            dma((1,)),
            dma((chips - 1,)),
            dma((chips - 1, 2, seqs, chunks)),
            dma((seqs,)),
            dma((seqs,)),
            dma((seqs, g)),
            dma((seqs,)),
            dma((seqs,)),
            dma((seqs,)),
            dma((seqs,)),
            dma((seqs,)),
            dma((seqs,)),
            pltpu.SemaphoreType.REGULAR,
        ],
        compiler_params=pltpu.CompilerParams(
            collective_id=0, has_side_effects=True, vmem_limit_bytes=53 * 1024 * 1024
        ),
    )(*[pltpu.with_memory_space_constraint(a, pltpu.HBM) for a in operands])


def emit_kernel(mixed_ref, cache_ref, first_ref, mixed_out, cache_out, first_out, sem):
    copies = [
        pltpu.make_async_copy(a, b, sem.at[i])
        for i, (a, b) in enumerate(((mixed_ref, mixed_out), (cache_ref, cache_out), (first_ref, first_out)))
    ]
    for copy in copies:
        copy.start()
    for copy in copies:
        copy.wait()


def emit(*results):
    return pl.pallas_call(
        emit_kernel,
        out_shape=tuple(jax.ShapeDtypeStruct(r.shape, r.dtype) for r in results),
        in_specs=[pl.BlockSpec(memory_space=pltpu.VMEM)] * 3,
        out_specs=(pl.BlockSpec(memory_space=pltpu.HBM),) * 3,
        scratch_shapes=[pltpu.SemaphoreType.DMA((3,))],
        compiler_params=pltpu.CompilerParams(vmem_limit_bytes=4 * 1024 * 1024),
    )(*results)


def shards(
    tokens, query_weight, key_weight, value_weight, gate_weight, beta_weight, decay_weight,
    beta_bias, rate_log, out_gain, new_query, new_key, new_value, new_beta, new_decay,
):
    seqs, span, kd = tokens.shape
    heads = rate_log.shape[0]
    extent = out_gain.shape[0]
    tp, sp = lax.axis_size("tp"), lax.axis_size("sp")
    weights = (query_weight, key_weight, value_weight, gate_weight)
    mixed, cache, first = fused(
        tp, sp, seqs, heads, tokens.reshape(seqs * span, kd), weights, beta_weight.T, decay_weight.T, beta_bias,
        rate_log, out_gain[None], new_query, new_key, new_value, new_beta, new_decay,
    )
    return emit(
        mixed.reshape(seqs, span, heads * extent), cache.reshape(seqs, heads, extent // sp, extent), first
    )


def solution(mesh):
    placed = (
        P(None, "sp", "tp"),
        P(None, "tp"),
        P(None, "tp"),
        P(None, "tp"),
        P(None, "tp"),
        P(None, "tp"),
        P(None, "tp"),
        P("tp"),
        P("tp"),
        P(),
        P(None, "tp", None),
        P(None, "tp", None),
        P(None, "tp", None),
        P(None, "tp"),
        P(None, "tp"),
    )
    return jax.shard_map(
        shards,
        mesh=mesh,
        in_specs=placed,
        out_specs=(P(None, "sp", "tp"), P(None, "tp", "sp", None), P(None, "tp")),
        check_vma=False,
    )
```
